128 devices in a mesh: ep: 32 (over z, y, core), tp: 4 (over x).
Axes of the slice: x: 4, y: 4, z: 4, core: 2. Of those that a mesh axis runs over, the one named last changes fastest.
Arguments:
- queries: bfloat16 [16384, 1024], P('ep', 'tp'), may hold values from -6 to 6
- key_rows: bfloat16 [16384, 512], P('ep', 'tp'), may hold values from -6 to 6
- value_rows: bfloat16 [16384, 512], P('ep', 'tp'), may hold values from -6 to 6
- forget_logit: float32 [8, 16384], P('tp', 'ep'), may hold values from -1 to 17
- out_weight: bfloat16 [1024, 2048], P('tp'), may hold values from -0.1875 to 0.1875
- out_gain: float32 [2048], replicated, may hold values from 0.1 to 1.9
- moe_input: bfloat16 [16384, 2048], P('ep'), may hold values from -6 to 6
- moe_gain: float32 [2048], replicated, may hold values from 0.1 to 1.9
- router_group: bfloat16 [2048, 4], replicated, may hold values from -2 to 2
- router_expert: bfloat16 [2048, 32], replicated, may hold values from -0.125 to 0.125
- route_group: int32 [16384], P('ep'), may hold values from 0 to 3
- route_pick: int32 [16384, 2], P('ep'), may hold values from 0 to 7, as said below
- expert_gate: bfloat16 [32, 2048, 1024], P('ep', None, 'tp'), may hold values from -0.125 to 0.125
- expert_up: bfloat16 [32, 2048, 1024], P('ep', None, 'tp'), may hold values from -0.125 to 0.125
- expert_down: bfloat16 [32, 1024, 2048], P('ep', 'tp'), may hold values from -42 to 42
Outputs:
- mixer_out: bfloat16 [16384, 2048], P(('ep', 'tp'))
- moe_out: bfloat16 [16384, 2048], P(('ep', 'tp'))
The draws below stay inside these ranges and needn't reach their ends.
Inputs may be any that keep to these rules, and one draw needn't show every extreme that they name: `route_pick`: the two entries of a row differ.
All inputs are finite; a program needn't handle non-finite values.
Results may differ from the reference program's by a relative error of at most 0.013.
Values may be sent and summed in bfloat16 or wider, within the bound.
No kernel may reach another device: no remote copies, remote signals or barrier semaphores. Data moves between devices by JAX's collectives and lax.ppermute only.
A program may use at most 128 MiB of HBM per device.

```python
import math
import jax
import jax.numpy as jnp
from jax import lax

D = 2048
H = 8
KVH = 4
DH = 128
FF = 1024
GROUPS = 4
TOK_DEV = 128
EXPERTS = 32
CAPD = 16
TOKENS_A = 16384
TOKENS_B = 16384
N_TP = 4


def draw_queries(key, part):
    own_key = jax.random.fold_in(key, 21)
    values = jnp.clip(jax.random.normal(own_key, (TOKENS_A, H * DH), jnp.float32), -6.0, 6.0)
    return values.astype(jnp.bfloat16)


def draw_key_rows(key, part):
    own_key = jax.random.fold_in(key, 22)
    values = jnp.clip(jax.random.normal(own_key, (TOKENS_A, KVH * DH), jnp.float32), -6.0, 6.0)
    return values.astype(jnp.bfloat16)


def draw_forget_logit(key, part):
    order_key, block_key, noise_key = jax.random.split(jax.random.fold_in(key, 31), 3)
    ranking = jax.random.permutation(order_key, H)
    slow = ranking >= H // 2
    base = jnp.where(slow, jnp.log(1.0 * TOKENS_A), jnp.log(50.0))
    shift = jax.random.uniform(block_key, (H, EXPERTS), jnp.float32, -0.8, 0.8)
    shift = jnp.repeat(shift, TOKENS_A // EXPERTS, axis=1)
    noise = 0.7 * jnp.clip(jax.random.normal(noise_key, (H, TOKENS_A), jnp.float32), -4.0, 4.0)
    return (base[:, None] + shift + noise).astype(jnp.float32)


def group_directions(key):
    sign_key, common_key = jax.random.split(jax.random.fold_in(key, 43))
    directions = jnp.where(jax.random.randint(sign_key, (GROUPS, D), 0, 2) == 0, -1.0, 1.0)
    common = jnp.where(jax.random.randint(common_key, (D,), 0, 2) == 0, -1.0, 1.0)
    return (directions.astype(jnp.float32), common.astype(jnp.float32))


def routing(key):
    base = jax.random.fold_in(key, 61)
    group_key, first_key, second_key, hot_key, pick_key, order_key = jax.random.split(base, 6)
    per_group = EXPERTS // GROUPS
    groups = jax.random.randint(group_key, (TOKENS_B,), 0, GROUPS)
    first = jax.random.randint(first_key, (TOKENS_B,), 0, per_group)
    offset = jax.random.randint(second_key, (TOKENS_B,), 0, per_group - 1)
    hot_group = jax.random.randint(hot_key, (), 0, GROUPS)
    hot_pick = jax.random.randint(pick_key, (), 0, per_group)
    blocks = TOKENS_B // TOK_DEV
    scores = jax.random.randint(order_key, (blocks, TOK_DEV), 0, 1 << 20) * TOK_DEV
    scores = scores + jnp.arange(TOK_DEV, dtype=jnp.int32)[None, :]
    ranking = jnp.argsort(jnp.argsort(scores, axis=1), axis=1).reshape(-1)
    forced = ranking < CAPD
    groups = jnp.where(forced, hot_group, groups)
    first = jnp.where(forced, hot_pick, first)
    second = (first + 1 + offset) % per_group
    return (groups.astype(jnp.int32), jnp.stack([first, second], axis=1).astype(jnp.int32))


def draw_moe_input(key, part):
    groups = routing(key)[0]
    directions, common = group_directions(key)
    noise_key = jax.random.fold_in(key, 41)
    level_key, jitter_key, mark_key, sign_key = jax.random.split(jax.random.fold_in(key, 44), 4)
    noise = jnp.clip(jax.random.normal(noise_key, (TOKENS_B, D), jnp.float32), -4.0, 4.0)
    level = jax.random.uniform(level_key, (TOKENS_B, 1), jnp.float32, 0.35, 0.7)
    jitter = jax.random.uniform(jitter_key, (TOKENS_B, GROUPS), jnp.float32, 0.8, 1.2)
    routed = jnp.arange(GROUPS, dtype=jnp.int32)[None, :] == groups[:, None]
    amounts = level * jnp.where(routed, -1.0, jitter)
    values = noise + jnp.dot(amounts, directions, precision=lax.Precision.HIGHEST)
    return jnp.clip(values, -6.0, 6.0).astype(jnp.bfloat16)


def draw_router_group(key, part):
    directions, common = group_directions(key)
    own_key = jax.random.fold_in(key, 51)
    noise = 0.2 * jnp.clip(jax.random.normal(own_key, (D, GROUPS), jnp.float32), -6.0, 6.0) / jnp.sqrt(1.0 * D)
    values = noise + 5.0 * directions.T / D
    return values.astype(jnp.bfloat16)


def draw_route_group(key, part):
    return routing(key)[0]


def draw_route_pick(key, part):
    return routing(key)[1]


def block_scale(key, shape, shards, smallest, largest):
    loudness, own = 1.0, jax.random.fold_in(key, 6)
    for dim, blocks in shards:
        heights = jnp.exp(jax.random.uniform(jax.random.fold_in(own, dim), (blocks,), jnp.float32, smallest / len(shards), largest / len(shards)))
        loudness = loudness * jnp.repeat(heights, shape[dim] // blocks).reshape([-1 if axis == dim else 1 for axis in range(len(shape))])
    return loudness


def normal_values(key, dims, deviation, bound, pieces=(), kind=jnp.bfloat16):
    factor_of = block_scale(key, dims, pieces, -0.22, 0.18) if pieces else 1.0
    values = jax.random.normal(key, dims, jnp.float32) * deviation * factor_of
    return jnp.minimum(jnp.maximum(values, -bound), bound).astype(kind)


def setup_inputs(seed: int = 0) -> dict:
    seeds = jax.random.split(jax.random.key(seed), 16)
    queries = draw_queries(jax.random.fold_in(seeds[15], 71), 0)
    key_rows = draw_key_rows(jax.random.fold_in(seeds[15], 71), 0)
    value_rows = normal_values(seeds[2], (TOKENS_A, KVH * DH), 1.0, 6.0, ((0, 32), (1, 4)))
    forget_logit = draw_forget_logit(jax.random.fold_in(seeds[15], 71), 0)
    out_weight = normal_values(seeds[4], (H * DH, D), (H * DH) ** -0.5, 0.1875, ((0, 4),))
    out_gain = jnp.clip(1.0 + 0.18 * jax.random.normal(seeds[5], (D,), jnp.float32), 0.1, 1.9)
    moe_input = draw_moe_input(jax.random.fold_in(seeds[15], 71), 0)
    moe_gain = jnp.clip(1.0 + 0.18 * jax.random.normal(seeds[7], (D,), jnp.float32), 0.1, 1.9)
    router_group = draw_router_group(jax.random.fold_in(seeds[15], 71), 0)
    router_expert = normal_values(seeds[9], (D, EXPERTS), D ** -0.5, 0.125)
    route_group = draw_route_group(jax.random.fold_in(seeds[15], 71), 0)
    route_pick = draw_route_pick(jax.random.fold_in(seeds[15], 71), 0)
    expert_gate = normal_values(seeds[12], (EXPERTS, D, FF), D ** -0.5, 0.125, ((0, 32), (2, 4)))
    expert_up = normal_values(seeds[13], (EXPERTS, D, FF), D ** -0.5, 0.125, ((0, 32), (2, 4)))
    expert_down = normal_values(seeds[14], (EXPERTS, FF, D), 7.0, 42.0, ((0, 32), (1, 4)))
    return {"queries": queries, "key_rows": key_rows, "value_rows": value_rows, "forget_logit": forget_logit, "out_weight": out_weight, "out_gain": out_gain, "moe_input": moe_input, "moe_gain": moe_gain, "router_group": router_group, "router_expert": router_expert, "route_group": route_group, "route_pick": route_pick, "expert_gate": expert_gate, "expert_up": expert_up, "expert_down": expert_down}


def rms_scale(row_block, scale_gain):
    values = row_block.astype(jnp.float32)
    return values * lax.rsqrt(lax.optimization_barrier(jnp.mean(values * values, axis=-1, keepdims=True)) + 1e-06) * scale_gain

def slot_ranks(chosen, block_rows, experts):
    expert_ids = jnp.arange(experts, dtype=jnp.int32)
    matches = chosen[:, :, None] == expert_ids
    usage = jnp.any(matches, axis=1).astype(jnp.int32)
    grouped = usage.reshape(-1, block_rows, experts)
    before = (jnp.cumsum(grouped, axis=1) - grouped).reshape(-1, experts)
    return lax.optimization_barrier(jnp.sum(jnp.where(matches, before[:, None, :], 0), axis=2)).astype(jnp.int32)

def reference(queries, key_rows, value_rows, forget_logit, out_weight, out_gain, moe_input, moe_gain, router_group, router_expert, route_group, route_pick, expert_gate, expert_up, expert_down):
    length = TOKENS_A
    ratio = H // KVH
    cum_gate = jnp.cumsum(jax.nn.log_sigmoid(forget_logit), axis=1)
    query_heads = queries.reshape(length, H, DH)
    key_heads = key_rows.reshape(length, KVH, DH)
    value_heads = value_rows.reshape(length, KVH, DH)
    block_len = math.gcd(512, length)
    positions = jnp.arange(length, dtype=jnp.int32)

    def one_block(block_index):
        start = (block_index * block_len).astype(jnp.int32)
        query_block = lax.dynamic_slice_in_dim(query_heads, start, block_len, 0)
        cum_block = lax.dynamic_slice_in_dim(cum_gate, start, block_len, 1)
        query_pos = start + jnp.arange(block_len, dtype=jnp.int32)
        visible = positions[None, :] <= query_pos[:, None]
        results = []
        for head_index in range(H):
            shared = head_index // ratio
            scores = jnp.dot(query_block[:, head_index], key_heads[:, shared].T, preferred_element_type=jnp.float32) / math.sqrt(DH)
            scores = scores + cum_block[head_index][:, None] - cum_gate[head_index][None, :]
            scores = jnp.where(visible, scores, -jnp.inf)
            row_top = lax.optimization_barrier(jnp.max(scores, axis=1, keepdims=True))
            expo = jnp.exp(scores - row_top)
            row_total = lax.optimization_barrier(jnp.sum(expo, axis=1, keepdims=True))
            weighted = jnp.dot(expo.astype(jnp.bfloat16), value_heads[:, shared], preferred_element_type=jnp.float32)
            results.append((weighted / row_total).astype(jnp.bfloat16))
        return jnp.concatenate(results, axis=1)
    attended = lax.map(one_block, jnp.arange(length // block_len, dtype=jnp.int32)).reshape(length, H * DH)
    block_width = H * DH // N_TP
    projected = jnp.zeros((length, D), jnp.float32)
    for portion in range(N_TP):
        piece = jnp.dot(attended[:, portion * block_width:(portion + 1) * block_width], out_weight[portion * block_width:(portion + 1) * block_width], preferred_element_type=jnp.float32).astype(jnp.bfloat16)
        projected = projected + lax.optimization_barrier(piece).astype(jnp.float32)
    mixer_out = rms_scale(projected, out_gain).astype(jnp.bfloat16)
    tokens = TOKENS_B
    experts = EXPERTS
    per_group = experts // GROUPS
    normed = rms_scale(moe_input, moe_gain).astype(jnp.bfloat16)
    group_logits = jnp.dot(normed, router_group, preferred_element_type=jnp.float32)
    expert_logits = jnp.dot(normed, router_expert, preferred_element_type=jnp.float32)
    group_top = lax.optimization_barrier(jnp.max(group_logits, axis=1, keepdims=True))
    group_exp = jnp.exp(group_logits - group_top)
    group_hit = jnp.arange(GROUPS, dtype=jnp.int32)[None, :] == route_group[:, None]
    group_share = lax.optimization_barrier(jnp.sum(jnp.where(group_hit, group_exp, 0.0), axis=1)) / lax.optimization_barrier(jnp.sum(group_exp, axis=1))
    chosen = (route_group[:, None] * per_group + route_pick).astype(jnp.int32)
    expert_hit = jnp.arange(experts, dtype=jnp.int32)[None, None, :] == chosen[:, :, None]
    picked_logits = lax.optimization_barrier(jnp.sum(jnp.where(expert_hit, expert_logits[:, None, :], 0.0), axis=2))
    shares = group_share[:, None] * jax.nn.sigmoid(picked_logits - picked_logits[:, ::-1])
    slot_rank = slot_ranks(chosen, TOK_DEV, experts)
    is_kept = slot_rank < CAPD
    slots = tokens // TOK_DEV * CAPD
    block_of = (jnp.arange(tokens, dtype=jnp.int32) // TOK_DEV)[:, None]
    slot_pos = (block_of * CAPD + slot_rank).astype(jnp.int32)
    target = jnp.where(is_kept, chosen * slots + slot_pos, experts * slots).astype(jnp.int32)
    sources = jnp.broadcast_to(jnp.arange(tokens, dtype=jnp.int32)[:, None], target.shape)
    slot_table = jnp.full((experts * slots,), tokens, jnp.int32).at[target.reshape(-1)].set(sources.reshape(-1), mode='drop').reshape(experts, slots)
    padded = jnp.concatenate([normed, jnp.zeros((1, D), jnp.bfloat16)], axis=0)
    quarter = FF // N_TP

    def one_expert(inputs):
        table_row, gate_w, up_w, down_w = inputs
        gathered = padded[table_row]
        gated = jnp.dot(gathered, gate_w, preferred_element_type=jnp.float32)
        lifted = jnp.dot(gathered, up_w, preferred_element_type=jnp.float32)
        hidden = (jax.nn.silu(gated) * lifted).astype(jnp.bfloat16)
        summed = jnp.zeros((slots, D), jnp.float32)
        for portion in range(N_TP):
            piece = jnp.dot(hidden[:, portion * quarter:(portion + 1) * quarter], down_w[portion * quarter:(portion + 1) * quarter], preferred_element_type=jnp.float32).astype(jnp.bfloat16)
            summed = summed + lax.optimization_barrier(piece).astype(jnp.float32)
        return summed.astype(jnp.bfloat16)
    results = lax.map(one_expert, (slot_table, expert_gate, expert_up, expert_down)).reshape(experts * slots, D)
    slot_index = jnp.where(is_kept, chosen * slots + slot_pos, 0).astype(jnp.int32)
    picked = results[slot_index]
    moe_out = lax.optimization_barrier(jnp.sum(jnp.where(is_kept, shares, 0.0)[:, :, None] * picked.astype(jnp.float32), axis=1))
    return (mixer_out, moe_out.astype(jnp.bfloat16))
```

```python
import math
import jax
import jax.numpy as jnp
from jax import lax
from jax.experimental import pallas as pl
from jax.experimental.pallas import tpu as pltpu
from jax.sharding import PartitionSpec as P

DH = 128
GROUPS = 4
BLOCK = 512
ROOT = math.sqrt(DH)
LOG2E = 1.4426950408889634
SCALE = LOG2E / ROOT
QT = 256


def attention_kernel(own_ref, q_ref, w_ref, kv_hbm, out_ref, buf, sems, top, gap, acc):
    own = own_ref[0]
    width = q_ref.shape[1]
    half = width // 2

    def copy(j):
        return pltpu.make_async_copy(kv_hbm.at[j], buf.at[j], sems.at[j])

    def launch(i, carry):
        copy(own - i).start()
        return carry

    lax.fori_loop(0, own + 1, launch, 0)
    top[...] = jnp.full_like(top, -1e30)
    gap[...] = jnp.zeros_like(gap)
    acc[...] = jnp.zeros_like(acc)

    def block(j, masked):
        copy(j).wait()
        gates = buf[j, BLOCK:, :]
        gates = jnp.concatenate([gates, jnp.zeros((DH - 16, 2 * DH), jnp.bfloat16)], axis=0)
        turned = jnp.transpose(gates.astype(jnp.float32)).astype(jnp.bfloat16)
        lane = lax.broadcasted_iota(jnp.int32, turned.shape, 1)
        zero = jnp.zeros_like(turned)
        extra = jnp.concatenate(
            [jnp.where(lane < 8, turned, zero), jnp.where(lane < 8, zero, turned)], axis=0
        )
        keys = jnp.concatenate([buf[j, :BLOCK, :DH], extra], axis=1)
        values = jnp.concatenate(
            [buf[j, c * DH : (c + 1) * DH, DH:] for c in range(BLOCK // DH)]
            , axis=1)
        values = jnp.concatenate([values, jnp.ones((16, BLOCK), jnp.bfloat16)], axis=0)
        if not masked:
            last = buf[j, BLOCK:, 2 * DH - DH :].astype(jnp.float32)
            for h in range(2):
                total = (
                    last[8 + 3 * h : 9 + 3 * h, DH - 1 : DH]
                    + last[9 + 3 * h : 10 + 3 * h, DH - 1 : DH]
                    + last[10 + 3 * h : 11 + 3 * h, DH - 1 : DH]
                )
                gap[:, h * half : (h + 1) * half] = gap[:, h * half : (h + 1) * half] + total
        for t in range(width // QT):
            cols = slice(t * QT, (t + 1) * QT)
            s = jnp.dot(keys, q_ref[:, cols], preferred_element_type=jnp.float32)
            if masked:
                key_at = lax.broadcasted_iota(jnp.int32, s.shape, 0)
                query_at = lax.broadcasted_iota(jnp.int32, s.shape, 1) + (t * QT) % half
                s = jnp.where(key_at <= query_at, s, -1e30)
            old = top[:, cols]
            new = jnp.maximum(old, jnp.max(s, axis=0, keepdims=True) + gap[:, cols])
            top[:, cols] = new
            shift = (new - gap[:, cols]) * SCALE
            p = jnp.exp2(s * SCALE - shift)
            part = jnp.dot(values, p.astype(jnp.bfloat16), preferred_element_type=jnp.float32)
            acc[:, cols] = acc[:, cols] * jnp.exp2((old - new) * SCALE) + part

    block(own, True)

    def step(i, carry):
        block(own - i, False)
        return carry

    lax.fori_loop(1, own + 1, step, 0)
    total = acc[DH : DH + 1, :]
    attended = acc[:DH, :] / total
    stacked = jnp.concatenate([attended[:, :half], attended[:, half:]], axis=0)
    rows = jnp.transpose(stacked).astype(jnp.bfloat16)
    out_ref[...] = jnp.dot(rows, w_ref[...], preferred_element_type=jnp.float32).astype(jnp.bfloat16)


def three(x):
    hi = lax.reduce_precision(x, 8, 7)
    mid = lax.reduce_precision(x - hi, 8, 7)
    return jnp.stack([hi, mid, x - hi - mid], axis=-2).astype(jnp.bfloat16)


def pack(keys, values, gates):
    turned = values.reshape(BLOCK // DH, DH, DH).transpose(0, 2, 1).reshape(BLOCK, DH)
    parts = three(gates * ROOT).reshape(6, 2, 2 * DH).transpose(1, 0, 2)
    parts = jnp.pad(parts, ((0, 0), (0, 2), (0, 0))).reshape(16, 2 * DH)
    return jnp.concatenate([jnp.concatenate([keys, turned], axis=1), parts], axis=0)


def widen(queries):
    rows = queries.shape[0]
    q = queries.reshape(rows, 2, DH).transpose(2, 1, 0).reshape(DH, 2 * rows)
    line = jnp.arange(DH, dtype=jnp.int32)[:, None]
    head = (jnp.arange(2 * rows, dtype=jnp.int32) // rows)[None, :]
    idx = line % 8
    pick = (line < 16) & (idx >= 3 * head) & (idx < 3 * head + 3)
    return jnp.concatenate([q, jnp.where(pick, -1.0, 0.0).astype(jnp.bfloat16)], axis=0)


def attention(own, q, w, kv):
    n = kv.shape[0]
    width = q.shape[1]
    return pl.pallas_call(
        attention_kernel,
        out_shape=jax.ShapeDtypeStruct((width // 2, w.shape[1]), jnp.bfloat16),
        in_specs=[
            pl.BlockSpec(memory_space=pltpu.SMEM),
            pl.BlockSpec(memory_space=pltpu.VMEM),
            pl.BlockSpec(memory_space=pltpu.VMEM),
            pl.BlockSpec(memory_space=pl.ANY),
        ],
        out_specs=pl.BlockSpec(memory_space=pltpu.VMEM),
        scratch_shapes=[
            pltpu.VMEM(kv.shape, jnp.bfloat16),
            pltpu.SemaphoreType.DMA((n,)),
            pltpu.VMEM((1, width), jnp.float32),
            pltpu.VMEM((1, width), jnp.float32),
            pltpu.VMEM((DH + 16, width), jnp.float32),
        ],
        compiler_params=pltpu.CompilerParams(vmem_limit_bytes=40 << 20),
        cost_estimate=pl.CostEstimate(flops=9_000_000_000, bytes_accessed=12_000_000, transcendentals=16_000_000),
    )(own, q, w, kv)


def shift(x, by):
    count = lax.axis_size("tp")
    return lax.ppermute(x, "tp", [(i, (i + by) % count) for i in range(count)])


def rms_scale(row_block, scale_gain):
    values = row_block.astype(jnp.float32)
    return (
        values * lax.rsqrt(jnp.mean(values * values, axis=-1, keepdims=True) + 1e-06) * scale_gain
    )


def expert_part(rows, gate, up, down):
    gated = jnp.dot(rows, gate, preferred_element_type=jnp.float32)
    lifted = jnp.dot(rows, up, preferred_element_type=jnp.float32)
    hidden = (jax.nn.silu(gated) * lifted).astype(jnp.bfloat16)
    return jnp.dot(hidden, down, preferred_element_type=jnp.float32)


def body(
    queries,
    key_rows,
    value_rows,
    forget_logit,
    out_weight,
    out_gain,
    moe_input,
    moe_gain,
    router_group,
    router_expert,
    route_group,
    route_pick,
    expert_gate,
    expert_up,
    expert_down,
):
    tp_count = lax.axis_size("tp")
    ep_count = lax.axis_size("ep")
    tp_index = lax.axis_index("tp")
    ep_index = lax.axis_index("ep")
    group_rows, width_model = moe_input.shape
    own_rows = group_rows // tp_count
    experts = ep_count
    per_group = experts // GROUPS
    capacity = tp_count * own_rows // experts
    slots = experts * capacity

    gate, up, down = expert_gate[0], expert_up[0], expert_down[0]
    half = gate.shape[1] // 2
    left = [shift(w, 1) for w in (gate, up, down)]
    right = [shift(w, -1) for w in (gate, up, down)]
    far_a = [shift(left[0][:, :half], 1), shift(left[1][:, :half], 1), shift(left[2][:half], 1)]
    far_b = [shift(right[0][:, half:], -1), shift(right[1][:, half:], -1), shift(right[2][half:], -1)]

    running = jnp.cumsum(jax.nn.log_sigmoid(forget_logit), axis=1)
    packed = pack(key_rows, value_rows, running)
    gathered = lax.all_gather(packed, "ep", axis=0, tiled=True).reshape(ep_count, *packed.shape)

    own_first = tp_index * own_rows
    own_group = lax.dynamic_slice_in_dim(route_group, own_first, own_rows, 0)
    own_pick = lax.dynamic_slice_in_dim(route_pick, own_first, own_rows, 0)
    chosen = own_group[:, None] * per_group + own_pick
    expert_hit = chosen[:, :, None] == jnp.arange(experts, dtype=jnp.int32)
    usage = jnp.any(expert_hit, axis=1).astype(jnp.bfloat16)
    place = jnp.arange(own_rows, dtype=jnp.int32)
    earlier = (place[None, :] < place[:, None]).astype(jnp.bfloat16)
    before = jnp.dot(earlier, usage, preferred_element_type=jnp.float32).astype(jnp.int32)
    ranks = jnp.sum(jnp.where(expert_hit, before[:, None, :], 0), axis=2)
    target = jnp.where(ranks < capacity, chosen * capacity + ranks, slots)
    normed = rms_scale(
        lax.dynamic_slice_in_dim(moe_input, own_first, own_rows, 0), moe_gain
    ).astype(jnp.bfloat16)
    slot_at = jnp.arange(slots, dtype=jnp.int32)[:, None]
    sent = ((slot_at == target[None, :, 0]) | (slot_at == target[None, :, 1])).astype(jnp.bfloat16)
    outgoing = jnp.dot(sent, normed, preferred_element_type=jnp.float32).astype(jnp.bfloat16)
    arrived = lax.all_to_all(
        outgoing.reshape(experts, capacity, width_model), "ep", split_axis=0, concat_axis=0, tiled=True
    ).reshape(slots, width_model)

    total = expert_part(arrived, gate, up, down)
    total = total + expert_part(arrived, *left)
    total = total + expert_part(arrived, *right)
    total = total + expert_part(arrived, *far_a)
    total = total + expert_part(arrived, *far_b)
    results = total.astype(jnp.bfloat16).reshape(experts, capacity, width_model)
    returned = lax.all_to_all(results, "ep", split_axis=0, concat_axis=0, tiled=True).reshape(
        slots, width_model
    )

    mixer_term = attention(ep_index.reshape(1), widen(queries), out_weight, gathered)
    mixer_summed = lax.psum_scatter(mixer_term, "tp", scatter_dimension=0, tiled=True)
    mixer_out = rms_scale(mixer_summed, out_gain).astype(jnp.bfloat16)

    group_logits = jnp.dot(normed, router_group, preferred_element_type=jnp.float32)
    expert_logits = jnp.dot(normed, router_expert, preferred_element_type=jnp.float32)
    group_top = jnp.max(group_logits, axis=1, keepdims=True)
    group_exp = jnp.exp(group_logits - group_top)
    group_hit = jnp.arange(GROUPS, dtype=jnp.int32)[None, :] == own_group[:, None]
    group_share = jnp.sum(jnp.where(group_hit, group_exp, 0.0), axis=1) / jnp.sum(group_exp, axis=1)
    picked_logits = jnp.sum(jnp.where(expert_hit, expert_logits[:, None, :], 0.0), axis=2)
    shares = group_share[:, None] * jax.nn.sigmoid(picked_logits - picked_logits[:, ::-1])
    column = jnp.arange(slots, dtype=jnp.int32)[None, :]
    weight = jnp.where(column == target[:, :1], shares[:, :1], 0.0) + jnp.where(
        column == target[:, 1:], shares[:, 1:], 0.0
    )
    high = lax.reduce_precision(weight, 8, 7)
    moe_out = jnp.dot(
        high.astype(jnp.bfloat16), returned, preferred_element_type=jnp.float32
    ) + jnp.dot((weight - high).astype(jnp.bfloat16), returned, preferred_element_type=jnp.float32)
    return (mixer_out, moe_out.astype(jnp.bfloat16))


def solution(mesh):
    in_specs = (
        P("ep", "tp"),
        P("ep", "tp"),
        P("ep", "tp"),
        P("tp", "ep"),
        P("tp", None),
        P(),
        P("ep", None),
        P(),
        P(),
        P(),
        P("ep"),
        P("ep", None),
        P("ep", None, "tp"),
        P("ep", None, "tp"),
        P("ep", "tp", None),
    )
    out_specs = (P(("ep", "tp"), None), P(("ep", "tp"), None))
    return jax.shard_map(body, mesh=mesh, in_specs=in_specs, out_specs=out_specs, check_vma=False)
```

```python
import math
import jax
import jax.numpy as jnp
from jax import lax
from jax.experimental import pallas as pl
from jax.experimental.pallas import tpu as pltpu
from jax.sharding import PartitionSpec as P

DH = 128
GROUPS = 4
BLOCK = 512
ROOT = math.sqrt(DH)
LOG2E = 1.4426950408889634
SCALE = LOG2E / ROOT
QT = 256


def attention_kernel(
    own_ref, q_ref, w_ref, kv_hbm, out_ref, buf, sems, even, odd, peak_even, peak_odd, top, gap, acc
):
    own = own_ref[0]
    width = q_ref.shape[1]
    half = width // 2
    tiles = [slice(t * QT, (t + 1) * QT) for t in range(width // QT)]

    def copy(j):
        return pltpu.make_async_copy(kv_hbm.at[j], buf.at[j], sems.at[j])

    def launch(i, carry):
        copy(own - i).start()
        return carry

    lax.fori_loop(0, own + 1, launch, 0)
    top[...] = jnp.full_like(top, -1e30)
    gap[...] = jnp.zeros_like(gap)
    acc[...] = jnp.zeros_like(acc)

    def keys_of(j):
        gates = buf[j, BLOCK:, :]
        gates = jnp.concatenate([gates, jnp.zeros((DH - 16, 2 * DH), jnp.bfloat16)], axis=0)
        turned = jnp.transpose(gates.astype(jnp.float32)).astype(jnp.bfloat16)
        lane = lax.broadcasted_iota(jnp.int32, turned.shape, 1)
        zero = jnp.zeros_like(turned)
        extra = jnp.concatenate(
            [jnp.where(lane < 8, turned, zero), jnp.where(lane < 8, zero, turned)], axis=0
        )
        return jnp.concatenate([buf[j, :BLOCK, :DH], extra], axis=1)

    def values_of(j):
        values = jnp.concatenate(
            [buf[j, c * DH : (c + 1) * DH, DH:] for c in range(BLOCK // DH)], axis=1
        )
        return jnp.concatenate([values, jnp.ones((16, BLOCK), jnp.bfloat16)], axis=0)

    def move_gap(j, alive):
        last = buf[j, BLOCK:, DH:].astype(jnp.float32)
        dead = jnp.where(alive, 0.0, -1e30)
        for h in range(2):
            total = (
                last[8 + 3 * h : 9 + 3 * h, DH - 1 : DH]
                + last[9 + 3 * h : 10 + 3 * h, DH - 1 : DH]
                + last[10 + 3 * h : 11 + 3 * h, DH - 1 : DH]
                + dead
            )
            gap[:, h * half : (h + 1) * half] = gap[:, h * half : (h + 1) * half] + total

    def score(keys, t, into, peak, masked):
        s = jnp.dot(keys, q_ref[:, tiles[t]], preferred_element_type=jnp.float32)
        if masked:
            key_at = lax.broadcasted_iota(jnp.int32, s.shape, 0)
            query_at = lax.broadcasted_iota(jnp.int32, s.shape, 1) + (t * QT) % half
            s = jnp.where(key_at <= query_at, s, -1e30)
        into[:, tiles[t]] = s
        peak[:, tiles[t]] = jnp.max(s, axis=0, keepdims=True)

    def absorb(values, t, held, peak):
        cols = tiles[t]
        old = top[:, cols]
        new = jnp.maximum(old, peak[:, cols] + gap[:, cols])
        top[:, cols] = new
        p = jnp.exp2(held[:, cols] * SCALE - (new - gap[:, cols]) * SCALE)
        part = jnp.dot(values, p.astype(jnp.bfloat16), preferred_element_type=jnp.float32)
        acc[:, cols] = acc[:, cols] * jnp.exp2((old - new) * SCALE) + part

    def phase(now, later, held, held_peak, into, into_peak):
        values = values_of(jnp.maximum(now, 0))
        keys = keys_of(jnp.maximum(later, 0))
        for t in range(len(tiles)):
            score(keys, t, into, into_peak, False)
            absorb(values, t, held, held_peak)
        move_gap(jnp.maximum(later, 0), later >= 0)

    def arrive(j):
        @pl.when(j >= 0)
        def _():
            copy(j).wait()

    copy(own).wait()
    keys = keys_of(own)
    for t in range(len(tiles)):
        score(keys, t, even, peak_even, True)

    def step(i, carry):
        now = own - 2 * i
        arrive(now - 1)
        arrive(now - 2)
        phase(now, now - 1, even, peak_even, odd, peak_odd)
        phase(now - 1, now - 2, odd, peak_odd, even, peak_even)
        return carry

    lax.fori_loop(0, lax.div(own + 2, 2), step, 0)
    total = acc[DH : DH + 1, :]
    attended = acc[:DH, :] / total
    stacked = jnp.concatenate([attended[:, :half], attended[:, half:]], axis=0)
    rows = jnp.transpose(stacked).astype(jnp.bfloat16)
    out_ref[...] = jnp.dot(rows, w_ref[...], preferred_element_type=jnp.float32).astype(jnp.bfloat16)


def three(x):
    hi = lax.reduce_precision(x, 8, 7)
    mid = lax.reduce_precision(x - hi, 8, 7)
    return jnp.stack([hi, mid, x - hi - mid], axis=-2).astype(jnp.bfloat16)


def pack(keys, values, gates):
    turned = values.reshape(BLOCK // DH, DH, DH).transpose(0, 2, 1).reshape(BLOCK, DH)
    parts = three(gates * ROOT).reshape(6, 2, 2 * DH).transpose(1, 0, 2)
    parts = jnp.pad(parts, ((0, 0), (0, 2), (0, 0))).reshape(16, 2 * DH)
    return jnp.concatenate([jnp.concatenate([keys, turned], axis=1), parts], axis=0)


def widen(queries):
    rows = queries.shape[0]
    q = queries.reshape(rows, 2, DH).transpose(2, 1, 0).reshape(DH, 2 * rows)
    line = jnp.arange(DH, dtype=jnp.int32)[:, None]
    head = (jnp.arange(2 * rows, dtype=jnp.int32) // rows)[None, :]
    idx = line % 8
    pick = (line < 16) & (idx >= 3 * head) & (idx < 3 * head + 3)
    return jnp.concatenate([q, jnp.where(pick, -1.0, 0.0).astype(jnp.bfloat16)], axis=0)


def attention(own, q, w, kv):
    n = kv.shape[0]
    width = q.shape[1]
    return pl.pallas_call(
        attention_kernel,
        out_shape=jax.ShapeDtypeStruct((width // 2, w.shape[1]), jnp.bfloat16),
        in_specs=[
            pl.BlockSpec(memory_space=pltpu.SMEM),
            pl.BlockSpec(memory_space=pltpu.VMEM),
            pl.BlockSpec(memory_space=pltpu.VMEM),
            pl.BlockSpec(memory_space=pltpu.HBM),
        ],
        out_specs=pl.BlockSpec(memory_space=pltpu.VMEM),
        scratch_shapes=[
            pltpu.VMEM(kv.shape, jnp.bfloat16),
            pltpu.SemaphoreType.DMA((n,)),
            pltpu.VMEM((BLOCK, width), jnp.float32),
            pltpu.VMEM((BLOCK, width), jnp.float32),
            pltpu.VMEM((1, width), jnp.float32),
            pltpu.VMEM((1, width), jnp.float32),
            pltpu.VMEM((1, width), jnp.float32),
            pltpu.VMEM((1, width), jnp.float32),
            pltpu.VMEM((DH + 16, width), jnp.float32),
        ],
        cost_estimate=pl.CostEstimate(flops=9_000_000_000, bytes_accessed=12_000_000, transcendentals=16_000_000),
    )(own, q, w, kv)


def expert_hidden(x_ref, both, hidden_ref, at):
    rows, ff = x_ref.shape[0], both.shape[1] // 2
    for r in range(0, rows, 256):
        lines = slice(r, r + 256)
        pre = jnp.dot(x_ref[lines, :], both[...], preferred_element_type=jnp.float32)
        gated, lifted = pre[:, :ff], pre[:, ff:]
        hidden_ref[lines, at : at + ff] = (gated * jax.nn.sigmoid(gated) * lifted).astype(jnp.bfloat16)


def column_tiles(width):
    return [slice(n, n + 512) for n in range(0, width, 512)]


def first_kernel(x_hbm, *refs):
    count = (len(refs) - 7) // 3
    weights, (out_hbm, x_ref, both, down, hidden, out, sems) = refs[: 3 * count], refs[3 * count :]
    ff = down.shape[0] // count
    rows = pltpu.make_async_copy(x_hbm, x_ref, sems.at[3 * count])
    rows.start()
    copies = []
    for q in range(count):
        gate, up, low = weights[3 * q : 3 * q + 3]
        pairs = (
            (gate, both.at[q, :, :ff]),
            (up, both.at[q, :, ff:]),
            (low, down.at[q * ff : (q + 1) * ff, :]),
        )
        for k, (src, dst) in enumerate(pairs):
            copies.append(pltpu.make_async_copy(src, dst, sems.at[3 * q + k]))
    for c in copies:
        c.start()
    rows.wait()
    for q in range(count):
        copies[3 * q].wait()
        copies[3 * q + 1].wait()
        expert_hidden(x_ref, both.at[q], hidden, q * ff)
    for q in range(count):
        copies[3 * q + 2].wait()
    stores = []
    for n, cols in enumerate(column_tiles(out.shape[1])):
        out[:, cols] = jnp.dot(hidden[...], down[:, cols], preferred_element_type=jnp.float32)
        stores.append(
            pltpu.make_async_copy(out.at[:, cols], out_hbm.at[:, cols], sems.at[3 * count + 1 + n])
        )
        stores[-1].start()
    for c in stores:
        c.wait()


def first_parts(x, weights):
    rows, width = x.shape
    count, ff = len(weights) // 3, weights[0].shape[1]
    return pl.pallas_call(
        first_kernel,
        out_shape=jax.ShapeDtypeStruct((rows, width), jnp.float32),
        in_specs=[pl.BlockSpec(memory_space=pltpu.HBM)] * (1 + len(weights)),
        out_specs=pl.BlockSpec(memory_space=pltpu.HBM),
        scratch_shapes=[
            pltpu.VMEM((rows, width), jnp.bfloat16),
            pltpu.VMEM((count, width, 2 * ff), jnp.bfloat16),
            pltpu.VMEM((count * ff, width), jnp.bfloat16),
            pltpu.VMEM((rows, count * ff), jnp.bfloat16),
            pltpu.VMEM((rows, width), jnp.float32),
            pltpu.SemaphoreType.DMA((3 * count + 1 + len(column_tiles(width)),)),
        ],
        cost_estimate=pl.CostEstimate(
            flops=count * 6 * rows * width * ff,
            bytes_accessed=count * 6 * width * ff,
            transcendentals=rows * count * ff,
        ),
    )(x, *weights)


def last_kernel(
    x_hbm, part_hbm, gate, up, top_half, bottom_half, out_hbm, x_ref, part, both, down, hidden, out, sems
):
    ff = gate.shape[1]
    pairs = (
        (x_hbm, x_ref),
        (gate, both.at[:, :ff]),
        (up, both.at[:, ff:]),
        (top_half, down.at[: ff // 2, :]),
        (bottom_half, down.at[ff // 2 :, :]),
        (part_hbm, part),
    )
    copies = [pltpu.make_async_copy(src, dst, sems.at[k]) for k, (src, dst) in enumerate(pairs)]
    for c in copies:
        c.start()
    for c in copies[:3]:
        c.wait()
    expert_hidden(x_ref, both, hidden, 0)
    for c in copies[3:]:
        c.wait()
    stores = []
    for n, cols in enumerate(column_tiles(out.shape[1])):
        out[:, cols] = (
            part[:, cols]
            + jnp.dot(hidden[...], down[:, cols], preferred_element_type=jnp.float32)
        ).astype(jnp.bfloat16)
        stores.append(
            pltpu.make_async_copy(out.at[:, cols], out_hbm.at[:, cols], sems.at[len(pairs) + n])
        )
        stores[-1].start()
    for c in stores:
        c.wait()


def last_part(x, part, gate, up, top_half, bottom_half):
    rows, width = x.shape
    ff = gate.shape[1]
    return pl.pallas_call(
        last_kernel,
        out_shape=jax.ShapeDtypeStruct((rows, width), jnp.bfloat16),
        in_specs=[pl.BlockSpec(memory_space=pltpu.HBM)] * 6,
        out_specs=pl.BlockSpec(memory_space=pltpu.HBM),
        scratch_shapes=[
            pltpu.VMEM((rows, width), jnp.bfloat16),
            pltpu.VMEM((rows, width), jnp.float32),
            pltpu.VMEM((width, 2 * ff), jnp.bfloat16),
            pltpu.VMEM((ff, width), jnp.bfloat16),
            pltpu.VMEM((rows, ff), jnp.bfloat16),
            pltpu.VMEM((rows, width), jnp.bfloat16),
            pltpu.SemaphoreType.DMA((6 + len(column_tiles(width)),)),
        ],
        cost_estimate=pl.CostEstimate(
            flops=6 * rows * width * ff, bytes_accessed=6 * width * ff, transcendentals=rows * ff
        ),
    )(x, part, gate, up, top_half, bottom_half)


def shift(x, by):
    count = lax.axis_size("tp")
    return lax.ppermute(x, "tp", [(i, (i + by) % count) for i in range(count)])


def rms_scale(row_block, scale_gain):
    values = row_block.astype(jnp.float32)
    return (
        values * lax.rsqrt(jnp.mean(values * values, axis=-1, keepdims=True) + 1e-06) * scale_gain
    )


def inner(
    queries,
    key_rows,
    value_rows,
    forget_logit,
    out_weight,
    out_gain,
    moe_input,
    moe_gain,
    router_group,
    router_expert,
    route_group,
    route_pick,
    expert_gate,
    expert_up,
    expert_down,
):
    tp_count = lax.axis_size("tp")
    ep_count = lax.axis_size("ep")
    tp_index = lax.axis_index("tp")
    ep_index = lax.axis_index("ep")
    group_rows, width_model = moe_input.shape
    own_rows = group_rows // tp_count
    experts = ep_count
    per_group = experts // GROUPS
    capacity = tp_count * own_rows // experts
    slots = experts * capacity

    gate, up, down = expert_gate[0], expert_up[0], expert_down[0]
    half = gate.shape[1] // 2
    from_left = [shift(w, 1) for w in (gate, down, up)]
    from_right = [shift(w, -1) for w in (up, down, gate)]
    far_gate = shift(from_left[0], 1)
    far_up = shift(from_right[0], -1)
    far_top = shift(from_left[1][:half], 1)
    far_bottom = shift(from_right[1][half:], -1)

    running = jnp.cumsum(jax.nn.log_sigmoid(forget_logit), axis=1)
    packed = pack(key_rows, value_rows, running)
    gathered = lax.all_gather(packed, "ep", axis=0, tiled=True)
    gathered = gathered.reshape(ep_count, *packed.shape)

    own_first = tp_index * own_rows
    own_group = lax.dynamic_slice_in_dim(route_group, own_first, own_rows, 0)
    own_pick = lax.dynamic_slice_in_dim(route_pick, own_first, own_rows, 0)
    chosen = own_group[:, None] * per_group + own_pick
    expert_hit = chosen[:, :, None] == jnp.arange(experts, dtype=jnp.int32)
    usage = jnp.any(expert_hit, axis=1).astype(jnp.bfloat16)
    place = jnp.arange(own_rows, dtype=jnp.int32)
    earlier = (place[None, :] < place[:, None]).astype(jnp.bfloat16)
    before = jnp.dot(earlier, usage, preferred_element_type=jnp.float32).astype(jnp.int32)
    ranks = jnp.sum(jnp.where(expert_hit, before[:, None, :], 0), axis=2)
    target = jnp.where(ranks < capacity, chosen * capacity + ranks, slots)
    normed = rms_scale(
        lax.dynamic_slice_in_dim(moe_input, own_first, own_rows, 0), moe_gain
    ).astype(jnp.bfloat16)
    slot_at = jnp.arange(slots, dtype=jnp.int32)[:, None]
    sent = ((slot_at == target[None, :, 0]) | (slot_at == target[None, :, 1])).astype(jnp.bfloat16)
    outgoing = jnp.dot(sent, normed, preferred_element_type=jnp.float32).astype(jnp.bfloat16)
    outgoing = outgoing.reshape(experts, capacity, width_model)
    arrived = lax.all_to_all(outgoing, "ep", split_axis=0, concat_axis=0, tiled=True)
    arrived = arrived.reshape(slots, width_model)

    part = first_parts(
        arrived,
        (gate, up, down)
        + (from_left[0], from_left[2], from_left[1])
        + (from_right[2], from_right[0], from_right[1]),
    )
    gathered, part = lax.optimization_barrier((gathered, part))
    mixer_term = attention(ep_index.reshape(1), widen(queries), out_weight, gathered)
    part, mixer_term = lax.optimization_barrier((part, mixer_term))
    results = last_part(arrived, part, far_gate, far_up, far_top, far_bottom)
    results = results.reshape(experts, capacity, width_model)
    returned = lax.all_to_all(results, "ep", split_axis=0, concat_axis=0, tiled=True).reshape(
        slots, width_model
    )

    mixer_summed = lax.psum_scatter(mixer_term, "tp", scatter_dimension=0, tiled=True)
    mixer_out = rms_scale(mixer_summed, out_gain).astype(jnp.bfloat16)

    group_logits = jnp.dot(normed, router_group, preferred_element_type=jnp.float32)
    expert_logits = jnp.dot(normed, router_expert, preferred_element_type=jnp.float32)
    group_top = jnp.max(group_logits, axis=1, keepdims=True)
    group_exp = jnp.exp(group_logits - group_top)
    group_hit = jnp.arange(GROUPS, dtype=jnp.int32)[None, :] == own_group[:, None]
    group_share = jnp.sum(jnp.where(group_hit, group_exp, 0.0), axis=1) / jnp.sum(group_exp, axis=1)
    picked_logits = jnp.sum(jnp.where(expert_hit, expert_logits[:, None, :], 0.0), axis=2)
    shares = group_share[:, None] * jax.nn.sigmoid(picked_logits - picked_logits[:, ::-1])
    column = jnp.arange(slots, dtype=jnp.int32)[None, :]
    weight = jnp.where(column == target[:, :1], shares[:, :1], 0.0) + jnp.where(
        column == target[:, 1:], shares[:, 1:], 0.0
    )
    high = lax.reduce_precision(weight, 8, 7)
    moe_out = jnp.dot(
        high.astype(jnp.bfloat16), returned, preferred_element_type=jnp.float32
    ) + jnp.dot((weight - high).astype(jnp.bfloat16), returned, preferred_element_type=jnp.float32)
    return (mixer_out, moe_out.astype(jnp.bfloat16))


def solution(mesh):
    in_specs = (
        P("ep", "tp"),
        P("ep", "tp"),
        P("ep", "tp"),
        P("tp", "ep"),
        P("tp", None),
        P(),
        P("ep", None),
        P(),
        P(),
        P(),
        P("ep"),
        P("ep", None),
        P("ep", None, "tp"),
        P("ep", None, "tp"),
        P("ep", "tp", None),
    )
    out_specs = (P(("ep", "tp"), None), P(("ep", "tp"), None))
    return jax.shard_map(inner, mesh=mesh, in_specs=in_specs, out_specs=out_specs, check_vma=False)
```

```python
import math
import jax
import jax.numpy as jnp
from jax import lax
from jax.experimental import pallas as pl
from jax.experimental.pallas import tpu as pltpu
from jax.sharding import PartitionSpec as P

DH = 128
GROUPS = 4
BLOCK = 512
PLANE = 8
DEPTH = 4
ROOT = math.sqrt(DH)
LOG2E = 1.4426950408889634
SCALE = LOG2E / ROOT
QT = 256


def put_rows(stat, first, row, half):
    for h in range(2):
        rest = row[:, h * half : (h + 1) * half]
        for p in range(3):
            piece = rest.astype(jnp.bfloat16).astype(jnp.float32)
            stat[first + 3 * h + p : first + 3 * h + p + 1, :] = piece
            rest = rest - piece


def attend_kernel(
    pos_ref, q0, q1, q2, q3, kv_hbm, o0, o1, o2, o3,
    kv, raw, sems, wide, keys, values, even, odd, peak_even, peak_odd, top, gap, acc, stat,
):
    own, ahead = pos_ref[0], DEPTH - 1 - pos_ref[1]
    width = wide.shape[2]
    half = width // 2
    tiles = [slice(t * QT, (t + 1) * QT) for t in range(width // QT)]
    arriving = [pltpu.make_async_copy(q, raw.at[s], sems.at[s]) for s, q in enumerate((q0, q1, q2, q3))]
    arriving += [
        pltpu.make_async_copy(kv_hbm.at[b], kv.at[b], sems.at[DEPTH + b]) for b in range(PLANE)
    ]
    for c in arriving:
        c.start()
    top[...] = jnp.full_like(top, -1e30)
    acc[...] = jnp.zeros_like(acc)
    line = lax.broadcasted_iota(jnp.int32, (DH, width), 0)
    head = lax.broadcasted_iota(jnp.int32, (DH, width), 1) // half
    index = line % 8
    pick = (line < 16) & (index >= 3 * head) & (index < 3 * head + 3)
    picks = jnp.where(pick, -1.0, 0.0).astype(jnp.bfloat16)
    for s in range(DEPTH):
        arriving[s].wait()

    def turn(s, carry):
        turned = jnp.transpose(raw[s].astype(jnp.float32)).astype(jnp.bfloat16)
        for h in range(2):
            wide[s, :DH, h * half : (h + 1) * half] = turned[h * DH : (h + 1) * DH, :]
        wide[s, DH:, :] = picks
        return carry

    lax.fori_loop(0, ahead + 1, turn, 0)
    for b in range(PLANE):
        arriving[DEPTH + b].wait()
    sums = jnp.zeros((1, width), jnp.float32)
    first_total = None
    for b in reversed(range(PLANE)):
        gates = kv[b, BLOCK:, :]
        last = gates[:, DH:].astype(jnp.float32)
        total = jnp.concatenate(
            [
                jnp.broadcast_to(
                    last[8 + 3 * h : 9 + 3 * h, DH - 1 : DH]
                    + last[9 + 3 * h : 10 + 3 * h, DH - 1 : DH]
                    + last[10 + 3 * h : 11 + 3 * h, DH - 1 : DH],
                    (1, half),
                )
                for h in range(2)
            ],
            axis=1,
        )
        if b == PLANE - 1:
            first_total = total
        else:
            sums = sums + total
        gap[b] = sums

    def prepare(b, carry):
        gates = kv[b, BLOCK:, :]
        gates = jnp.concatenate([gates, jnp.zeros((DH - 16, 2 * DH), jnp.bfloat16)], axis=0)
        turned = jnp.transpose(gates.astype(jnp.float32)).astype(jnp.bfloat16)
        lane = lax.broadcasted_iota(jnp.int32, turned.shape, 1)
        zero = jnp.zeros_like(turned)
        keys[b, :, :DH] = kv[b, :BLOCK, :DH]
        keys[b, : 2 * DH, DH:] = jnp.where(lane < 8, turned, zero)
        keys[b, 2 * DH :, DH:] = jnp.where(lane < 8, zero, turned)
        for c in range(BLOCK // DH):
            values[b, :DH, c * DH : (c + 1) * DH] = kv[b, c * DH : (c + 1) * DH, DH:]
        values[b, DH:, :] = jnp.ones((16, BLOCK), jnp.bfloat16)
        return carry

    lax.fori_loop(0, PLANE, prepare, 0)
    steps = own + 1 + PLANE * ahead

    def place(n):
        m = jnp.maximum(n - (own + 1), 0)
        mine = n <= own
        s = jnp.where(mine, 0, jnp.minimum(1 + (m >> 3), DEPTH - 1))
        b = jnp.where(mine, own - n, PLANE - 1 - (m & 7))
        return s, b

    def score(s, b, t, into, peak, masked):
        scores = jnp.dot(keys[b], wide[s, :, tiles[t]], preferred_element_type=jnp.float32)
        if masked:
            key_at = lax.broadcasted_iota(jnp.int32, scores.shape, 0)
            query_at = lax.broadcasted_iota(jnp.int32, scores.shape, 1) + (t * QT) % half
            scores = jnp.where(key_at <= query_at, scores, -1e30)
        into[:, tiles[t]] = scores
        peak[:, tiles[t]] = jnp.max(scores, axis=0, keepdims=True)

    def absorb(s, b, dead, t, held, peak):
        cols = tiles[t]
        old = top[s, :, cols]
        shift = gap[b, :, cols] + dead
        new = jnp.maximum(old, peak[:, cols] + shift)
        top[s, :, cols] = new
        p = jnp.exp2(held[:, cols] * SCALE - (new - shift) * SCALE)
        part = jnp.dot(values[b], p.astype(jnp.bfloat16), preferred_element_type=jnp.float32)
        acc[s, :, cols] = acc[s, :, cols] * jnp.exp2((old - new) * SCALE) + part

    def phase(n, held, held_peak, into, into_peak):
        s, b = place(n)
        dead = jnp.where(n < steps, 0.0, -1e30)
        later_s, later_b = place(n + 1)
        for t in range(len(tiles)):
            score(later_s, later_b, t, into, into_peak, False)
            absorb(s, b, dead, t, held, held_peak)

    for t in range(len(tiles)):
        score(0, own, t, even, peak_even, True)

    def step(i, carry):
        phase(2 * i, even, peak_even, odd, peak_odd)
        phase(2 * i + 1, odd, peak_odd, even, peak_even)
        return carry

    lax.fori_loop(0, (steps + 1) >> 1, step, 0)
    for s, out in enumerate((o0, o1, o2, o3)):

        @pl.when(s <= ahead)
        def _():
            weight = acc[s, DH : DH + 1, :]
            mean = acc[s, :DH, :] / weight
            for h in range(2):
                out[h * DH : (h + 1) * DH, :] = mean[:, h * half : (h + 1) * half].astype(jnp.bfloat16)
            level = top[s] * SCALE + jnp.log(weight) * LOG2E
            if s == 0:
                level = level - gap[own] * SCALE
                passed = gap[0] - gap[own]
            else:
                level = level + first_total * SCALE
                passed = gap[0] + first_total
            stat[...] = jnp.zeros_like(stat)
            put_rows(stat, 0, level, half)
            put_rows(stat, 6, passed * SCALE, half)
            out[2 * DH :, :] = stat[...].astype(jnp.bfloat16)


def attend(pos, sets, kv):
    rows = sets[0].shape[0]
    width = 2 * rows
    return pl.pallas_call(
        attend_kernel,
        out_shape=[jax.ShapeDtypeStruct((2 * DH + 16, rows), jnp.bfloat16)] * DEPTH,
        in_specs=[pl.BlockSpec(memory_space=pltpu.SMEM)]
        + [pl.BlockSpec(memory_space=pltpu.HBM)] * (DEPTH + 1),
        out_specs=[pl.BlockSpec(memory_space=pltpu.VMEM)] * DEPTH,
        scratch_shapes=[
            pltpu.VMEM(kv.shape, jnp.bfloat16),
            pltpu.VMEM((DEPTH, rows, 2 * DH), jnp.bfloat16),
            pltpu.SemaphoreType.DMA((DEPTH + PLANE,)),
            pltpu.VMEM((DEPTH, 2 * DH, width), jnp.bfloat16),
            pltpu.VMEM((PLANE, BLOCK, 2 * DH), jnp.bfloat16),
            pltpu.VMEM((PLANE, DH + 16, BLOCK), jnp.bfloat16),
            pltpu.VMEM((BLOCK, width), jnp.float32),
            pltpu.VMEM((BLOCK, width), jnp.float32),
            pltpu.VMEM((1, width), jnp.float32),
            pltpu.VMEM((1, width), jnp.float32),
            pltpu.VMEM((DEPTH, 1, width), jnp.float32),
            pltpu.VMEM((PLANE, 1, width), jnp.float32),
            pltpu.VMEM((DEPTH, DH + 16, width), jnp.float32),
            pltpu.VMEM((16, rows), jnp.float32),
        ],
        cost_estimate=pl.CostEstimate(
            flops=9_000_000_000, bytes_accessed=4_000_000, transcendentals=16_000_000
        ),
    )(pos, *sets, kv)


def merge_kernel(pos_ref, p0, p1, p2, p3, w_ref, out_ref):
    depth = pos_ref[1]
    parts = (p0, p1, p2, p3)

    def read(ref, first):
        stat = ref[2 * DH :, :].astype(jnp.float32)
        return [
            sum(stat[first + 3 * h + p : first + 3 * h + p + 1, :] for p in range(3)) for h in range(2)
        ]

    merged = []
    passed = read(p0, 6)
    levels = [read(p0, 0)]
    for d in range(1, DEPTH):
        own = read(parts[d], 0)
        lost = jnp.where(d <= depth, 0.0, -1e30)
        levels.append([own[h] + passed[h] + lost for h in range(2)])
        more = read(parts[d], 6)
        passed = [passed[h] + more[h] for h in range(2)]
    for h in range(2):
        high = levels[0][h]
        for d in range(1, DEPTH):
            high = jnp.maximum(high, levels[d][h])
        weights = [jnp.exp2(levels[d][h] - high) for d in range(DEPTH)]
        total = weights[0] + weights[1] + weights[2] + weights[3]
        mixed = None
        for d in range(DEPTH):
            term = parts[d][h * DH : (h + 1) * DH, :].astype(jnp.float32) * (weights[d] / total)
            mixed = term if mixed is None else mixed + term
        merged.append(mixed)
    attended = jnp.transpose(jnp.concatenate(merged, axis=0)).astype(jnp.bfloat16)
    for n in range(0, out_ref.shape[1], 512):
        out_ref[:, n : n + 512] = jnp.dot(
            attended, w_ref[:, n : n + 512], preferred_element_type=jnp.float32
        ).astype(jnp.bfloat16)


def merge(pos, parts, w):
    rows = parts[0].shape[1]
    return pl.pallas_call(
        merge_kernel,
        out_shape=jax.ShapeDtypeStruct((rows, w.shape[1]), jnp.bfloat16),
        in_specs=[pl.BlockSpec(memory_space=pltpu.SMEM)]
        + [pl.BlockSpec(memory_space=pltpu.VMEM)] * (DEPTH + 1),
        out_specs=pl.BlockSpec(memory_space=pltpu.VMEM),
        cost_estimate=pl.CostEstimate(
            flops=2 * rows * w.shape[0] * w.shape[1], bytes_accessed=4_000_000, transcendentals=8 * rows
        ),
    )(pos, *parts, w)


def three(x):
    hi = lax.reduce_precision(x, 8, 7)
    mid = lax.reduce_precision(x - hi, 8, 7)
    return jnp.stack([hi, mid, x - hi - mid], axis=-2).astype(jnp.bfloat16)


def pack(keys, values, gates):
    turned = values.reshape(BLOCK // DH, DH, DH).transpose(0, 2, 1).reshape(BLOCK, DH)
    parts = three(gates * ROOT).reshape(6, 2, 2 * DH).transpose(1, 0, 2)
    parts = jnp.pad(parts, ((0, 0), (0, 2), (0, 0))).reshape(16, 2 * DH)
    return jnp.concatenate([jnp.concatenate([keys, turned], axis=1), parts], axis=0)


def expert_hidden(x_ref, both, hidden_ref, at):
    rows, ff = x_ref.shape[0], both.shape[1] // 2
    for r in range(0, rows, 256):
        lines = slice(r, r + 256)
        pre = jnp.dot(x_ref[lines, :], both[...], preferred_element_type=jnp.float32)
        gated, lifted = pre[:, :ff], pre[:, ff:]
        hidden_ref[lines, at : at + ff] = (gated * jax.nn.sigmoid(gated) * lifted).astype(jnp.bfloat16)


def column_tiles(width):
    return [slice(n, n + 512) for n in range(0, width, 512)]


def first_kernel(x_hbm, *refs):
    count = (len(refs) - 7) // 3
    weights, (out_hbm, x_ref, both, down, hidden, out, sems) = refs[: 3 * count], refs[3 * count :]
    ff = down.shape[0] // count
    rows = pltpu.make_async_copy(x_hbm, x_ref, sems.at[3 * count])
    rows.start()
    copies = []
    for q in range(count):
        gate, up, low = weights[3 * q : 3 * q + 3]
        pairs = (
            (gate, both.at[q, :, :ff]),
            (up, both.at[q, :, ff:]),
            (low, down.at[q * ff : (q + 1) * ff, :]),
        )
        for k, (src, dst) in enumerate(pairs):
            copies.append(pltpu.make_async_copy(src, dst, sems.at[3 * q + k]))
    for c in copies:
        c.start()
    rows.wait()
    for q in range(count):
        copies[3 * q].wait()
        copies[3 * q + 1].wait()
        expert_hidden(x_ref, both.at[q], hidden, q * ff)
    for q in range(count):
        copies[3 * q + 2].wait()
    stores = []
    for n, cols in enumerate(column_tiles(out.shape[1])):
        out[:, cols] = jnp.dot(hidden[...], down[:, cols], preferred_element_type=jnp.float32)
        stores.append(
            pltpu.make_async_copy(out.at[:, cols], out_hbm.at[:, cols], sems.at[3 * count + 1 + n])
        )
        stores[-1].start()
    for c in stores:
        c.wait()


def first_parts(x, weights):
    rows, width = x.shape
    count, ff = len(weights) // 3, weights[0].shape[1]
    return pl.pallas_call(
        first_kernel,
        out_shape=jax.ShapeDtypeStruct((rows, width), jnp.float32),
        in_specs=[pl.BlockSpec(memory_space=pltpu.HBM)] * (1 + len(weights)),
        out_specs=pl.BlockSpec(memory_space=pltpu.HBM),
        scratch_shapes=[
            pltpu.VMEM((rows, width), jnp.bfloat16),
            pltpu.VMEM((count, width, 2 * ff), jnp.bfloat16),
            pltpu.VMEM((count * ff, width), jnp.bfloat16),
            pltpu.VMEM((rows, count * ff), jnp.bfloat16),
            pltpu.VMEM((rows, width), jnp.float32),
            pltpu.SemaphoreType.DMA((3 * count + 1 + len(column_tiles(width)),)),
        ],
        cost_estimate=pl.CostEstimate(
            flops=count * 6 * rows * width * ff,
            bytes_accessed=count * 6 * width * ff,
            transcendentals=rows * count * ff,
        ),
    )(x, *weights)


def last_kernel(
    x_hbm, part_hbm, gate, up, top_half, bottom_half, out_hbm, x_ref, part, both, down, hidden, out, sems
):
    ff = gate.shape[1]
    pairs = (
        (x_hbm, x_ref),
        (gate, both.at[:, :ff]),
        (up, both.at[:, ff:]),
        (top_half, down.at[: ff // 2, :]),
        (bottom_half, down.at[ff // 2 :, :]),
        (part_hbm, part),
    )
    copies = [pltpu.make_async_copy(src, dst, sems.at[k]) for k, (src, dst) in enumerate(pairs)]
    for c in copies:
        c.start()
    for c in copies[:3]:
        c.wait()
    expert_hidden(x_ref, both, hidden, 0)
    for c in copies[3:]:
        c.wait()
    stores = []
    for n, cols in enumerate(column_tiles(out.shape[1])):
        out[:, cols] = (
            part[:, cols]
            + jnp.dot(hidden[...], down[:, cols], preferred_element_type=jnp.float32)
        ).astype(jnp.bfloat16)
        stores.append(
            pltpu.make_async_copy(out.at[:, cols], out_hbm.at[:, cols], sems.at[len(pairs) + n])
        )
        stores[-1].start()
    for c in stores:
        c.wait()


def last_part(x, part, gate, up, top_half, bottom_half):
    rows, width = x.shape
    ff = gate.shape[1]
    return pl.pallas_call(
        last_kernel,
        out_shape=jax.ShapeDtypeStruct((rows, width), jnp.bfloat16),
        in_specs=[pl.BlockSpec(memory_space=pltpu.HBM)] * 6,
        out_specs=pl.BlockSpec(memory_space=pltpu.HBM),
        scratch_shapes=[
            pltpu.VMEM((rows, width), jnp.bfloat16),
            pltpu.VMEM((rows, width), jnp.float32),
            pltpu.VMEM((width, 2 * ff), jnp.bfloat16),
            pltpu.VMEM((ff, width), jnp.bfloat16),
            pltpu.VMEM((rows, ff), jnp.bfloat16),
            pltpu.VMEM((rows, width), jnp.bfloat16),
            pltpu.SemaphoreType.DMA((6 + len(column_tiles(width)),)),
        ],
        cost_estimate=pl.CostEstimate(
            flops=6 * rows * width * ff, bytes_accessed=6 * width * ff, transcendentals=rows * ff
        ),
    )(x, part, gate, up, top_half, bottom_half)


def shift(x, by):
    count = lax.axis_size("tp")
    return lax.ppermute(x, "tp", [(i, (i + by) % count) for i in range(count)])


def rms_scale(row_block, scale_gain):
    values = row_block.astype(jnp.float32)
    return (
        values * lax.rsqrt(jnp.mean(values * values, axis=-1, keepdims=True) + 1e-06) * scale_gain
    )


def inner(
    queries,
    key_rows,
    value_rows,
    forget_logit,
    out_weight,
    out_gain,
    moe_input,
    moe_gain,
    router_group,
    router_expert,
    route_group,
    route_pick,
    expert_gate,
    expert_up,
    expert_down,
):
    tp_count = lax.axis_size("tp")
    ep_count = lax.axis_size("ep")
    tp_index = lax.axis_index("tp")
    ep_index = lax.axis_index("ep")
    group_rows, width_model = moe_input.shape
    own_rows = group_rows // tp_count
    experts = ep_count
    per_group = experts // GROUPS
    capacity = tp_count * own_rows // experts
    slots = experts * capacity

    gate, up, down = expert_gate[0], expert_up[0], expert_down[0]
    half = gate.shape[1] // 2
    from_left = [shift(w, 1) for w in (gate, down, up)]
    from_right = [shift(w, -1) for w in (up, down, gate)]
    far_gate = shift(from_left[0], 1)
    far_up = shift(from_right[0], -1)
    far_top = shift(from_left[1][:half], 1)
    far_bottom = shift(from_right[1][half:], -1)

    running = jnp.cumsum(jax.nn.log_sigmoid(forget_logit), axis=1)
    packed = pack(key_rows, value_rows, running)
    planes = [[z * PLANE + i for i in range(PLANE)] for z in range(ep_count // PLANE)]
    gathered = lax.all_gather(packed, "ep", axis=0, tiled=True, axis_index_groups=planes)
    gathered = gathered.reshape(PLANE, *packed.shape)
    place = jnp.stack([ep_index % PLANE, ep_index // PLANE])
    asked = [queries]
    for d in range(1, DEPTH):
        pairs = [(i, i - PLANE * d) for i in range(PLANE * d, ep_count)]
        asked.append(lax.ppermute(queries, "ep", pairs))
    answers = attend(place, asked, gathered)
    told = [answers[0]]
    for d in range(1, DEPTH):
        pairs = [(i, i + PLANE * d) for i in range(ep_count - PLANE * d)]
        told.append(lax.ppermute(answers[d], "ep", pairs))

    own_first = tp_index * own_rows
    own_group = lax.dynamic_slice_in_dim(route_group, own_first, own_rows, 0)
    own_pick = lax.dynamic_slice_in_dim(route_pick, own_first, own_rows, 0)
    chosen = own_group[:, None] * per_group + own_pick
    expert_hit = chosen[:, :, None] == jnp.arange(experts, dtype=jnp.int32)
    usage = jnp.any(expert_hit, axis=1).astype(jnp.bfloat16)
    line = jnp.arange(own_rows, dtype=jnp.int32)
    earlier = (line[None, :] < line[:, None]).astype(jnp.bfloat16)
    before = jnp.dot(earlier, usage, preferred_element_type=jnp.float32).astype(jnp.int32)
    ranks = jnp.sum(jnp.where(expert_hit, before[:, None, :], 0), axis=2)
    target = jnp.where(ranks < capacity, chosen * capacity + ranks, slots)
    normed = rms_scale(
        lax.dynamic_slice_in_dim(moe_input, own_first, own_rows, 0), moe_gain
    ).astype(jnp.bfloat16)
    slot_at = jnp.arange(slots, dtype=jnp.int32)[:, None]
    sent = ((slot_at == target[None, :, 0]) | (slot_at == target[None, :, 1])).astype(jnp.bfloat16)
    outgoing = jnp.dot(sent, normed, preferred_element_type=jnp.float32).astype(jnp.bfloat16)
    outgoing = outgoing.reshape(experts, capacity, width_model)
    arrived = lax.all_to_all(outgoing, "ep", split_axis=0, concat_axis=0, tiled=True)
    arrived = arrived.reshape(slots, width_model)

    part = first_parts(
        arrived,
        (gate, up, down)
        + (from_left[0], from_left[2], from_left[1])
        + (from_right[2], from_right[0], from_right[1]),
    )
    mixer_term = merge(place, told, out_weight)
    results = last_part(arrived, part, far_gate, far_up, far_top, far_bottom)
    results = results.reshape(experts, capacity, width_model)
    returned = lax.all_to_all(results, "ep", split_axis=0, concat_axis=0, tiled=True).reshape(
        slots, width_model
    )

    mixer_summed = lax.psum_scatter(mixer_term, "tp", scatter_dimension=0, tiled=True)
    mixer_out = rms_scale(mixer_summed, out_gain).astype(jnp.bfloat16)

    group_logits = jnp.dot(normed, router_group, preferred_element_type=jnp.float32)
    expert_logits = jnp.dot(normed, router_expert, preferred_element_type=jnp.float32)
    group_top = jnp.max(group_logits, axis=1, keepdims=True)
    group_exp = jnp.exp(group_logits - group_top)
    group_hit = jnp.arange(GROUPS, dtype=jnp.int32)[None, :] == own_group[:, None]
    group_share = jnp.sum(jnp.where(group_hit, group_exp, 0.0), axis=1) / jnp.sum(group_exp, axis=1)
    picked_logits = jnp.sum(jnp.where(expert_hit, expert_logits[:, None, :], 0.0), axis=2)
    shares = group_share[:, None] * jax.nn.sigmoid(picked_logits - picked_logits[:, ::-1])
    column = jnp.arange(slots, dtype=jnp.int32)[None, :]
    weight = jnp.where(column == target[:, :1], shares[:, :1], 0.0) + jnp.where(
        column == target[:, 1:], shares[:, 1:], 0.0
    )
    high = lax.reduce_precision(weight, 8, 7)
    moe_out = jnp.dot(
        high.astype(jnp.bfloat16), returned, preferred_element_type=jnp.float32
    ) + jnp.dot((weight - high).astype(jnp.bfloat16), returned, preferred_element_type=jnp.float32)
    return (mixer_out, moe_out.astype(jnp.bfloat16))


def solution(mesh):
    in_specs = (
        P("ep", "tp"),
        P("ep", "tp"),
        P("ep", "tp"),
        P("tp", "ep"),
        P("tp", None),
        P(),
        P("ep", None),
        P(),
        P(),
        P(),
        P("ep"),
        P("ep", None),
        P("ep", None, "tp"),
        P("ep", None, "tp"),
        P("ep", "tp", None),
    )
    out_specs = (P(("ep", "tp"), None), P(("ep", "tp"), None))
    return jax.shard_map(inner, mesh=mesh, in_specs=in_specs, out_specs=out_specs, check_vma=False)
```

```python
import math
import jax
import jax.numpy as jnp
from jax import lax
from jax.experimental import pallas as pl
from jax.experimental.pallas import tpu as pltpu
from jax.sharding import PartitionSpec as P

DH = 128
GROUPS = 4
BLOCK = 512
PLANE = 8
DEPTH = 4
ROOT = math.sqrt(DH)
LOG2E = 1.4426950408889634
SCALE = LOG2E / ROOT
QT = 256


def put_rows(stat, first, row, half):
    for h in range(2):
        rest = row[:, h * half : (h + 1) * half]
        for p in range(3):
            piece = rest.astype(jnp.bfloat16).astype(jnp.float32)
            stat[first + 3 * h + p : first + 3 * h + p + 1, :] = piece
            rest = rest - piece


def attend_kernel(
    pos_ref, q0, q1, q2, q3, kv_hbm, o0, o1, o2, o3,
    kv, raw, sems, wide, keys, values, even, odd, peak_even, peak_odd, top, gap, acc, stat,
):
    own, ahead = pos_ref[0], DEPTH - 1 - pos_ref[1]
    width = wide.shape[2]
    half = width // 2
    tiles = [slice(t * QT, (t + 1) * QT) for t in range(width // QT)]
    arriving = [pltpu.make_async_copy(q, raw.at[s], sems.at[s]) for s, q in enumerate((q0, q1, q2, q3))]
    arriving += [
        pltpu.make_async_copy(kv_hbm.at[b], kv.at[b], sems.at[DEPTH + b]) for b in range(PLANE)
    ]
    for c in arriving:
        c.start()
    top[...] = jnp.full_like(top, -1e30)
    acc[...] = jnp.zeros_like(acc)
    line = lax.broadcasted_iota(jnp.int32, (DH, width), 0)
    head = lax.broadcasted_iota(jnp.int32, (DH, width), 1) // half
    index = line % 8
    pick = (line < 16) & (index >= 3 * head) & (index < 3 * head + 3)
    picks = jnp.where(pick, -1.0, 0.0).astype(jnp.bfloat16)
    for s in range(DEPTH):
        arriving[s].wait()

    def turn(s, carry):
        turned = jnp.transpose(raw[s].astype(jnp.float32)).astype(jnp.bfloat16)
        for h in range(2):
            wide[s, :DH, h * half : (h + 1) * half] = turned[h * DH : (h + 1) * DH, :]
        wide[s, DH:, :] = picks
        return carry

    lax.fori_loop(0, ahead + 1, turn, 0)
    for b in range(PLANE):
        arriving[DEPTH + b].wait()
    sums = jnp.zeros((1, width), jnp.float32)
    first_total = None
    for b in reversed(range(PLANE)):
        gates = kv[b, BLOCK:, :]
        last = gates[:, DH:].astype(jnp.float32)
        total = jnp.concatenate(
            [
                jnp.broadcast_to(
                    last[8 + 3 * h : 9 + 3 * h, DH - 1 : DH]
                    + last[9 + 3 * h : 10 + 3 * h, DH - 1 : DH]
                    + last[10 + 3 * h : 11 + 3 * h, DH - 1 : DH],
                    (1, half),
                )
                for h in range(2)
            ],
            axis=1,
        )
        if b == PLANE - 1:
            first_total = total
        else:
            sums = sums + total
        gap[b] = sums

    def prepare(b, carry):
        gates = kv[b, BLOCK:, :]
        gates = jnp.concatenate([gates, jnp.zeros((DH - 16, 2 * DH), jnp.bfloat16)], axis=0)
        turned = jnp.transpose(gates.astype(jnp.float32)).astype(jnp.bfloat16)
        lane = lax.broadcasted_iota(jnp.int32, turned.shape, 1)
        zero = jnp.zeros_like(turned)
        keys[b, :, :DH] = kv[b, :BLOCK, :DH]
        keys[b, : 2 * DH, DH:] = jnp.where(lane < 8, turned, zero)
        keys[b, 2 * DH :, DH:] = jnp.where(lane < 8, zero, turned)
        for c in range(BLOCK // DH):
            values[b, :DH, c * DH : (c + 1) * DH] = kv[b, c * DH : (c + 1) * DH, DH:]
        values[b, DH:, :] = jnp.ones((16, BLOCK), jnp.bfloat16)
        return carry

    lax.fori_loop(0, PLANE, prepare, 0)
    steps = own + 1 + PLANE * ahead

    def place(n):
        m = jnp.maximum(n - (own + 1), 0)
        mine = n <= own
        s = jnp.where(mine, 0, jnp.minimum(1 + (m >> 3), DEPTH - 1))
        b = jnp.where(mine, own - n, PLANE - 1 - (m & 7))
        return s, b

    def score(s, b, t, into, peak, masked):
        scores = jnp.dot(keys[b], wide[s, :, tiles[t]], preferred_element_type=jnp.float32)
        if masked:
            key_at = lax.broadcasted_iota(jnp.int32, scores.shape, 0)
            query_at = lax.broadcasted_iota(jnp.int32, scores.shape, 1) + (t * QT) % half
            scores = jnp.where(key_at <= query_at, scores, -1e30)
        into[:, tiles[t]] = scores
        peak[:, tiles[t]] = jnp.max(scores, axis=0, keepdims=True)

    def absorb(s, b, dead, t, held, peak):
        cols = tiles[t]
        old = top[s, :, cols]
        shift = gap[b, :, cols] + dead
        new = jnp.maximum(old, peak[:, cols] + shift)
        top[s, :, cols] = new
        p = jnp.exp2(held[:, cols] * SCALE - (new - shift) * SCALE)
        part = jnp.dot(values[b], p.astype(jnp.bfloat16), preferred_element_type=jnp.float32)
        acc[s, :, cols] = acc[s, :, cols] * jnp.exp2((old - new) * SCALE) + part

    def phase(n, held, held_peak, into, into_peak):
        s, b = place(n)
        dead = jnp.where(n < steps, 0.0, -1e30)
        later_s, later_b = place(n + 1)
        for t in range(len(tiles)):
            score(later_s, later_b, t, into, into_peak, False)
            absorb(s, b, dead, t, held, held_peak)

    for t in range(len(tiles)):
        score(0, own, t, even, peak_even, True)

    def step(i, carry):
        phase(2 * i, even, peak_even, odd, peak_odd)
        phase(2 * i + 1, odd, peak_odd, even, peak_even)
        return carry

    lax.fori_loop(0, (steps + 1) >> 1, step, 0)
    for s, out in enumerate((o0, o1, o2, o3)):

        @pl.when(s <= ahead)
        def _():
            weight = acc[s, DH : DH + 1, :]
            mean = acc[s, :DH, :] / weight
            for h in range(2):
                out[h * DH : (h + 1) * DH, :] = mean[:, h * half : (h + 1) * half].astype(jnp.bfloat16)
            level = top[s] * SCALE + jnp.log(weight) * LOG2E
            if s == 0:
                level = level - gap[own] * SCALE
                passed = gap[0] - gap[own]
            else:
                level = level + first_total * SCALE
                passed = gap[0] + first_total
            stat[...] = jnp.zeros_like(stat)
            put_rows(stat, 0, level, half)
            put_rows(stat, 6, passed * SCALE, half)
            out[2 * DH :, :] = stat[...].astype(jnp.bfloat16)


def attend(pos, sets, kv):
    rows = sets[0].shape[0]
    width = 2 * rows
    return pl.pallas_call(
        attend_kernel,
        out_shape=[jax.ShapeDtypeStruct((2 * DH + 16, rows), jnp.bfloat16)] * DEPTH,
        in_specs=[pl.BlockSpec(memory_space=pltpu.SMEM)]
        + [pl.BlockSpec(memory_space=pltpu.HBM)] * (DEPTH + 1),
        out_specs=[pl.BlockSpec(memory_space=pltpu.VMEM)] * DEPTH,
        scratch_shapes=[
            pltpu.VMEM(kv.shape, jnp.bfloat16),
            pltpu.VMEM((DEPTH, rows, 2 * DH), jnp.bfloat16),
            pltpu.SemaphoreType.DMA((DEPTH + PLANE,)),
            pltpu.VMEM((DEPTH, 2 * DH, width), jnp.bfloat16),
            pltpu.VMEM((PLANE, BLOCK, 2 * DH), jnp.bfloat16),
            pltpu.VMEM((PLANE, DH + 16, BLOCK), jnp.bfloat16),
            pltpu.VMEM((BLOCK, width), jnp.float32),
            pltpu.VMEM((BLOCK, width), jnp.float32),
            pltpu.VMEM((1, width), jnp.float32),
            pltpu.VMEM((1, width), jnp.float32),
            pltpu.VMEM((DEPTH, 1, width), jnp.float32),
            pltpu.VMEM((PLANE, 1, width), jnp.float32),
            pltpu.VMEM((DEPTH, DH + 16, width), jnp.float32),
            pltpu.VMEM((16, rows), jnp.float32),
        ],
        cost_estimate=pl.CostEstimate(
            flops=9_000_000_000, bytes_accessed=4_000_000, transcendentals=16_000_000
        ),
    )(pos, *sets, kv)


def merge_kernel(pos_ref, p0, p1, p2, p3, w_ref, out_ref):
    depth = pos_ref[1]
    parts = (p0, p1, p2, p3)

    def read(ref, first):
        stat = ref[2 * DH :, :].astype(jnp.float32)
        return [
            sum(stat[first + 3 * h + p : first + 3 * h + p + 1, :] for p in range(3)) for h in range(2)
        ]

    merged = []
    passed = read(p0, 6)
    levels = [read(p0, 0)]
    for d in range(1, DEPTH):
        own = read(parts[d], 0)
        lost = jnp.where(d <= depth, 0.0, -1e30)
        levels.append([own[h] + passed[h] + lost for h in range(2)])
        more = read(parts[d], 6)
        passed = [passed[h] + more[h] for h in range(2)]
    for h in range(2):
        high = levels[0][h]
        for d in range(1, DEPTH):
            high = jnp.maximum(high, levels[d][h])
        weights = [jnp.exp2(levels[d][h] - high) for d in range(DEPTH)]
        total = weights[0] + weights[1] + weights[2] + weights[3]
        mixed = None
        for d in range(DEPTH):
            term = parts[d][h * DH : (h + 1) * DH, :].astype(jnp.float32) * (weights[d] / total)
            mixed = term if mixed is None else mixed + term
        merged.append(mixed)
    attended = jnp.transpose(jnp.concatenate(merged, axis=0)).astype(jnp.bfloat16)
    for n in range(0, out_ref.shape[1], 512):
        out_ref[:, n : n + 512] = jnp.dot(
            attended, w_ref[:, n : n + 512], preferred_element_type=jnp.float32
        ).astype(jnp.bfloat16)


def merge(pos, parts, w):
    rows = parts[0].shape[1]
    return pl.pallas_call(
        merge_kernel,
        out_shape=jax.ShapeDtypeStruct((rows, w.shape[1]), jnp.bfloat16),
        in_specs=[pl.BlockSpec(memory_space=pltpu.SMEM)]
        + [pl.BlockSpec(memory_space=pltpu.VMEM)] * (DEPTH + 1),
        out_specs=pl.BlockSpec(memory_space=pltpu.VMEM),
        cost_estimate=pl.CostEstimate(
            flops=2 * rows * w.shape[0] * w.shape[1], bytes_accessed=4_000_000, transcendentals=8 * rows
        ),
    )(pos, *parts, w)


def three(x):
    hi = lax.reduce_precision(x, 8, 7)
    mid = lax.reduce_precision(x - hi, 8, 7)
    return jnp.stack([hi, mid, x - hi - mid], axis=-2).astype(jnp.bfloat16)


def pack(keys, values, gates):
    turned = values.reshape(BLOCK // DH, DH, DH).transpose(0, 2, 1).reshape(BLOCK, DH)
    parts = three(gates * ROOT).reshape(6, 2, 2 * DH).transpose(1, 0, 2)
    parts = jnp.pad(parts, ((0, 0), (0, 2), (0, 0))).reshape(16, 2 * DH)
    return jnp.concatenate([jnp.concatenate([keys, turned], axis=1), parts], axis=0)


def expert_hidden(x_ref, both, hidden_ref, at):
    rows, ff = x_ref.shape[0], both.shape[1] // 2
    for r in range(0, rows, 256):
        lines = slice(r, r + 256)
        pre = jnp.dot(x_ref[lines, :], both[...], preferred_element_type=jnp.float32)
        gated, lifted = pre[:, :ff], pre[:, ff:]
        hidden_ref[lines, at : at + ff] = (gated * jax.nn.sigmoid(gated) * lifted).astype(jnp.bfloat16)


def column_tiles(width):
    return [slice(n, n + 512) for n in range(0, width, 512)]


def first_kernel(x_hbm, *refs):
    count = (len(refs) - 7) // 4
    weights, (out_hbm, x_ref, both, down, hidden, out, sems) = refs[: 4 * count], refs[4 * count :]
    ff = down.shape[0] // count
    rows = pltpu.make_async_copy(x_hbm, x_ref, sems.at[4 * count])
    rows.start()
    copies = []
    for q in range(count):
        gate, up, upper, lower = weights[4 * q : 4 * q + 4]
        middle = q * ff + ff // 2
        pairs = (
            (gate, both.at[q, :, :ff]),
            (up, both.at[q, :, ff:]),
            (upper, down.at[q * ff : middle, :]),
            (lower, down.at[middle : (q + 1) * ff, :]),
        )
        for k, (src, dst) in enumerate(pairs):
            copies.append(pltpu.make_async_copy(src, dst, sems.at[4 * q + k]))
    for c in copies:
        c.start()
    rows.wait()
    for q in range(count):
        copies[4 * q].wait()
        copies[4 * q + 1].wait()
        expert_hidden(x_ref, both.at[q], hidden, q * ff)
    for q in range(count):
        copies[4 * q + 2].wait()
        copies[4 * q + 3].wait()
    stores = []
    for n, cols in enumerate(column_tiles(out.shape[1])):
        out[:, cols] = jnp.dot(hidden[...], down[:, cols], preferred_element_type=jnp.float32)
        stores.append(
            pltpu.make_async_copy(out.at[:, cols], out_hbm.at[:, cols], sems.at[4 * count + 1 + n])
        )
        stores[-1].start()
    for c in stores:
        c.wait()


def first_parts(x, weights):
    rows, width = x.shape
    count, ff = len(weights) // 4, weights[0].shape[1]
    return pl.pallas_call(
        first_kernel,
        out_shape=jax.ShapeDtypeStruct((rows, width), jnp.float32),
        in_specs=[pl.BlockSpec(memory_space=pltpu.HBM)] * (1 + len(weights)),
        out_specs=pl.BlockSpec(memory_space=pltpu.HBM),
        scratch_shapes=[
            pltpu.VMEM((rows, width), jnp.bfloat16),
            pltpu.VMEM((count, width, 2 * ff), jnp.bfloat16),
            pltpu.VMEM((count * ff, width), jnp.bfloat16),
            pltpu.VMEM((rows, count * ff), jnp.bfloat16),
            pltpu.VMEM((rows, width), jnp.float32),
            pltpu.SemaphoreType.DMA((4 * count + 1 + len(column_tiles(width)),)),
        ],
        cost_estimate=pl.CostEstimate(
            flops=count * 6 * rows * width * ff,
            bytes_accessed=count * 6 * width * ff,
            transcendentals=rows * count * ff,
        ),
    )(x, *weights)


def last_kernel(
    x_hbm, part_hbm, gate, up, top_half, bottom_half, out_hbm, x_ref, part, both, down, hidden, out, sems
):
    ff = gate.shape[1]
    pairs = (
        (x_hbm, x_ref),
        (gate, both.at[:, :ff]),
        (up, both.at[:, ff:]),
        (top_half, down.at[: ff // 2, :]),
        (bottom_half, down.at[ff // 2 :, :]),
        (part_hbm, part),
    )
    copies = [pltpu.make_async_copy(src, dst, sems.at[k]) for k, (src, dst) in enumerate(pairs)]
    for c in copies:
        c.start()
    for c in copies[:3]:
        c.wait()
    expert_hidden(x_ref, both, hidden, 0)
    for c in copies[3:]:
        c.wait()
    stores = []
    for n, cols in enumerate(column_tiles(out.shape[1])):
        out[:, cols] = (
            part[:, cols]
            + jnp.dot(hidden[...], down[:, cols], preferred_element_type=jnp.float32)
        ).astype(jnp.bfloat16)
        stores.append(
            pltpu.make_async_copy(out.at[:, cols], out_hbm.at[:, cols], sems.at[len(pairs) + n])
        )
        stores[-1].start()
    for c in stores:
        c.wait()


def last_part(x, part, gate, up, top_half, bottom_half):
    rows, width = x.shape
    ff = gate.shape[1]
    return pl.pallas_call(
        last_kernel,
        out_shape=jax.ShapeDtypeStruct((rows, width), jnp.bfloat16),
        in_specs=[pl.BlockSpec(memory_space=pltpu.HBM)] * 6,
        out_specs=pl.BlockSpec(memory_space=pltpu.HBM),
        scratch_shapes=[
            pltpu.VMEM((rows, width), jnp.bfloat16),
            pltpu.VMEM((rows, width), jnp.float32),
            pltpu.VMEM((width, 2 * ff), jnp.bfloat16),
            pltpu.VMEM((ff, width), jnp.bfloat16),
            pltpu.VMEM((rows, ff), jnp.bfloat16),
            pltpu.VMEM((rows, width), jnp.bfloat16),
            pltpu.SemaphoreType.DMA((6 + len(column_tiles(width)),)),
        ],
        cost_estimate=pl.CostEstimate(
            flops=6 * rows * width * ff, bytes_accessed=6 * width * ff, transcendentals=rows * ff
        ),
    )(x, part, gate, up, top_half, bottom_half)


def shift(x, by):
    count = lax.axis_size("tp")
    return lax.ppermute(x, "tp", [(i, (i + by) % count) for i in range(count)])


def rms_scale(row_block, scale_gain):
    values = row_block.astype(jnp.float32)
    return (
        values * lax.rsqrt(jnp.mean(values * values, axis=-1, keepdims=True) + 1e-06) * scale_gain
    )


def inner(
    queries,
    key_rows,
    value_rows,
    forget_logit,
    out_weight,
    out_gain,
    moe_input,
    moe_gain,
    router_group,
    router_expert,
    route_group,
    route_pick,
    expert_gate,
    expert_up,
    expert_down,
):
    tp_count = lax.axis_size("tp")
    ep_count = lax.axis_size("ep")
    tp_index = lax.axis_index("tp")
    ep_index = lax.axis_index("ep")
    group_rows, width_model = moe_input.shape
    own_rows = group_rows // tp_count
    experts = ep_count
    per_group = experts // GROUPS
    capacity = tp_count * own_rows // experts
    slots = experts * capacity

    gate, up, down = expert_gate[0], expert_up[0], expert_down[0]
    half = gate.shape[1] // 2
    upper, lower = down[:half], down[half:]
    own = {"gate": gate, "upper": upper, "up": up, "lower": lower}
    first, second = ("gate", "upper"), ("up", "lower")
    left = {n: shift(own[n], 1) for n in first + second}
    right = {n: shift(own[n], -1) for n in second + first}
    far = {n: shift(left[n], 1) for n in first}
    far |= {n: shift(right[n], -1) for n in second}
    names = ("gate", "up", "upper", "lower")

    running = jnp.cumsum(jax.nn.log_sigmoid(forget_logit), axis=1)
    packed = pack(key_rows, value_rows, running)
    planes = [[z * PLANE + i for i in range(PLANE)] for z in range(ep_count // PLANE)]
    gathered = lax.all_gather(packed, "ep", axis=0, tiled=True, axis_index_groups=planes)
    gathered = gathered.reshape(PLANE, *packed.shape)
    place = jnp.stack([ep_index % PLANE, ep_index // PLANE])
    asked = [queries]
    for d in range(1, DEPTH):
        pairs = [(i, i - PLANE * d) for i in range(PLANE * d, ep_count)]
        asked.append(lax.ppermute(queries, "ep", pairs))
    answers = attend(place, asked, gathered)
    told = [answers[0]]
    for d in range(1, DEPTH):
        pairs = [(i, i + PLANE * d) for i in range(ep_count - PLANE * d)]
        told.append(lax.ppermute(answers[d], "ep", pairs))

    own_first = tp_index * own_rows
    own_group = lax.dynamic_slice_in_dim(route_group, own_first, own_rows, 0)
    own_pick = lax.dynamic_slice_in_dim(route_pick, own_first, own_rows, 0)
    chosen = own_group[:, None] * per_group + own_pick
    expert_hit = chosen[:, :, None] == jnp.arange(experts, dtype=jnp.int32)
    usage = jnp.any(expert_hit, axis=1).astype(jnp.bfloat16)
    line = jnp.arange(own_rows, dtype=jnp.int32)
    earlier = (line[None, :] < line[:, None]).astype(jnp.bfloat16)
    before = jnp.dot(earlier, usage, preferred_element_type=jnp.float32).astype(jnp.int32)
    ranks = jnp.sum(jnp.where(expert_hit, before[:, None, :], 0), axis=2)
    target = jnp.where(ranks < capacity, chosen * capacity + ranks, slots)
    normed = rms_scale(
        lax.dynamic_slice_in_dim(moe_input, own_first, own_rows, 0), moe_gain
    ).astype(jnp.bfloat16)
    slot_at = jnp.arange(slots, dtype=jnp.int32)[:, None]
    sent = ((slot_at == target[None, :, 0]) | (slot_at == target[None, :, 1])).astype(jnp.bfloat16)
    outgoing = jnp.dot(sent, normed, preferred_element_type=jnp.float32).astype(jnp.bfloat16)
    outgoing = outgoing.reshape(experts, capacity, width_model)
    arrived = lax.all_to_all(outgoing, "ep", split_axis=0, concat_axis=0, tiled=True)
    arrived = arrived.reshape(slots, width_model)

    part = first_parts(arrived, [q[n] for q in (own, left, right) for n in names])
    results = last_part(arrived, part, *[far[n] for n in names])
    results, told[0] = lax.optimization_barrier((results, told[0]))
    mixer_term = merge(place, told, out_weight)
    results = results.reshape(experts, capacity, width_model)
    returned = lax.all_to_all(results, "ep", split_axis=0, concat_axis=0, tiled=True)
    returned = returned.reshape(slots, width_model)

    mixer_summed = lax.psum_scatter(mixer_term, "tp", scatter_dimension=0, tiled=True)
    mixer_out = rms_scale(mixer_summed, out_gain).astype(jnp.bfloat16)

    group_logits = jnp.dot(normed, router_group, preferred_element_type=jnp.float32)
    expert_logits = jnp.dot(normed, router_expert, preferred_element_type=jnp.float32)
    group_top = jnp.max(group_logits, axis=1, keepdims=True)
    group_exp = jnp.exp(group_logits - group_top)
    group_hit = jnp.arange(GROUPS, dtype=jnp.int32)[None, :] == own_group[:, None]
    group_share = jnp.sum(jnp.where(group_hit, group_exp, 0.0), axis=1) / jnp.sum(group_exp, axis=1)
    picked_logits = jnp.sum(jnp.where(expert_hit, expert_logits[:, None, :], 0.0), axis=2)
    shares = group_share[:, None] * jax.nn.sigmoid(picked_logits - picked_logits[:, ::-1])
    column = jnp.arange(slots, dtype=jnp.int32)[None, :]
    weight = jnp.where(column == target[:, :1], shares[:, :1], 0.0) + jnp.where(
        column == target[:, 1:], shares[:, 1:], 0.0
    )
    high = lax.reduce_precision(weight, 8, 7)
    moe_out = jnp.dot(
        high.astype(jnp.bfloat16), returned, preferred_element_type=jnp.float32
    ) + jnp.dot((weight - high).astype(jnp.bfloat16), returned, preferred_element_type=jnp.float32)
    return (mixer_out, moe_out.astype(jnp.bfloat16))


def solution(mesh):
    in_specs = (
        P("ep", "tp"),
        P("ep", "tp"),
        P("ep", "tp"),
        P("tp", "ep"),
        P("tp", None),
        P(),
        P("ep", None),
        P(),
        P(),
        P(),
        P("ep"),
        P("ep", None),
        P("ep", None, "tp"),
        P("ep", None, "tp"),
        P("ep", "tp", None),
    )
    out_specs = (P(("ep", "tp"), None), P(("ep", "tp"), None))
    return jax.shard_map(inner, mesh=mesh, in_specs=in_specs, out_specs=out_specs, check_vma=False)
```

```python
import functools
import math
import jax
import jax.numpy as jnp
from jax import lax
from jax.experimental import pallas as pl
from jax.experimental.pallas import tpu as pltpu
from jax.sharding import PartitionSpec as P

DH = 128
GROUPS = 4
BLOCK = 512
PLANE = 8
DEPTH = 4
ROOT = math.sqrt(DH)
LOG2E = 1.4426950408889634
SCALE = LOG2E / ROOT
QT = 256


def put_rows(stat, first, row, half):
    for h in range(2):
        rest = row[:, h * half : (h + 1) * half]
        for p in range(3):
            piece = rest.astype(jnp.bfloat16).astype(jnp.float32)
            stat[first + 3 * h + p : first + 3 * h + p + 1, :] = piece
            rest = rest - piece


def attend_kernel(
    pos_ref, q0, q1, q2, q3, kv_hbm, o0, o1, o2, o3,
    kv, raw, sems, wide, keys, values, even, odd, peak_even, peak_odd, top, gap, acc, stat,
):
    own, ahead = pos_ref[0], DEPTH - 1 - pos_ref[1]
    width = wide.shape[2]
    half = width // 2
    tiles = [slice(t * QT, (t + 1) * QT) for t in range(width // QT)]
    arriving = [pltpu.make_async_copy(q, raw.at[s], sems.at[s]) for s, q in enumerate((q0, q1, q2, q3))]
    arriving += [
        pltpu.make_async_copy(kv_hbm.at[b], kv.at[b], sems.at[DEPTH + b]) for b in range(PLANE)
    ]
    for c in arriving:
        c.start()
    top[...] = jnp.full_like(top, -1e30)
    acc[...] = jnp.zeros_like(acc)
    line = lax.broadcasted_iota(jnp.int32, (DH, width), 0)
    head = lax.broadcasted_iota(jnp.int32, (DH, width), 1) // half
    index = line % 8
    pick = (line < 16) & (index >= 3 * head) & (index < 3 * head + 3)
    picks = jnp.where(pick, -1.0, 0.0).astype(jnp.bfloat16)
    for s in range(DEPTH):
        arriving[s].wait()

    def turn(s, carry):
        turned = jnp.transpose(raw[s].astype(jnp.float32)).astype(jnp.bfloat16)
        for h in range(2):
            wide[s, :DH, h * half : (h + 1) * half] = turned[h * DH : (h + 1) * DH, :]
        wide[s, DH:, :] = picks
        return carry

    lax.fori_loop(0, ahead + 1, turn, 0)
    for b in range(PLANE):
        arriving[DEPTH + b].wait()
    sums = jnp.zeros((1, width), jnp.float32)
    first_total = None
    for b in reversed(range(PLANE)):
        gates = kv[b, BLOCK:, :]
        last = gates[:, DH:].astype(jnp.float32)
        total = jnp.concatenate(
            [
                jnp.broadcast_to(
                    last[8 + 3 * h : 9 + 3 * h, DH - 1 : DH]
                    + last[9 + 3 * h : 10 + 3 * h, DH - 1 : DH]
                    + last[10 + 3 * h : 11 + 3 * h, DH - 1 : DH],
                    (1, half),
                )
                for h in range(2)
            ],
            axis=1,
        )
        if b == PLANE - 1:
            first_total = total
        else:
            sums = sums + total
        gap[b] = sums

    def prepare(b, carry):
        gates = kv[b, BLOCK:, :]
        gates = jnp.concatenate([gates, jnp.zeros((DH - 16, 2 * DH), jnp.bfloat16)], axis=0)
        turned = jnp.transpose(gates.astype(jnp.float32)).astype(jnp.bfloat16)
        lane = lax.broadcasted_iota(jnp.int32, turned.shape, 1)
        zero = jnp.zeros_like(turned)
        keys[b, :, :DH] = kv[b, :BLOCK, :DH]
        keys[b, : 2 * DH, DH:] = jnp.where(lane < 8, turned, zero)
        keys[b, 2 * DH :, DH:] = jnp.where(lane < 8, zero, turned)
        for c in range(BLOCK // DH):
            values[b, :DH, c * DH : (c + 1) * DH] = kv[b, c * DH : (c + 1) * DH, DH:]
        values[b, DH:, :] = jnp.ones((16, BLOCK), jnp.bfloat16)
        return carry

    lax.fori_loop(0, PLANE, prepare, 0)
    steps = own + 1 + PLANE * ahead

    def place(n):
        m = jnp.maximum(n - (own + 1), 0)
        mine = n <= own
        s = jnp.where(mine, 0, jnp.minimum(1 + (m >> 3), DEPTH - 1))
        b = jnp.where(mine, own - n, PLANE - 1 - (m & 7))
        return s, b

    def score(s, b, t, into, peak, masked):
        scores = jnp.dot(keys[b], wide[s, :, tiles[t]], preferred_element_type=jnp.float32)
        if masked:
            key_at = lax.broadcasted_iota(jnp.int32, scores.shape, 0)
            query_at = lax.broadcasted_iota(jnp.int32, scores.shape, 1) + (t * QT) % half
            scores = jnp.where(key_at <= query_at, scores, -1e30)
        into[:, tiles[t]] = scores
        peak[:, tiles[t]] = jnp.max(scores, axis=0, keepdims=True)

    def absorb(s, b, dead, t, held, peak):
        cols = tiles[t]
        old = top[s, :, cols]
        shift = gap[b, :, cols] + dead
        new = jnp.maximum(old, peak[:, cols] + shift)
        top[s, :, cols] = new
        p = jnp.exp2(held[:, cols] * SCALE - (new - shift) * SCALE)
        part = jnp.dot(values[b], p.astype(jnp.bfloat16), preferred_element_type=jnp.float32)
        acc[s, :, cols] = acc[s, :, cols] * jnp.exp2((old - new) * SCALE) + part

    def phase(n, held, held_peak, into, into_peak):
        s, b = place(n)
        dead = jnp.where(n < steps, 0.0, -1e30)
        later_s, later_b = place(n + 1)
        for t in range(len(tiles)):
            score(later_s, later_b, t, into, into_peak, False)
            absorb(s, b, dead, t, held, held_peak)

    for t in range(len(tiles)):
        score(0, own, t, even, peak_even, True)

    def step(i, carry):
        phase(2 * i, even, peak_even, odd, peak_odd)
        phase(2 * i + 1, odd, peak_odd, even, peak_even)
        return carry

    lax.fori_loop(0, (steps + 1) >> 1, step, 0)
    for s, out in enumerate((o0, o1, o2, o3)):

        @pl.when(s <= ahead)
        def _():
            weight = acc[s, DH : DH + 1, :]
            mean = acc[s, :DH, :] / weight
            for h in range(2):
                out[h * DH : (h + 1) * DH, :] = mean[:, h * half : (h + 1) * half].astype(jnp.bfloat16)
            level = top[s] * SCALE + jnp.log(weight) * LOG2E
            if s == 0:
                level = level - gap[own] * SCALE
                passed = gap[0] - gap[own]
            else:
                level = level + first_total * SCALE
                passed = gap[0] + first_total
            stat[...] = jnp.zeros_like(stat)
            put_rows(stat, 0, level, half)
            put_rows(stat, 6, passed * SCALE, half)
            out[2 * DH :, :] = stat[...].astype(jnp.bfloat16)


def attend(pos, sets, kv):
    rows = sets[0].shape[0]
    width = 2 * rows
    return pl.pallas_call(
        attend_kernel,
        out_shape=[jax.ShapeDtypeStruct((2 * DH + 16, rows), jnp.bfloat16)] * DEPTH,
        in_specs=[pl.BlockSpec(memory_space=pltpu.SMEM)]
        + [pl.BlockSpec(memory_space=pltpu.HBM)] * (DEPTH + 1),
        out_specs=[pl.BlockSpec(memory_space=pltpu.VMEM)] * DEPTH,
        scratch_shapes=[
            pltpu.VMEM(kv.shape, jnp.bfloat16),
            pltpu.VMEM((DEPTH, rows, 2 * DH), jnp.bfloat16),
            pltpu.SemaphoreType.DMA((DEPTH + PLANE,)),
            pltpu.VMEM((DEPTH, 2 * DH, width), jnp.bfloat16),
            pltpu.VMEM((PLANE, BLOCK, 2 * DH), jnp.bfloat16),
            pltpu.VMEM((PLANE, DH + 16, BLOCK), jnp.bfloat16),
            pltpu.VMEM((BLOCK, width), jnp.float32),
            pltpu.VMEM((BLOCK, width), jnp.float32),
            pltpu.VMEM((1, width), jnp.float32),
            pltpu.VMEM((1, width), jnp.float32),
            pltpu.VMEM((DEPTH, 1, width), jnp.float32),
            pltpu.VMEM((PLANE, 1, width), jnp.float32),
            pltpu.VMEM((DEPTH, DH + 16, width), jnp.float32),
            pltpu.VMEM((16, rows), jnp.float32),
        ],
        cost_estimate=pl.CostEstimate(
            flops=9_000_000_000, bytes_accessed=4_000_000, transcendentals=16_000_000
        ),
    )(pos, *sets, kv)


def merge_kernel(pos_ref, p0, p1, p2, p3, w_ref, out_ref):
    depth = pos_ref[1]
    parts = (p0, p1, p2, p3)

    def read(ref, first):
        stat = ref[2 * DH :, :].astype(jnp.float32)
        return [
            sum(stat[first + 3 * h + p : first + 3 * h + p + 1, :] for p in range(3)) for h in range(2)
        ]

    merged = []
    passed = read(p0, 6)
    levels = [read(p0, 0)]
    for d in range(1, DEPTH):
        own = read(parts[d], 0)
        lost = jnp.where(d <= depth, 0.0, -1e30)
        levels.append([own[h] + passed[h] + lost for h in range(2)])
        more = read(parts[d], 6)
        passed = [passed[h] + more[h] for h in range(2)]
    for h in range(2):
        high = levels[0][h]
        for d in range(1, DEPTH):
            high = jnp.maximum(high, levels[d][h])
        weights = [jnp.exp2(levels[d][h] - high) for d in range(DEPTH)]
        total = weights[0] + weights[1] + weights[2] + weights[3]
        mixed = None
        for d in range(DEPTH):
            term = parts[d][h * DH : (h + 1) * DH, :].astype(jnp.float32) * (weights[d] / total)
            mixed = term if mixed is None else mixed + term
        merged.append(mixed)
    attended = jnp.transpose(jnp.concatenate(merged, axis=0)).astype(jnp.bfloat16)
    for n in range(0, out_ref.shape[1], 512):
        out_ref[:, n : n + 512] = jnp.dot(
            attended, w_ref[:, n : n + 512], preferred_element_type=jnp.float32
        ).astype(jnp.bfloat16)


def merge(pos, parts, w):
    rows = parts[0].shape[1]
    return pl.pallas_call(
        merge_kernel,
        out_shape=jax.ShapeDtypeStruct((rows, w.shape[1]), jnp.bfloat16),
        in_specs=[pl.BlockSpec(memory_space=pltpu.SMEM)]
        + [pl.BlockSpec(memory_space=pltpu.VMEM)] * (DEPTH + 1),
        out_specs=pl.BlockSpec(memory_space=pltpu.VMEM),
        cost_estimate=pl.CostEstimate(
            flops=2 * rows * w.shape[0] * w.shape[1], bytes_accessed=4_000_000, transcendentals=8 * rows
        ),
    )(pos, *parts, w)


def three(x):
    hi = lax.reduce_precision(x, 8, 7)
    mid = lax.reduce_precision(x - hi, 8, 7)
    return jnp.stack([hi, mid, x - hi - mid], axis=-2).astype(jnp.bfloat16)


def pack(keys, values, gates):
    turned = values.reshape(BLOCK // DH, DH, DH).transpose(0, 2, 1).reshape(BLOCK, DH)
    parts = three(gates * ROOT).reshape(6, 2, 2 * DH).transpose(1, 0, 2)
    parts = jnp.pad(parts, ((0, 0), (0, 2), (0, 0))).reshape(16, 2 * DH)
    return jnp.concatenate([jnp.concatenate([keys, turned], axis=1), parts], axis=0)


def column_tiles(width):
    return [slice(n, n + 512) for n in range(0, width, 512)]


def fold_kernel(gate_hbm, up_hbm, down_hbm, one_hbm, two_hbm, gate, up, down, sems):
    outs, ff = (one_hbm, two_hbm), gate.shape[1] // 2
    blocks = down.shape[1] // DH
    sources = ((gate_hbm, gate), (up_hbm, up), (down_hbm, down))
    copies = [pltpu.make_async_copy(src, dst, sems.at[k]) for k, (src, dst) in enumerate(sources)]
    for c in copies:
        c.start()
    stores = []

    def store(src, dst):
        stores.append(pltpu.make_async_copy(src, dst, sems.at[len(sources) + len(stores)]))
        stores[-1].start()

    for k, held in enumerate((gate, up)):
        copies[k].wait()
        for i, out in enumerate(outs):
            store(held.at[:, i * ff : (i + 1) * ff], out.at[:, k * ff : (k + 1) * ff])
    copies[2].wait()
    for i, out in enumerate(outs):
        for b in range(blocks):
            store(
                down.at[i * ff : (i + 1) * ff, b * DH : (b + 1) * DH],
                out.at[b * ff : (b + 1) * ff, 2 * ff : 3 * ff],
            )
    for c in stores:
        c.wait()


def fold(gate, up, down):
    width, ff = gate.shape
    shape = jax.ShapeDtypeStruct((width, 3 * ff // 2), jnp.bfloat16)
    return pl.pallas_call(
        fold_kernel,
        out_shape=[shape] * 2,
        in_specs=[pl.BlockSpec(memory_space=pltpu.HBM)] * 3,
        out_specs=[pl.BlockSpec(memory_space=pltpu.HBM)] * 2,
        scratch_shapes=[
            pltpu.VMEM(gate.shape, jnp.bfloat16),
            pltpu.VMEM(up.shape, jnp.bfloat16),
            pltpu.VMEM(down.shape, jnp.bfloat16),
            pltpu.SemaphoreType.DMA((7 + 2 * (width // DH),)),
        ],
        cost_estimate=pl.CostEstimate(flops=1_000_000, bytes_accessed=12 * width * ff, transcendentals=0),
    )(gate, up, down)


def expert_kernel(count, joins, *refs):
    holds, x_hbm, pieces, twins = refs[0], refs[1], refs[2 : 2 + count], refs[2 + count : 2 + 2 * count]
    refs = refs[2 + 2 * count :]
    if joins:
        part_hbm, refs = refs[0], refs[1:]
    out_hbm, x_ref, held, hidden, out, sems = refs[:6]
    ff = held.shape[2] // 3
    copies = [pltpu.make_async_copy(x_hbm, x_ref, sems.at[0])]
    copies += [pltpu.make_async_copy(p, held.at[i], sems.at[1 + i]) for i, p in enumerate(pieces)]
    copies[0].start()

    @pl.when(holds[0] == 1)
    def _():
        for i in range(count):
            copies[1 + i].start()

    @pl.when(holds[0] == 0)
    def _():
        for i in range(count):
            pltpu.make_async_copy(twins[i], held.at[i], sems.at[1 + i]).start()

    if joins:
        part = refs[6]
        copies.append(pltpu.make_async_copy(part_hbm, part, sems.at[1 + count]))
        copies[1 + count].start()
    copies[0].wait()
    for i in range(count):
        copies[1 + i].wait()
        for r in range(0, x_ref.shape[0], 256):
            lines = slice(r, r + 256)
            pre = jnp.dot(x_ref[lines, :], held[i, :, : 2 * ff], preferred_element_type=jnp.float32)
            gated, lifted = pre[:, :ff], pre[:, ff:]
            hidden[lines, i * ff : (i + 1) * ff] = (gated * jax.nn.sigmoid(gated) * lifted).astype(
                jnp.bfloat16
            )
    if joins:
        copies[1 + count].wait()
    stores = []
    for n, cols in enumerate(column_tiles(out.shape[1])):
        weights = jnp.concatenate(
            [
                jnp.concatenate(
                    [held[i, b * ff : (b + 1) * ff, 2 * ff :] for b in range(4 * n, 4 * n + 4)], axis=1
                )
                for i in range(count)
            ],
            axis=0,
        )
        total = jnp.dot(hidden[...], weights, preferred_element_type=jnp.float32)
        if joins:
            total = total + part[:, cols]
        out[:, cols] = total.astype(out.dtype)
        stores.append(
            pltpu.make_async_copy(out.at[:, cols], out_hbm.at[:, cols], sems.at[2 + count + n])
        )
        stores[-1].start()
    for c in stores:
        c.wait()


def expert_parts(holds, x, pieces, part, out_type):
    rows, width = x.shape
    count, ff = len(pieces), pieces[0][0].shape[1] // 3
    joined = [] if part is None else [part]
    return pl.pallas_call(
        functools.partial(expert_kernel, count, part is not None),
        out_shape=jax.ShapeDtypeStruct((rows, width), out_type),
        in_specs=[pl.BlockSpec(memory_space=pltpu.SMEM)]
        + [pl.BlockSpec(memory_space=pltpu.HBM)] * (1 + 2 * count + len(joined)),
        out_specs=pl.BlockSpec(memory_space=pltpu.HBM),
        scratch_shapes=[
            pltpu.VMEM((rows, width), jnp.bfloat16),
            pltpu.VMEM((count, width, 3 * ff), jnp.bfloat16),
            pltpu.VMEM((rows, count * ff), jnp.bfloat16),
            pltpu.VMEM((rows, width), out_type),
            pltpu.SemaphoreType.DMA((2 + count + len(column_tiles(width)),)),
        ]
        + [pltpu.VMEM((rows, width), jnp.float32)] * len(joined),
        cost_estimate=pl.CostEstimate(
            flops=count * 6 * rows * width * ff,
            bytes_accessed=count * 6 * width * ff,
            transcendentals=rows * count * ff,
        ),
    )(holds, x, *[p[0] for p in pieces], *[p[1] for p in pieces], *joined)


def shift(x, by, relays=False):
    eps, tps = lax.axis_size("ep"), lax.axis_size("tp")
    pairs = [
        (e * tps + t, e * tps + (t + by) % tps)
        for e in range(eps)
        for t in range(tps)
        if not relays or t % 2 != e % 2
    ]
    return lax.ppermute(x, ("ep", "tp"), pairs)


def to_sibling(x):
    eps, tps = lax.axis_size("ep"), lax.axis_size("tp")
    pairs = [
        (e * tps + t, (e ^ 1) * tps + t) for e in range(eps) for t in range(tps) if t % 2 == e % 2
    ]
    return lax.ppermute(x, ("ep", "tp"), pairs)


def rms_scale(row_block, scale_gain):
    values = row_block.astype(jnp.float32)
    return (
        values * lax.rsqrt(jnp.mean(values * values, axis=-1, keepdims=True) + 1e-06) * scale_gain
    )


def inner(
    queries,
    key_rows,
    value_rows,
    forget_logit,
    out_weight,
    out_gain,
    moe_input,
    moe_gain,
    router_group,
    router_expert,
    route_group,
    route_pick,
    expert_gate,
    expert_up,
    expert_down,
):
    tp_count = lax.axis_size("tp")
    ep_count = lax.axis_size("ep")
    tp_index = lax.axis_index("tp")
    ep_index = lax.axis_index("ep")
    group_rows, width_model = moe_input.shape
    own_rows = group_rows // tp_count
    experts = ep_count
    per_group = experts // GROUPS
    capacity = tp_count * own_rows // experts
    slots = experts * capacity

    one, two = fold(expert_gate[0], expert_up[0], expert_down[0])
    east, west = shift(one, 1), shift(two, -1)
    east_more, west_more = shift(two, 1, True), shift(one, -1, True)
    far_east, far_west = shift(east, 1, True), shift(west, -1, True)
    mine = {
        "one": one, "two": two, "east": east, "west": west,
        "east_more": east_more, "west_more": west_more, "far_east": far_east, "far_west": far_west,
    }
    holds = (ep_index % 2 == tp_index % 2).astype(jnp.int32).reshape(1)
    pieces = [(a, to_sibling(a)) for a in mine.values()]

    running = jnp.cumsum(jax.nn.log_sigmoid(forget_logit), axis=1)
    packed = pack(key_rows, value_rows, running)
    planes = [[z * PLANE + i for i in range(PLANE)] for z in range(ep_count // PLANE)]
    gathered = lax.all_gather(packed, "ep", axis=0, tiled=True, axis_index_groups=planes)
    gathered = gathered.reshape(PLANE, *packed.shape)
    place = jnp.stack([ep_index % PLANE, ep_index // PLANE])
    asked = [queries]
    for d in range(1, DEPTH):
        pairs = [(i, i - PLANE * d) for i in range(PLANE * d, ep_count)]
        asked.append(lax.ppermute(queries, "ep", pairs))
    answers = attend(place, asked, gathered)
    told = [answers[0]]
    for d in range(1, DEPTH):
        pairs = [(i, i + PLANE * d) for i in range(ep_count - PLANE * d)]
        told.append(lax.ppermute(answers[d], "ep", pairs))

    pair_rows = 2 * own_rows
    parity = tp_index % 2
    pair_first = (tp_index // 2) * pair_rows
    pair_group = lax.dynamic_slice_in_dim(route_group, pair_first, pair_rows, 0)
    pair_pick = lax.dynamic_slice_in_dim(route_pick, pair_first, pair_rows, 0)
    chosen = pair_group[:, None] * per_group + pair_pick
    expert_hit = chosen[:, :, None] == jnp.arange(experts, dtype=jnp.int32)
    usage = jnp.any(expert_hit, axis=1).astype(jnp.bfloat16)
    line = jnp.arange(pair_rows, dtype=jnp.int32)
    side = line // own_rows
    earlier = (line[None, :] < line[:, None]) & (side[None, :] == side[:, None])
    before = jnp.dot(
        earlier.astype(jnp.bfloat16), usage, preferred_element_type=jnp.float32
    ).astype(jnp.int32)
    ranks = jnp.sum(jnp.where(expert_hit, before[:, None, :], 0), axis=2)
    goes = (ranks < capacity) & (chosen % 2 == parity)
    target = jnp.where(goes, (chosen - parity + side[:, None]) * capacity + ranks, slots)
    normed = rms_scale(
        lax.dynamic_slice_in_dim(moe_input, pair_first, pair_rows, 0), moe_gain
    ).astype(jnp.bfloat16)
    slot_at = jnp.arange(slots, dtype=jnp.int32)[:, None]
    sent = ((slot_at == target[None, :, 0]) | (slot_at == target[None, :, 1])).astype(jnp.bfloat16)
    outgoing = jnp.dot(sent, normed, preferred_element_type=jnp.float32).astype(jnp.bfloat16)
    outgoing = outgoing.reshape(experts, capacity, width_model)
    arrived = lax.all_to_all(outgoing, "ep", split_axis=0, concat_axis=0, tiled=True)
    arrived = arrived.reshape(slots, width_model)

    part = expert_parts(holds, arrived, pieces[:6], None, jnp.float32)
    results = expert_parts(holds, arrived, pieces[6:], part, jnp.bfloat16)
    results, told[0] = lax.optimization_barrier((results, told[0]))
    mixer_term = merge(place, told, out_weight)
    results = results.reshape(experts, capacity, width_model)
    returned = lax.all_to_all(results, "ep", split_axis=0, concat_axis=0, tiled=True)
    returned = returned.reshape(slots, width_model)

    mixer_summed = lax.psum_scatter(mixer_term, "tp", scatter_dimension=0, tiled=True)
    mixer_out = rms_scale(mixer_summed, out_gain).astype(jnp.bfloat16)

    group_logits = jnp.dot(normed, router_group, preferred_element_type=jnp.float32)
    expert_logits = jnp.dot(normed, router_expert, preferred_element_type=jnp.float32)
    group_top = jnp.max(group_logits, axis=1, keepdims=True)
    group_exp = jnp.exp(group_logits - group_top)
    group_hit = jnp.arange(GROUPS, dtype=jnp.int32)[None, :] == pair_group[:, None]
    group_share = jnp.sum(jnp.where(group_hit, group_exp, 0.0), axis=1) / jnp.sum(group_exp, axis=1)
    picked_logits = jnp.sum(jnp.where(expert_hit, expert_logits[:, None, :], 0.0), axis=2)
    shares = group_share[:, None] * jax.nn.sigmoid(picked_logits - picked_logits[:, ::-1])
    column = jnp.arange(slots, dtype=jnp.int32)[None, :]
    weight = jnp.where(column == target[:, :1], shares[:, :1], 0.0) + jnp.where(
        column == target[:, 1:], shares[:, 1:], 0.0
    )

    def combine(block):
        lines = lax.dynamic_slice_in_dim(weight, block * own_rows, own_rows, 0)
        high = lax.reduce_precision(lines, 8, 7)
        both = jnp.concatenate([high, lines - high], axis=1).astype(jnp.bfloat16)
        twice = jnp.concatenate([returned, returned], axis=0)
        return jnp.dot(both, twice, preferred_element_type=jnp.float32)

    other = lax.ppermute(
        combine(1 - parity).astype(jnp.bfloat16), "tp", [(t, t ^ 1) for t in range(tp_count)]
    )
    moe_out = combine(parity) + other.astype(jnp.float32)
    return (mixer_out, moe_out.astype(jnp.bfloat16))


def solution(mesh):
    in_specs = (
        P("ep", "tp"),
        P("ep", "tp"),
        P("ep", "tp"),
        P("tp", "ep"),
        P("tp", None),
        P(),
        P("ep", None),
        P(),
        P(),
        P(),
        P("ep"),
        P("ep", None),
        P("ep", None, "tp"),
        P("ep", None, "tp"),
        P("ep", "tp", None),
    )
    out_specs = (P(("ep", "tp"), None), P(("ep", "tp"), None))
    return jax.shard_map(inner, mesh=mesh, in_specs=in_specs, out_specs=out_specs, check_vma=False)
```

```python
import math
import jax
import jax.numpy as jnp
from jax import lax
from jax.experimental import pallas as pl
from jax.experimental.pallas import tpu as pltpu
from jax.sharding import PartitionSpec as P

DH = 128
GROUPS = 4
BLOCK = 512
PLANE = 8
DEPTH = 4
ROOT = math.sqrt(DH)
LOG2E = 1.4426950408889634
SCALE = LOG2E / ROOT
QT = 256


def put_rows(stat, first, row, half):
    for h in range(2):
        rest = row[:, h * half : (h + 1) * half]
        for p in range(3):
            piece = rest.astype(jnp.bfloat16).astype(jnp.float32)
            stat[first + 3 * h + p : first + 3 * h + p + 1, :] = piece
            rest = rest - piece


def attend_kernel(
    pos_ref, q0, q1, q2, q3, kv_hbm, o0, o1, o2, o3,
    kv, raw, sems, wide, keys, values, even, odd, peak_even, peak_odd, top, gap, acc, stat,
):
    own, ahead = pos_ref[0], DEPTH - 1 - pos_ref[1]
    width = wide.shape[2]
    half = width // 2
    tiles = [slice(t * QT, (t + 1) * QT) for t in range(width // QT)]
    arriving = [pltpu.make_async_copy(q, raw.at[s], sems.at[s]) for s, q in enumerate((q0, q1, q2, q3))]
    arriving += [
        pltpu.make_async_copy(kv_hbm.at[b], kv.at[b], sems.at[DEPTH + b]) for b in range(PLANE)
    ]
    for c in arriving:
        c.start()
    top[...] = jnp.full_like(top, -1e30)
    acc[...] = jnp.zeros_like(acc)
    line = lax.broadcasted_iota(jnp.int32, (DH, width), 0)
    head = lax.broadcasted_iota(jnp.int32, (DH, width), 1) // half
    index = line % 8
    pick = (line < 16) & (index >= 3 * head) & (index < 3 * head + 3)
    picks = jnp.where(pick, -1.0, 0.0).astype(jnp.bfloat16)
    for s in range(DEPTH):
        arriving[s].wait()

    def turn(s, carry):
        turned = jnp.transpose(raw[s].astype(jnp.float32)).astype(jnp.bfloat16)
        for h in range(2):
            wide[s, :DH, h * half : (h + 1) * half] = turned[h * DH : (h + 1) * DH, :]
        wide[s, DH:, :] = picks
        return carry

    lax.fori_loop(0, ahead + 1, turn, 0)
    for b in range(PLANE):
        arriving[DEPTH + b].wait()
    sums = jnp.zeros((1, width), jnp.float32)
    first_total = None
    for b in reversed(range(PLANE)):
        gates = kv[b, BLOCK:, :]
        last = gates[:, DH:].astype(jnp.float32)
        total = jnp.concatenate(
            [
                jnp.broadcast_to(
                    last[8 + 3 * h : 9 + 3 * h, DH - 1 : DH]
                    + last[9 + 3 * h : 10 + 3 * h, DH - 1 : DH]
                    + last[10 + 3 * h : 11 + 3 * h, DH - 1 : DH],
                    (1, half),
                )
                for h in range(2)
            ],
            axis=1,
        )
        if b == PLANE - 1:
            first_total = total
        else:
            sums = sums + total
        gap[b] = sums

    def prepare(b, carry):
        gates = kv[b, BLOCK:, :]
        gates = jnp.concatenate([gates, jnp.zeros((DH - 16, 2 * DH), jnp.bfloat16)], axis=0)
        turned = jnp.transpose(gates.astype(jnp.float32)).astype(jnp.bfloat16)
        lane = lax.broadcasted_iota(jnp.int32, turned.shape, 1)
        zero = jnp.zeros_like(turned)
        keys[b, :, :DH] = kv[b, :BLOCK, :DH]
        keys[b, : 2 * DH, DH:] = jnp.where(lane < 8, turned, zero)
        keys[b, 2 * DH :, DH:] = jnp.where(lane < 8, zero, turned)
        for c in range(BLOCK // DH):
            values[b, :DH, c * DH : (c + 1) * DH] = kv[b, c * DH : (c + 1) * DH, DH:]
        values[b, DH:, :] = jnp.ones((16, BLOCK), jnp.bfloat16)
        return carry

    lax.fori_loop(0, PLANE, prepare, 0)
    steps = own + 1 + PLANE * ahead

    def place(n):
        m = jnp.maximum(n - (own + 1), 0)
        mine = n <= own
        s = jnp.where(mine, 0, jnp.minimum(1 + (m >> 3), DEPTH - 1))
        b = jnp.where(mine, own - n, PLANE - 1 - (m & 7))
        return s, b

    def score(s, b, t, into, peak, masked):
        scores = jnp.dot(keys[b], wide[s, :, tiles[t]], preferred_element_type=jnp.float32)
        if masked:
            key_at = lax.broadcasted_iota(jnp.int32, scores.shape, 0)
            query_at = lax.broadcasted_iota(jnp.int32, scores.shape, 1) + (t * QT) % half
            scores = jnp.where(key_at <= query_at, scores, -1e30)
        into[:, tiles[t]] = scores
        peak[:, tiles[t]] = jnp.max(scores, axis=0, keepdims=True)

    def absorb(s, b, dead, t, held, peak):
        cols = tiles[t]
        old = top[s, :, cols]
        shift = gap[b, :, cols] + dead
        new = jnp.maximum(old, peak[:, cols] + shift)
        top[s, :, cols] = new
        p = jnp.exp2(held[:, cols] * SCALE - (new - shift) * SCALE)
        part = jnp.dot(values[b], p.astype(jnp.bfloat16), preferred_element_type=jnp.float32)
        acc[s, :, cols] = acc[s, :, cols] * jnp.exp2((old - new) * SCALE) + part

    def phase(n, held, held_peak, into, into_peak):
        s, b = place(n)
        dead = jnp.where(n < steps, 0.0, -1e30)
        later_s, later_b = place(n + 1)
        for t in range(len(tiles)):
            score(later_s, later_b, t, into, into_peak, False)
            absorb(s, b, dead, t, held, held_peak)

    for t in range(len(tiles)):
        score(0, own, t, even, peak_even, True)

    def step(i, carry):
        phase(2 * i, even, peak_even, odd, peak_odd)
        phase(2 * i + 1, odd, peak_odd, even, peak_even)
        return carry

    lax.fori_loop(0, (steps + 1) >> 1, step, 0)
    for s, out in enumerate((o0, o1, o2, o3)):

        @pl.when(s <= ahead)
        def _():
            weight = acc[s, DH : DH + 1, :]
            mean = acc[s, :DH, :] / weight
            for h in range(2):
                out[h * DH : (h + 1) * DH, :] = mean[:, h * half : (h + 1) * half].astype(jnp.bfloat16)
            level = top[s] * SCALE + jnp.log(weight) * LOG2E
            if s == 0:
                level = level - gap[own] * SCALE
                passed = gap[0] - gap[own]
            else:
                level = level + first_total * SCALE
                passed = gap[0] + first_total
            stat[...] = jnp.zeros_like(stat)
            put_rows(stat, 0, level, half)
            put_rows(stat, 6, passed * SCALE, half)
            out[2 * DH :, :] = stat[...].astype(jnp.bfloat16)


def attend(pos, sets, kv):
    rows = sets[0].shape[0]
    width = 2 * rows
    return pl.pallas_call(
        attend_kernel,
        out_shape=[jax.ShapeDtypeStruct((2 * DH + 16, rows), jnp.bfloat16)] * DEPTH,
        in_specs=[pl.BlockSpec(memory_space=pltpu.SMEM)]
        + [pl.BlockSpec(memory_space=pltpu.HBM)] * (DEPTH + 1),
        out_specs=[pl.BlockSpec(memory_space=pltpu.VMEM)] * DEPTH,
        scratch_shapes=[
            pltpu.VMEM(kv.shape, jnp.bfloat16),
            pltpu.VMEM((DEPTH, rows, 2 * DH), jnp.bfloat16),
            pltpu.SemaphoreType.DMA((DEPTH + PLANE,)),
            pltpu.VMEM((DEPTH, 2 * DH, width), jnp.bfloat16),
            pltpu.VMEM((PLANE, BLOCK, 2 * DH), jnp.bfloat16),
            pltpu.VMEM((PLANE, DH + 16, BLOCK), jnp.bfloat16),
            pltpu.VMEM((BLOCK, width), jnp.float32),
            pltpu.VMEM((BLOCK, width), jnp.float32),
            pltpu.VMEM((1, width), jnp.float32),
            pltpu.VMEM((1, width), jnp.float32),
            pltpu.VMEM((DEPTH, 1, width), jnp.float32),
            pltpu.VMEM((PLANE, 1, width), jnp.float32),
            pltpu.VMEM((DEPTH, DH + 16, width), jnp.float32),
            pltpu.VMEM((16, rows), jnp.float32),
        ],
        cost_estimate=pl.CostEstimate(
            flops=9_000_000_000, bytes_accessed=4_000_000, transcendentals=16_000_000
        ),
    )(pos, *sets, kv)


def merge_kernel(pos_ref, p0, p1, p2, p3, w_ref, out_ref):
    depth = pos_ref[1]
    parts = (p0, p1, p2, p3)

    def read(ref, first):
        stat = ref[2 * DH :, :].astype(jnp.float32)
        return [
            sum(stat[first + 3 * h + p : first + 3 * h + p + 1, :] for p in range(3)) for h in range(2)
        ]

    merged = []
    passed = read(p0, 6)
    levels = [read(p0, 0)]
    for d in range(1, DEPTH):
        own = read(parts[d], 0)
        lost = jnp.where(d <= depth, 0.0, -1e30)
        levels.append([own[h] + passed[h] + lost for h in range(2)])
        more = read(parts[d], 6)
        passed = [passed[h] + more[h] for h in range(2)]
    for h in range(2):
        high = levels[0][h]
        for d in range(1, DEPTH):
            high = jnp.maximum(high, levels[d][h])
        weights = [jnp.exp2(levels[d][h] - high) for d in range(DEPTH)]
        total = weights[0] + weights[1] + weights[2] + weights[3]
        mixed = None
        for d in range(DEPTH):
            term = parts[d][h * DH : (h + 1) * DH, :].astype(jnp.float32) * (weights[d] / total)
            mixed = term if mixed is None else mixed + term
        merged.append(mixed)
    attended = jnp.transpose(jnp.concatenate(merged, axis=0)).astype(jnp.bfloat16)
    for n in range(0, out_ref.shape[1], 512):
        out_ref[:, n : n + 512] = jnp.dot(
            attended, w_ref[:, n : n + 512], preferred_element_type=jnp.float32
        ).astype(jnp.bfloat16)


def merge(pos, parts, w):
    rows = parts[0].shape[1]
    return pl.pallas_call(
        merge_kernel,
        out_shape=jax.ShapeDtypeStruct((rows, w.shape[1]), jnp.bfloat16),
        in_specs=[pl.BlockSpec(memory_space=pltpu.SMEM)]
        + [pl.BlockSpec(memory_space=pltpu.VMEM)] * (DEPTH + 1),
        out_specs=pl.BlockSpec(memory_space=pltpu.VMEM),
        cost_estimate=pl.CostEstimate(
            flops=2 * rows * w.shape[0] * w.shape[1], bytes_accessed=4_000_000, transcendentals=8 * rows
        ),
    )(pos, *parts, w)


def three(x):
    hi = lax.reduce_precision(x, 8, 7)
    mid = lax.reduce_precision(x - hi, 8, 7)
    return jnp.stack([hi, mid, x - hi - mid], axis=-2).astype(jnp.bfloat16)


def pack(keys, values, gates):
    turned = values.reshape(BLOCK // DH, DH, DH).transpose(0, 2, 1).reshape(BLOCK, DH)
    parts = three(gates * ROOT).reshape(6, 2, 2 * DH).transpose(1, 0, 2)
    parts = jnp.pad(parts, ((0, 0), (0, 2), (0, 0))).reshape(16, 2 * DH)
    return jnp.concatenate([jnp.concatenate([keys, turned], axis=1), parts], axis=0)


def column_tiles(width):
    return [slice(n, n + 512) for n in range(0, width, 512)]


def fold_kernel(gate_hbm, up_hbm, down_hbm, one_hbm, two_hbm, gate, up, down, sems):
    outs, ff = (one_hbm, two_hbm), gate.shape[1] // 2
    blocks = down.shape[1] // DH
    sources = ((gate_hbm, gate), (up_hbm, up), (down_hbm, down))
    copies = [pltpu.make_async_copy(src, dst, sems.at[k]) for k, (src, dst) in enumerate(sources)]
    for c in copies:
        c.start()
    stores = []

    def store(src, dst):
        stores.append(pltpu.make_async_copy(src, dst, sems.at[len(sources) + len(stores)]))
        stores[-1].start()

    for k, held in enumerate((gate, up)):
        copies[k].wait()
        for i, out in enumerate(outs):
            store(held.at[:, i * ff : (i + 1) * ff], out.at[:, k * ff : (k + 1) * ff])
    copies[2].wait()
    for i, out in enumerate(outs):
        for b in range(blocks):
            store(
                down.at[i * ff : (i + 1) * ff, b * DH : (b + 1) * DH],
                out.at[b * ff : (b + 1) * ff, 2 * ff : 3 * ff],
            )
    for c in stores:
        c.wait()


def fold(gate, up, down):
    width, ff = gate.shape
    shape = jax.ShapeDtypeStruct((width, 3 * ff // 2), jnp.bfloat16)
    return pl.pallas_call(
        fold_kernel,
        out_shape=[shape] * 2,
        in_specs=[pl.BlockSpec(memory_space=pltpu.HBM)] * 3,
        out_specs=[pl.BlockSpec(memory_space=pltpu.HBM)] * 2,
        scratch_shapes=[
            pltpu.VMEM(gate.shape, jnp.bfloat16),
            pltpu.VMEM(up.shape, jnp.bfloat16),
            pltpu.VMEM(down.shape, jnp.bfloat16),
            pltpu.SemaphoreType.DMA((7 + 2 * (width // DH),)),
        ],
        cost_estimate=pl.CostEstimate(flops=1_000_000, bytes_accessed=12 * width * ff, transcendentals=0),
    )(gate, up, down)


def fetch(holds, held, other, dst, sem):
    @pl.when(holds[0] == 1)
    def _():
        pltpu.make_async_copy(held, dst, sem).start()

    @pl.when(holds[0] == 0)
    def _():
        pltpu.make_async_copy(other, dst, sem).start()

    return pltpu.make_async_copy(held, dst, sem)


def gate_lines(x_ref, piece, hidden, first):
    ff = piece.shape[1] // 2
    for r in range(0, x_ref.shape[0], 256):
        lines = slice(r, r + 256)
        pre = jnp.dot(x_ref[lines, :], piece[...], preferred_element_type=jnp.float32)
        gated, lifted = pre[:, :ff], pre[:, ff:]
        hidden[lines, first : first + ff] = (gated * jax.nn.sigmoid(gated) * lifted).astype(jnp.bfloat16)


def early_kernel(
    holds, xa_hbm, xb_hbm, held0, held1, other0, other1, ha_ref, hb_ref, xa, xb, both, sems
):
    ff = both.shape[2] // 2
    rows = [
        pltpu.make_async_copy(src, dst, sems.at[k])
        for k, (src, dst) in enumerate(((xa_hbm, xa), (xb_hbm, xb)))
    ]
    for c in rows:
        c.start()
    copies = [
        fetch(holds, a.at[:, : 2 * ff], b.at[:, : 2 * ff], both.at[i], sems.at[2 + i])
        for i, (a, b) in enumerate(((held0, other0), (held1, other1)))
    ]
    for c in rows:
        c.wait()
    for i, c in enumerate(copies):
        c.wait()
        gate_lines(xa, both.at[i], ha_ref, i * ff)
        gate_lines(xb, both.at[i], hb_ref, i * ff)


def early(holds, xa, xb, pieces):
    rows, width = xa.shape
    ff = pieces[0][0].shape[1] // 3
    shape = jax.ShapeDtypeStruct((rows, 2 * ff), jnp.bfloat16)
    return pl.pallas_call(
        early_kernel,
        out_shape=[shape] * 2,
        in_specs=[pl.BlockSpec(memory_space=pltpu.SMEM)] + [pl.BlockSpec(memory_space=pltpu.HBM)] * 6,
        out_specs=[pl.BlockSpec(memory_space=pltpu.VMEM)] * 2,
        scratch_shapes=[
            pltpu.VMEM((rows, width), jnp.bfloat16),
            pltpu.VMEM((rows, width), jnp.bfloat16),
            pltpu.VMEM((2, width, 2 * ff), jnp.bfloat16),
            pltpu.SemaphoreType.DMA((4,)),
        ],
        cost_estimate=pl.CostEstimate(
            flops=16 * rows * width * ff, bytes_accessed=16 * width * ff, transcendentals=4 * rows * ff
        ),
    )(holds, xa, xb, pieces[0][0], pieces[1][0], pieces[0][1], pieces[1][1])


def late_kernel(
    holds, x_hbm, hid_hbm, h0, h1, h2, h3, o0, o1, o2, o3, out_hbm, x_ref, both, down, hidden, out, sems
):
    ff = both.shape[2] // 2
    rows = [
        pltpu.make_async_copy(x_hbm, x_ref, sems.at[0]),
        pltpu.make_async_copy(hid_hbm, hidden.at[:, : 2 * ff], sems.at[1]),
    ]
    for c in rows:
        c.start()
    gates = [
        fetch(holds, a.at[:, : 2 * ff], b.at[:, : 2 * ff], both.at[i], sems.at[2 + i])
        for i, (a, b) in enumerate(((h2, o2), (h3, o3)))
    ]
    downs = [
        fetch(holds, a.at[:, 2 * ff :], b.at[:, 2 * ff :], down.at[i], sems.at[4 + i])
        for i, (a, b) in enumerate(((h0, o0), (h1, o1), (h2, o2), (h3, o3)))
    ]
    rows[0].wait()
    rows[1].wait()
    for i, c in enumerate(gates):
        c.wait()
        gate_lines(x_ref, both.at[i], hidden, (2 + i) * ff)
    for c in downs:
        c.wait()
    stores = []
    for n, cols in enumerate(column_tiles(out.shape[1])):
        weights = jnp.concatenate(
            [
                jnp.concatenate([down[i, b * ff : (b + 1) * ff, :] for b in range(4 * n, 4 * n + 4)], axis=1)
                for i in range(4)
            ],
            axis=0,
        )
        out[:, cols] = jnp.dot(hidden[...], weights, preferred_element_type=jnp.float32).astype(out.dtype)
        stores.append(pltpu.make_async_copy(out.at[:, cols], out_hbm.at[:, cols], sems.at[8 + n]))
        stores[-1].start()
    for c in stores:
        c.wait()


def late(holds, x, hid, pieces):
    rows, width = x.shape
    ff = pieces[0][0].shape[1] // 3
    return pl.pallas_call(
        late_kernel,
        out_shape=jax.ShapeDtypeStruct((rows, width), jnp.bfloat16),
        in_specs=[pl.BlockSpec(memory_space=pltpu.SMEM)] + [pl.BlockSpec(memory_space=pltpu.HBM)] * 10,
        out_specs=pl.BlockSpec(memory_space=pltpu.HBM),
        scratch_shapes=[
            pltpu.VMEM((rows, width), jnp.bfloat16),
            pltpu.VMEM((2, width, 2 * ff), jnp.bfloat16),
            pltpu.VMEM((4, width, ff), jnp.bfloat16),
            pltpu.VMEM((rows, 4 * ff), jnp.bfloat16),
            pltpu.VMEM((rows, width), jnp.bfloat16),
            pltpu.SemaphoreType.DMA((8 + len(column_tiles(width)),)),
        ],
        cost_estimate=pl.CostEstimate(
            flops=16 * rows * width * ff, bytes_accessed=20 * width * ff, transcendentals=2 * rows * ff
        ),
    )(holds, x, hid, *[p[0] for p in pieces], *[p[1] for p in pieces])


def shift(x, by, sources=(0, 1)):
    eps, tps = lax.axis_size("ep"), lax.axis_size("tp")
    pairs = [
        (e * tps + t, (e ^ 1) * tps + (t + by) % tps)
        for e in range(eps)
        for t in range(tps)
        if (e + t) % 2 in sources
    ]
    return lax.ppermute(x, ("ep", "tp"), pairs)


def swap_cores(x):
    return lax.ppermute(x, "ep", [(e, e ^ 1) for e in range(lax.axis_size("ep"))])


def rms_scale(row_block, scale_gain):
    values = row_block.astype(jnp.float32)
    return (
        values * lax.rsqrt(jnp.mean(values * values, axis=-1, keepdims=True) + 1e-06) * scale_gain
    )


def inner(
    queries,
    key_rows,
    value_rows,
    forget_logit,
    out_weight,
    out_gain,
    moe_input,
    moe_gain,
    router_group,
    router_expert,
    route_group,
    route_pick,
    expert_gate,
    expert_up,
    expert_down,
):
    tp_count = lax.axis_size("tp")
    ep_count = lax.axis_size("ep")
    tp_index = lax.axis_index("tp")
    ep_index = lax.axis_index("ep")
    group_rows, width_model = moe_input.shape
    own_rows = group_rows // tp_count
    experts = ep_count
    per_group = experts // GROUPS
    capacity = tp_count * own_rows // experts
    slots = experts * capacity

    one, two = fold(expert_gate[0], expert_up[0], expert_down[0])
    east, west = shift(one, 1), shift(two, -1)
    east_more, west_more = shift(two, 1, (1,)), shift(one, -1, (1,))
    far_east, far_west = shift(east, 1, (0,)), shift(west, -1, (0,))
    holds = (ep_index % 2 == tp_index % 2).astype(jnp.int32).reshape(1)
    pieces = [(one, east), (two, west), (far_east, east_more), (far_west, west_more)]

    running = jnp.cumsum(jax.nn.log_sigmoid(forget_logit), axis=1)
    packed = pack(key_rows, value_rows, running)
    planes = [[z * PLANE + i for i in range(PLANE)] for z in range(ep_count // PLANE)]
    gathered = lax.all_gather(packed, "ep", axis=0, tiled=True, axis_index_groups=planes)
    gathered = gathered.reshape(PLANE, *packed.shape)
    place = jnp.stack([ep_index % PLANE, ep_index // PLANE])
    asked = [queries]
    for d in range(1, DEPTH):
        pairs = [(i, i - PLANE * d) for i in range(PLANE * d, ep_count)]
        asked.append(lax.ppermute(queries, "ep", pairs))
    answers = attend(place, asked, gathered)
    told = [answers[0]]
    for d in range(1, DEPTH):
        pairs = [(i, i + PLANE * d) for i in range(ep_count - PLANE * d)]
        told.append(lax.ppermute(answers[d], "ep", pairs))

    pair_rows = 2 * own_rows
    parity = tp_index % 2
    pair_first = (tp_index // 2) * pair_rows
    pair_group = lax.dynamic_slice_in_dim(route_group, pair_first, pair_rows, 0)
    pair_pick = lax.dynamic_slice_in_dim(route_pick, pair_first, pair_rows, 0)
    chosen = pair_group[:, None] * per_group + pair_pick
    expert_hit = chosen[:, :, None] == jnp.arange(experts, dtype=jnp.int32)
    usage = jnp.any(expert_hit, axis=1).astype(jnp.bfloat16)
    line = jnp.arange(pair_rows, dtype=jnp.int32)
    side = line // own_rows
    earlier = (line[None, :] < line[:, None]) & (side[None, :] == side[:, None])
    before = jnp.dot(
        earlier.astype(jnp.bfloat16), usage, preferred_element_type=jnp.float32
    ).astype(jnp.int32)
    ranks = jnp.sum(jnp.where(expert_hit, before[:, None, :], 0), axis=2)
    goes = (ranks < capacity) & (chosen % 2 == parity)
    target = jnp.where(goes, (chosen - parity + side[:, None]) * capacity + ranks, slots)
    normed = rms_scale(
        lax.dynamic_slice_in_dim(moe_input, pair_first, pair_rows, 0), moe_gain
    ).astype(jnp.bfloat16)
    slot_at = jnp.arange(slots, dtype=jnp.int32)[:, None]
    sent = ((slot_at == target[None, :, 0]) | (slot_at == target[None, :, 1])).astype(jnp.bfloat16)
    outgoing = jnp.dot(sent, normed, preferred_element_type=jnp.float32).astype(jnp.bfloat16)
    outgoing = outgoing.reshape(experts, capacity, width_model)
    arrived = lax.all_to_all(outgoing, "ep", split_axis=0, concat_axis=0, tiled=True)
    arrived = arrived.reshape(slots, width_model)

    twin_rows = swap_cores(arrived)
    own_hidden, twin_hidden = early(holds, arrived, twin_rows, pieces[:2])
    for_twin = late(holds, twin_rows, twin_hidden, pieces)
    from_twin = swap_cores(for_twin)
    results = late(holds, arrived, own_hidden, pieces)
    returned = []
    for k in range(2):
        cols = slice(k * width_model // 2, (k + 1) * width_model // 2)
        summed = results[:, cols].astype(jnp.float32) + from_twin[:, cols].astype(jnp.float32)
        summed = summed.astype(jnp.bfloat16).reshape(experts, capacity, width_model // 2)
        back = lax.all_to_all(summed, "ep", split_axis=0, concat_axis=0, tiled=True)
        returned.append(back.reshape(slots, width_model // 2))
    mixer_term = merge(place, told, out_weight)
    mixer_summed = lax.psum_scatter(mixer_term, "tp", scatter_dimension=0, tiled=True)
    mixer_out = rms_scale(mixer_summed, out_gain).astype(jnp.bfloat16)

    group_logits = jnp.dot(normed, router_group, preferred_element_type=jnp.float32)
    expert_logits = jnp.dot(normed, router_expert, preferred_element_type=jnp.float32)
    group_top = jnp.max(group_logits, axis=1, keepdims=True)
    group_exp = jnp.exp(group_logits - group_top)
    group_hit = jnp.arange(GROUPS, dtype=jnp.int32)[None, :] == pair_group[:, None]
    group_share = jnp.sum(jnp.where(group_hit, group_exp, 0.0), axis=1) / jnp.sum(group_exp, axis=1)
    picked_logits = jnp.sum(jnp.where(expert_hit, expert_logits[:, None, :], 0.0), axis=2)
    shares = group_share[:, None] * jax.nn.sigmoid(picked_logits - picked_logits[:, ::-1])
    column = jnp.arange(slots, dtype=jnp.int32)[None, :]
    weight = jnp.where(column == target[:, :1], shares[:, :1], 0.0) + jnp.where(
        column == target[:, 1:], shares[:, 1:], 0.0
    )

    def combine(block, back):
        lines = lax.dynamic_slice_in_dim(weight, block * own_rows, own_rows, 0)
        high = lax.reduce_precision(lines, 8, 7)
        both = jnp.concatenate([high, lines - high], axis=1).astype(jnp.bfloat16)
        twice = jnp.concatenate([back, back], axis=0)
        return jnp.dot(both, twice, preferred_element_type=jnp.float32)

    halves = []
    for back in returned:
        pairs = [(t, t ^ 1) for t in range(tp_count)]
        other = lax.ppermute(combine(1 - parity, back).astype(jnp.bfloat16), "tp", pairs)
        halves.append(combine(parity, back) + other.astype(jnp.float32))
    moe_out = jnp.concatenate(halves, axis=1)
    return (mixer_out, moe_out.astype(jnp.bfloat16))


def solution(mesh):
    in_specs = (
        P("ep", "tp"),
        P("ep", "tp"),
        P("ep", "tp"),
        P("tp", "ep"),
        P("tp", None),
        P(),
        P("ep", None),
        P(),
        P(),
        P(),
        P("ep"),
        P("ep", None),
        P("ep", None, "tp"),
        P("ep", None, "tp"),
        P("ep", "tp", None),
    )
    out_specs = (P(("ep", "tp"), None), P(("ep", "tp"), None))
    return jax.shard_map(inner, mesh=mesh, in_specs=in_specs, out_specs=out_specs, check_vma=False)
```

```python
import functools
import math
import jax
import jax.numpy as jnp
from jax import lax
from jax.experimental import pallas as pl
from jax.experimental.pallas import tpu as pltpu
from jax.sharding import PartitionSpec as P

DH = 128
GROUPS = 4
BLOCK = 512
PLANE = 8
DEPTH = 4
ROOT = math.sqrt(DH)
LOG2E = 1.4426950408889634
SCALE = LOG2E / ROOT
QT = 256


def put_rows(stat, first, row, half):
    for h in range(2):
        rest = row[:, h * half : (h + 1) * half]
        for p in range(3):
            piece = rest.astype(jnp.bfloat16).astype(jnp.float32)
            stat[first + 3 * h + p : first + 3 * h + p + 1, :] = piece
            rest = rest - piece


def attend_kernel(
    pos_ref, q0, q1, q2, q3, kv_hbm, o0, o1, o2, o3,
    kv, raw, sems, wide, keys, values, even, odd, peak_even, peak_odd, top, gap, acc, stat,
):
    own, ahead = pos_ref[0], DEPTH - 1 - pos_ref[1]
    width = wide.shape[2]
    half = width // 2
    tiles = [slice(t * QT, (t + 1) * QT) for t in range(width // QT)]
    arriving = [pltpu.make_async_copy(q, raw.at[s], sems.at[s]) for s, q in enumerate((q0, q1, q2, q3))]
    arriving += [
        pltpu.make_async_copy(kv_hbm.at[b], kv.at[b], sems.at[DEPTH + b]) for b in range(PLANE)
    ]
    for c in arriving:
        c.start()
    top[...] = jnp.full_like(top, -1e30)
    acc[...] = jnp.zeros_like(acc)
    line = lax.broadcasted_iota(jnp.int32, (DH, width), 0)
    head = lax.broadcasted_iota(jnp.int32, (DH, width), 1) // half
    index = line % 8
    pick = (line < 16) & (index >= 3 * head) & (index < 3 * head + 3)
    picks = jnp.where(pick, -1.0, 0.0).astype(jnp.bfloat16)
    for s in range(DEPTH):
        arriving[s].wait()

    def turn(s, carry):
        turned = jnp.transpose(raw[s].astype(jnp.float32)).astype(jnp.bfloat16)
        for h in range(2):
            wide[s, :DH, h * half : (h + 1) * half] = turned[h * DH : (h + 1) * DH, :]
        wide[s, DH:, :] = picks
        return carry

    lax.fori_loop(0, ahead + 1, turn, 0)
    for b in range(PLANE):
        arriving[DEPTH + b].wait()
    sums = jnp.zeros((1, width), jnp.float32)
    first_total = None
    for b in reversed(range(PLANE)):
        gates = kv[b, BLOCK:, :]
        last = gates[:, DH:].astype(jnp.float32)
        total = jnp.concatenate(
            [
                jnp.broadcast_to(
                    last[8 + 3 * h : 9 + 3 * h, DH - 1 : DH]
                    + last[9 + 3 * h : 10 + 3 * h, DH - 1 : DH]
                    + last[10 + 3 * h : 11 + 3 * h, DH - 1 : DH],
                    (1, half),
                )
                for h in range(2)
            ],
            axis=1,
        )
        if b == PLANE - 1:
            first_total = total
        else:
            sums = sums + total
        gap[b] = sums

    def prepare(b, carry):
        gates = kv[b, BLOCK:, :]
        gates = jnp.concatenate([gates, jnp.zeros((DH - 16, 2 * DH), jnp.bfloat16)], axis=0)
        turned = jnp.transpose(gates.astype(jnp.float32)).astype(jnp.bfloat16)
        lane = lax.broadcasted_iota(jnp.int32, turned.shape, 1)
        zero = jnp.zeros_like(turned)
        keys[b, :, :DH] = kv[b, :BLOCK, :DH]
        keys[b, : 2 * DH, DH:] = jnp.where(lane < 8, turned, zero)
        keys[b, 2 * DH :, DH:] = jnp.where(lane < 8, zero, turned)
        for c in range(BLOCK // DH):
            values[b, :DH, c * DH : (c + 1) * DH] = kv[b, c * DH : (c + 1) * DH, DH:]
        values[b, DH:, :] = jnp.ones((16, BLOCK), jnp.bfloat16)
        return carry

    lax.fori_loop(0, PLANE, prepare, 0)
    steps = own + 1 + PLANE * ahead

    def place(n):
        m = jnp.maximum(n - (own + 1), 0)
        mine = n <= own
        s = jnp.where(mine, 0, jnp.minimum(1 + (m >> 3), DEPTH - 1))
        b = jnp.where(mine, own - n, PLANE - 1 - (m & 7))
        return s, b

    def score(s, b, t, into, peak, masked):
        scores = jnp.dot(keys[b], wide[s, :, tiles[t]], preferred_element_type=jnp.float32)
        if masked:
            key_at = lax.broadcasted_iota(jnp.int32, scores.shape, 0)
            query_at = lax.broadcasted_iota(jnp.int32, scores.shape, 1) + (t * QT) % half
            scores = jnp.where(key_at <= query_at, scores, -1e30)
        into[:, tiles[t]] = scores
        peak[:, tiles[t]] = jnp.max(scores, axis=0, keepdims=True)

    def absorb(s, b, dead, t, held, peak):
        cols = tiles[t]
        old = top[s, :, cols]
        shift = gap[b, :, cols] + dead
        new = jnp.maximum(old, peak[:, cols] + shift)
        top[s, :, cols] = new
        p = jnp.exp2(held[:, cols] * SCALE - (new - shift) * SCALE)
        part = jnp.dot(values[b], p.astype(jnp.bfloat16), preferred_element_type=jnp.float32)
        acc[s, :, cols] = acc[s, :, cols] * jnp.exp2((old - new) * SCALE) + part

    def phase(n, held, held_peak, into, into_peak):
        s, b = place(n)
        dead = jnp.where(n < steps, 0.0, -1e30)
        later_s, later_b = place(n + 1)
        for t in range(len(tiles)):
            score(later_s, later_b, t, into, into_peak, False)
            absorb(s, b, dead, t, held, held_peak)

    for t in range(len(tiles)):
        score(0, own, t, even, peak_even, True)

    def step(i, carry):
        phase(2 * i, even, peak_even, odd, peak_odd)
        phase(2 * i + 1, odd, peak_odd, even, peak_even)
        return carry

    lax.fori_loop(0, (steps + 1) >> 1, step, 0)
    for s, out in enumerate((o0, o1, o2, o3)):

        @pl.when(s <= ahead)
        def _():
            weight = acc[s, DH : DH + 1, :]
            mean = acc[s, :DH, :] / weight
            for h in range(2):
                out[h * DH : (h + 1) * DH, :] = mean[:, h * half : (h + 1) * half].astype(jnp.bfloat16)
            level = top[s] * SCALE + jnp.log(weight) * LOG2E
            if s == 0:
                level = level - gap[own] * SCALE
                passed = gap[0] - gap[own]
            else:
                level = level + first_total * SCALE
                passed = gap[0] + first_total
            stat[...] = jnp.zeros_like(stat)
            put_rows(stat, 0, level, half)
            put_rows(stat, 6, passed * SCALE, half)
            out[2 * DH :, :] = stat[...].astype(jnp.bfloat16)


def attend(pos, sets, kv):
    rows = sets[0].shape[0]
    width = 2 * rows
    return pl.pallas_call(
        attend_kernel,
        out_shape=[jax.ShapeDtypeStruct((2 * DH + 16, rows), jnp.bfloat16)] * DEPTH,
        in_specs=[pl.BlockSpec(memory_space=pltpu.SMEM)]
        + [pl.BlockSpec(memory_space=pltpu.HBM)] * (DEPTH + 1),
        out_specs=[pl.BlockSpec(memory_space=pltpu.VMEM)] * DEPTH,
        scratch_shapes=[
            pltpu.VMEM(kv.shape, jnp.bfloat16),
            pltpu.VMEM((DEPTH, rows, 2 * DH), jnp.bfloat16),
            pltpu.SemaphoreType.DMA((DEPTH + PLANE,)),
            pltpu.VMEM((DEPTH, 2 * DH, width), jnp.bfloat16),
            pltpu.VMEM((PLANE, BLOCK, 2 * DH), jnp.bfloat16),
            pltpu.VMEM((PLANE, DH + 16, BLOCK), jnp.bfloat16),
            pltpu.VMEM((BLOCK, width), jnp.float32),
            pltpu.VMEM((BLOCK, width), jnp.float32),
            pltpu.VMEM((1, width), jnp.float32),
            pltpu.VMEM((1, width), jnp.float32),
            pltpu.VMEM((DEPTH, 1, width), jnp.float32),
            pltpu.VMEM((PLANE, 1, width), jnp.float32),
            pltpu.VMEM((DEPTH, DH + 16, width), jnp.float32),
            pltpu.VMEM((16, rows), jnp.float32),
        ],
        cost_estimate=pl.CostEstimate(
            flops=9_000_000_000, bytes_accessed=4_000_000, transcendentals=16_000_000
        ),
    )(pos, *sets, kv)


def merge_kernel(pos_ref, p0, p1, p2, p3, w_ref, out_ref):
    depth = pos_ref[1]
    parts = (p0, p1, p2, p3)

    def read(ref, first):
        stat = ref[2 * DH :, :].astype(jnp.float32)
        return [
            sum(stat[first + 3 * h + p : first + 3 * h + p + 1, :] for p in range(3)) for h in range(2)
        ]

    merged = []
    passed = read(p0, 6)
    levels = [read(p0, 0)]
    for d in range(1, DEPTH):
        own = read(parts[d], 0)
        lost = jnp.where(d <= depth, 0.0, -1e30)
        levels.append([own[h] + passed[h] + lost for h in range(2)])
        more = read(parts[d], 6)
        passed = [passed[h] + more[h] for h in range(2)]
    for h in range(2):
        high = levels[0][h]
        for d in range(1, DEPTH):
            high = jnp.maximum(high, levels[d][h])
        weights = [jnp.exp2(levels[d][h] - high) for d in range(DEPTH)]
        total = weights[0] + weights[1] + weights[2] + weights[3]
        mixed = None
        for d in range(DEPTH):
            term = parts[d][h * DH : (h + 1) * DH, :].astype(jnp.float32) * (weights[d] / total)
            mixed = term if mixed is None else mixed + term
        merged.append(mixed)
    attended = jnp.transpose(jnp.concatenate(merged, axis=0)).astype(jnp.bfloat16)
    for n in range(0, out_ref.shape[1], 512):
        out_ref[:, n : n + 512] = jnp.dot(
            attended, w_ref[:, n : n + 512], preferred_element_type=jnp.float32
        ).astype(jnp.bfloat16)


def merge(pos, parts, w):
    rows = parts[0].shape[1]
    return pl.pallas_call(
        merge_kernel,
        out_shape=jax.ShapeDtypeStruct((rows, w.shape[1]), jnp.bfloat16),
        in_specs=[pl.BlockSpec(memory_space=pltpu.SMEM)]
        + [pl.BlockSpec(memory_space=pltpu.VMEM)] * (DEPTH + 1),
        out_specs=pl.BlockSpec(memory_space=pltpu.VMEM),
        cost_estimate=pl.CostEstimate(
            flops=2 * rows * w.shape[0] * w.shape[1], bytes_accessed=4_000_000, transcendentals=8 * rows
        ),
    )(pos, *parts, w)


def three(x):
    hi = lax.reduce_precision(x, 8, 7)
    mid = lax.reduce_precision(x - hi, 8, 7)
    return jnp.stack([hi, mid, x - hi - mid], axis=-2).astype(jnp.bfloat16)


def pack(keys, values, gates):
    turned = values.reshape(BLOCK // DH, DH, DH).transpose(0, 2, 1).reshape(BLOCK, DH)
    parts = three(gates * ROOT).reshape(6, 2, 2 * DH).transpose(1, 0, 2)
    parts = jnp.pad(parts, ((0, 0), (0, 2), (0, 0))).reshape(16, 2 * DH)
    return jnp.concatenate([jnp.concatenate([keys, turned], axis=1), parts], axis=0)


def hidden_kernel(count, x_hbm, *refs):
    weights, (out_ref, x_ref, both, sems) = refs[: 2 * count], refs[2 * count :]
    ff = both.shape[2] // 2
    copies = [pltpu.make_async_copy(x_hbm, x_ref, sems.at[2 * count])]
    for q in range(count):
        copies.append(pltpu.make_async_copy(weights[2 * q], both.at[q, :, :ff], sems.at[2 * q]))
        copies.append(pltpu.make_async_copy(weights[2 * q + 1], both.at[q, :, ff:], sems.at[2 * q + 1]))
    for c in copies:
        c.start()
    copies[0].wait()
    for q in range(count):
        copies[1 + 2 * q].wait()
        copies[2 + 2 * q].wait()
        for r in range(0, x_ref.shape[0], 256):
            lines = slice(r, r + 256)
            pre = jnp.dot(x_ref[lines, :], both[q], preferred_element_type=jnp.float32)
            gated, lifted = pre[:, :ff], pre[:, ff:]
            out_ref[lines, q * ff : (q + 1) * ff] = (gated * jax.nn.sigmoid(gated) * lifted).astype(
                jnp.bfloat16
            )


def hidden_units(x, weights):
    rows, width = x.shape
    count, ff = len(weights) // 2, weights[0].shape[1]
    return pl.pallas_call(
        functools.partial(hidden_kernel, count),
        out_shape=jax.ShapeDtypeStruct((rows, count * ff), jnp.bfloat16),
        in_specs=[pl.BlockSpec(memory_space=pltpu.HBM)] * (1 + len(weights)),
        out_specs=pl.BlockSpec(memory_space=pltpu.VMEM),
        scratch_shapes=[
            pltpu.VMEM((rows, width), jnp.bfloat16),
            pltpu.VMEM((count, width, 2 * ff), jnp.bfloat16),
            pltpu.SemaphoreType.DMA((1 + 2 * count,)),
        ],
        cost_estimate=pl.CostEstimate(
            flops=count * 4 * rows * width * ff,
            bytes_accessed=count * 4 * width * ff,
            transcendentals=rows * count * ff,
        ),
    )(x, *weights)


def down_kernel(count, hidden_hbm, *refs):
    weights, (out_hbm, hidden, down, out, sems) = refs[:count], refs[count:]
    ff = down.shape[0] // count
    pairs = [(hidden_hbm, hidden)]
    pairs += [(w, down.at[q * ff : (q + 1) * ff, :]) for q, w in enumerate(weights)]
    copies = [pltpu.make_async_copy(src, dst, sems.at[k]) for k, (src, dst) in enumerate(pairs)]
    for c in copies:
        c.start()
    for c in copies:
        c.wait()
    stores = []
    for n in range(0, out.shape[1], 256):
        cols = slice(n, n + 256)
        out[:, cols] = jnp.dot(hidden[...], down[:, cols], preferred_element_type=jnp.float32).astype(
            out.dtype
        )
        stores.append(
            pltpu.make_async_copy(
                out.at[:, cols], out_hbm.at[:, cols], sems.at[len(pairs) + len(stores)]
            )
        )
        stores[-1].start()
    for c in stores:
        c.wait()


def down_columns(hidden, weights):
    rows, count = hidden.shape[0], len(weights)
    ff, columns = weights[0].shape
    return pl.pallas_call(
        functools.partial(down_kernel, count),
        out_shape=jax.ShapeDtypeStruct((rows, columns), jnp.bfloat16),
        in_specs=[pl.BlockSpec(memory_space=pltpu.HBM)] * (1 + count),
        out_specs=pl.BlockSpec(memory_space=pltpu.HBM),
        scratch_shapes=[
            pltpu.VMEM((rows, count * ff), jnp.bfloat16),
            pltpu.VMEM((count * ff, columns), jnp.bfloat16),
            pltpu.VMEM((rows, columns), jnp.bfloat16),
            pltpu.SemaphoreType.DMA((1 + count + columns // 256,)),
        ],
        cost_estimate=pl.CostEstimate(
            flops=2 * rows * count * ff * columns,
            bytes_accessed=2 * count * ff * columns,
            transcendentals=0,
        ),
    )(hidden, *weights)


def shift(x, by):
    count = lax.axis_size("tp")
    return lax.ppermute(x, "tp", [(i, (i + by) % count) for i in range(count)])


def rms_scale(row_block, scale_gain):
    values = row_block.astype(jnp.float32)
    return (
        values * lax.rsqrt(jnp.mean(values * values, axis=-1, keepdims=True) + 1e-06) * scale_gain
    )


def inner(
    queries,
    key_rows,
    value_rows,
    forget_logit,
    out_weight,
    out_gain,
    moe_input,
    moe_gain,
    router_group,
    router_expert,
    route_group,
    route_pick,
    expert_gate,
    expert_up,
    expert_down,
):
    tp_count = lax.axis_size("tp")
    ep_count = lax.axis_size("ep")
    tp_index = lax.axis_index("tp")
    ep_index = lax.axis_index("ep")
    group_rows, width_model = moe_input.shape
    own_rows = group_rows // tp_count
    experts = ep_count
    per_group = experts // GROUPS
    capacity = tp_count * own_rows // experts
    slots = experts * capacity

    gate, up, down = expert_gate[0], expert_up[0], expert_down[0]
    cuts = (slice(0, SPLIT), slice(SPLIT, width_model))
    low = [down[:, c] for c in cuts]
    left_gate, right_up = shift(gate, 1), shift(up, -1)
    left_low = [shift(low[0], 1), shift(low[1], 1)]
    right_low = [shift(low[0], -1), shift(low[1], -1)]
    left_up, right_gate = shift(up, 1), shift(gate, -1)
    far_gate, far_up = shift(left_gate, 1), shift(right_up, -1)
    far_low = [shift(left_low[0], 1), shift(right_low[1], -1)]

    running = jnp.cumsum(jax.nn.log_sigmoid(forget_logit), axis=1)
    packed = pack(key_rows, value_rows, running)
    planes = [[z * PLANE + i for i in range(PLANE)] for z in range(ep_count // PLANE)]
    gathered = lax.all_gather(packed, "ep", axis=0, tiled=True, axis_index_groups=planes)
    gathered = gathered.reshape(PLANE, *packed.shape)
    place = jnp.stack([ep_index % PLANE, ep_index // PLANE])
    asked = [queries]
    for d in range(1, DEPTH):
        pairs = [(i, i - PLANE * d) for i in range(PLANE * d, ep_count)]
        asked.append(lax.ppermute(queries, "ep", pairs))
    answers = attend(place, asked, gathered)
    told = [answers[0]]
    for d in range(1, DEPTH):
        pairs = [(i, i + PLANE * d) for i in range(ep_count - PLANE * d)]
        told.append(lax.ppermute(answers[d], "ep", pairs))

    own_first = tp_index * own_rows
    own_group = lax.dynamic_slice_in_dim(route_group, own_first, own_rows, 0)
    own_pick = lax.dynamic_slice_in_dim(route_pick, own_first, own_rows, 0)
    chosen = own_group[:, None] * per_group + own_pick
    expert_hit = chosen[:, :, None] == jnp.arange(experts, dtype=jnp.int32)
    usage = jnp.any(expert_hit, axis=1).astype(jnp.bfloat16)
    line = jnp.arange(own_rows, dtype=jnp.int32)
    earlier = (line[None, :] < line[:, None]).astype(jnp.bfloat16)
    before = jnp.dot(earlier, usage, preferred_element_type=jnp.float32).astype(jnp.int32)
    ranks = jnp.sum(jnp.where(expert_hit, before[:, None, :], 0), axis=2)
    target = jnp.where(ranks < capacity, chosen * capacity + ranks, slots)
    normed = rms_scale(
        lax.dynamic_slice_in_dim(moe_input, own_first, own_rows, 0), moe_gain
    ).astype(jnp.bfloat16)
    slot_at = jnp.arange(slots, dtype=jnp.int32)[:, None]
    sent = ((slot_at == target[None, :, 0]) | (slot_at == target[None, :, 1])).astype(jnp.bfloat16)
    outgoing = jnp.dot(sent, normed, preferred_element_type=jnp.float32).astype(jnp.bfloat16)
    outgoing = outgoing.reshape(experts, capacity, width_model)
    arrived = lax.all_to_all(outgoing, "ep", split_axis=0, concat_axis=0, tiled=True)
    arrived = arrived.reshape(slots, width_model)

    hidden = hidden_units(
        arrived, (gate, up, left_gate, left_up, right_gate, right_up, far_gate, far_up)
    )
    mixer_term = merge(place, told, out_weight)
    mixer_term, far_low[1] = lax.optimization_barrier((mixer_term, far_low[1]))
    returned = []
    for k in range(2):
        results = down_columns(hidden, (low[k], left_low[k], right_low[k], far_low[k]))
        back = lax.all_to_all(
            results.reshape(experts, capacity, -1), "ep", split_axis=0, concat_axis=0, tiled=True
        )
        returned.append(back.reshape(slots, -1))
    mixer_summed = lax.psum_scatter(mixer_term, "tp", scatter_dimension=0, tiled=True)
    mixer_out = rms_scale(mixer_summed, out_gain).astype(jnp.bfloat16)

    mixer_out, returned[1] = lax.optimization_barrier((mixer_out, returned[1]))
    group_logits = jnp.dot(normed, router_group, preferred_element_type=jnp.float32)
    expert_logits = jnp.dot(normed, router_expert, preferred_element_type=jnp.float32)
    group_top = jnp.max(group_logits, axis=1, keepdims=True)
    group_exp = jnp.exp(group_logits - group_top)
    group_hit = jnp.arange(GROUPS, dtype=jnp.int32)[None, :] == own_group[:, None]
    group_share = jnp.sum(jnp.where(group_hit, group_exp, 0.0), axis=1) / jnp.sum(group_exp, axis=1)
    picked_logits = jnp.sum(jnp.where(expert_hit, expert_logits[:, None, :], 0.0), axis=2)
    shares = group_share[:, None] * jax.nn.sigmoid(picked_logits - picked_logits[:, ::-1])
    column = jnp.arange(slots, dtype=jnp.int32)[None, :]
    weight = jnp.where(column == target[:, :1], shares[:, :1], 0.0) + jnp.where(
        column == target[:, 1:], shares[:, 1:], 0.0
    )
    high = lax.reduce_precision(weight, 8, 7)
    both = jnp.concatenate([high, weight - high], axis=1).astype(jnp.bfloat16)
    moe_out = jnp.concatenate(
        [
            jnp.dot(both, jnp.concatenate([back, back], axis=0), preferred_element_type=jnp.float32)
            for back in returned
        ],
        axis=1,
    )
    return (mixer_out, moe_out.astype(jnp.bfloat16))


SPLIT = 768


def solution(mesh):
    in_specs = (
        P("ep", "tp"),
        P("ep", "tp"),
        P("ep", "tp"),
        P("tp", "ep"),
        P("tp", None),
        P(),
        P("ep", None),
        P(),
        P(),
        P(),
        P("ep"),
        P("ep", None),
        P("ep", None, "tp"),
        P("ep", None, "tp"),
        P("ep", "tp", None),
    )
    out_specs = (P(("ep", "tp"), None), P(("ep", "tp"), None))
    return jax.shard_map(inner, mesh=mesh, in_specs=in_specs, out_specs=out_specs, check_vma=False)
```

```python
import functools
import math
import jax
import jax.numpy as jnp
from jax import lax
from jax.experimental import pallas as pl
from jax.experimental.pallas import tpu as pltpu
from jax.sharding import PartitionSpec as P

DH = 128
GROUPS = 4
BLOCK = 512
PLANE = 8
DEPTH = 4
ROOT = math.sqrt(DH)
LOG2E = 1.4426950408889634
SCALE = LOG2E / ROOT
QT = 256


def put_rows(stat, first, row, half):
    for h in range(2):
        rest = row[:, h * half : (h + 1) * half]
        for p in range(3):
            piece = rest.astype(jnp.bfloat16).astype(jnp.float32)
            stat[first + 3 * h + p : first + 3 * h + p + 1, :] = piece
            rest = rest - piece


def attend_kernel(
    pos_ref, q0, q1, q2, q3, kv_hbm, o0, o1, o2, o3,
    kv, raw, sems, wide, keys, values, even, odd, peak_even, peak_odd, top, gap, acc, stat,
):
    own, ahead = pos_ref[0], DEPTH - 1 - pos_ref[1]
    width = wide.shape[2]
    half = width // 2
    tiles = [slice(t * QT, (t + 1) * QT) for t in range(width // QT)]
    arriving = [pltpu.make_async_copy(q, raw.at[s], sems.at[s]) for s, q in enumerate((q0, q1, q2, q3))]
    arriving += [
        pltpu.make_async_copy(kv_hbm.at[b], kv.at[b], sems.at[DEPTH + b]) for b in range(PLANE)
    ]
    for c in arriving:
        c.start()
    top[...] = jnp.full_like(top, -1e30)
    acc[...] = jnp.zeros_like(acc)
    line = lax.broadcasted_iota(jnp.int32, (DH, width), 0)
    head = lax.broadcasted_iota(jnp.int32, (DH, width), 1) // half
    index = line % 8
    pick = (line < 16) & (index >= 3 * head) & (index < 3 * head + 3)
    picks = jnp.where(pick, -1.0, 0.0).astype(jnp.bfloat16)
    for s in range(DEPTH):
        arriving[s].wait()

    def turn(s, carry):
        turned = jnp.transpose(raw[s].astype(jnp.float32)).astype(jnp.bfloat16)
        for h in range(2):
            wide[s, :DH, h * half : (h + 1) * half] = turned[h * DH : (h + 1) * DH, :]
        wide[s, DH:, :] = picks
        return carry

    lax.fori_loop(0, ahead + 1, turn, 0)
    for b in range(PLANE):
        arriving[DEPTH + b].wait()
    sums = jnp.zeros((1, width), jnp.float32)
    first_total = None
    for b in reversed(range(PLANE)):
        gates = kv[b, BLOCK:, :]
        last = gates[:, DH:].astype(jnp.float32)
        total = jnp.concatenate(
            [
                jnp.broadcast_to(
                    last[8 + 3 * h : 9 + 3 * h, DH - 1 : DH]
                    + last[9 + 3 * h : 10 + 3 * h, DH - 1 : DH]
                    + last[10 + 3 * h : 11 + 3 * h, DH - 1 : DH],
                    (1, half),
                )
                for h in range(2)
            ],
            axis=1,
        )
        if b == PLANE - 1:
            first_total = total
        else:
            sums = sums + total
        gap[b] = sums

    def prepare(b, carry):
        gates = kv[b, BLOCK:, :]
        gates = jnp.concatenate([gates, jnp.zeros((DH - 16, 2 * DH), jnp.bfloat16)], axis=0)
        turned = jnp.transpose(gates.astype(jnp.float32)).astype(jnp.bfloat16)
        lane = lax.broadcasted_iota(jnp.int32, turned.shape, 1)
        zero = jnp.zeros_like(turned)
        keys[b, :, :DH] = kv[b, :BLOCK, :DH]
        keys[b, : 2 * DH, DH:] = jnp.where(lane < 8, turned, zero)
        keys[b, 2 * DH :, DH:] = jnp.where(lane < 8, zero, turned)
        for c in range(BLOCK // DH):
            values[b, :DH, c * DH : (c + 1) * DH] = kv[b, c * DH : (c + 1) * DH, DH:]
        values[b, DH:, :] = jnp.ones((16, BLOCK), jnp.bfloat16)
        return carry

    lax.fori_loop(0, PLANE, prepare, 0)
    steps = own + 1 + PLANE * ahead

    def place(n):
        m = jnp.maximum(n - (own + 1), 0)
        mine = n <= own
        s = jnp.where(mine, 0, jnp.minimum(1 + (m >> 3), DEPTH - 1))
        b = jnp.where(mine, own - n, PLANE - 1 - (m & 7))
        return s, b

    def score(s, b, t, into, peak, masked):
        scores = jnp.dot(keys[b], wide[s, :, tiles[t]], preferred_element_type=jnp.float32)
        if masked:
            key_at = lax.broadcasted_iota(jnp.int32, scores.shape, 0)
            query_at = lax.broadcasted_iota(jnp.int32, scores.shape, 1) + (t * QT) % half
            scores = jnp.where(key_at <= query_at, scores, -1e30)
        into[:, tiles[t]] = scores
        peak[:, tiles[t]] = jnp.max(scores, axis=0, keepdims=True)

    def absorb(s, b, dead, t, held, peak):
        cols = tiles[t]
        old = top[s, :, cols]
        shift = gap[b, :, cols] + dead
        new = jnp.maximum(old, peak[:, cols] + shift)
        top[s, :, cols] = new
        p = jnp.exp2(held[:, cols] * SCALE - (new - shift) * SCALE)
        part = jnp.dot(values[b], p.astype(jnp.bfloat16), preferred_element_type=jnp.float32)
        acc[s, :, cols] = acc[s, :, cols] * jnp.exp2((old - new) * SCALE) + part

    def phase(n, held, held_peak, into, into_peak):
        s, b = place(n)
        dead = jnp.where(n < steps, 0.0, -1e30)
        later_s, later_b = place(n + 1)
        for t in range(len(tiles)):
            score(later_s, later_b, t, into, into_peak, False)
            absorb(s, b, dead, t, held, held_peak)

    for t in range(len(tiles)):
        score(0, own, t, even, peak_even, True)

    def step(i, carry):
        phase(2 * i, even, peak_even, odd, peak_odd)
        phase(2 * i + 1, odd, peak_odd, even, peak_even)
        return carry

    lax.fori_loop(0, (steps + 1) >> 1, step, 0)
    for s, out in enumerate((o0, o1, o2, o3)):

        @pl.when(s <= ahead)
        def _():
            weight = acc[s, DH : DH + 1, :]
            mean = acc[s, :DH, :] / weight
            for h in range(2):
                out[h * DH : (h + 1) * DH, :] = mean[:, h * half : (h + 1) * half].astype(jnp.bfloat16)
            level = top[s] * SCALE + jnp.log(weight) * LOG2E
            if s == 0:
                level = level - gap[own] * SCALE
                passed = gap[0] - gap[own]
            else:
                level = level + first_total * SCALE
                passed = gap[0] + first_total
            stat[...] = jnp.zeros_like(stat)
            put_rows(stat, 0, level, half)
            put_rows(stat, 6, passed * SCALE, half)
            out[2 * DH :, :] = stat[...].astype(jnp.bfloat16)


def attend(pos, sets, kv):
    rows = sets[0].shape[0]
    width = 2 * rows
    return pl.pallas_call(
        attend_kernel,
        out_shape=[jax.ShapeDtypeStruct((2 * DH + 16, rows), jnp.bfloat16)] * DEPTH,
        in_specs=[pl.BlockSpec(memory_space=pltpu.SMEM)]
        + [pl.BlockSpec(memory_space=pltpu.HBM)] * (DEPTH + 1),
        out_specs=[pl.BlockSpec(memory_space=pltpu.VMEM)] * DEPTH,
        scratch_shapes=[
            pltpu.VMEM(kv.shape, jnp.bfloat16),
            pltpu.VMEM((DEPTH, rows, 2 * DH), jnp.bfloat16),
            pltpu.SemaphoreType.DMA((DEPTH + PLANE,)),
            pltpu.VMEM((DEPTH, 2 * DH, width), jnp.bfloat16),
            pltpu.VMEM((PLANE, BLOCK, 2 * DH), jnp.bfloat16),
            pltpu.VMEM((PLANE, DH + 16, BLOCK), jnp.bfloat16),
            pltpu.VMEM((BLOCK, width), jnp.float32),
            pltpu.VMEM((BLOCK, width), jnp.float32),
            pltpu.VMEM((1, width), jnp.float32),
            pltpu.VMEM((1, width), jnp.float32),
            pltpu.VMEM((DEPTH, 1, width), jnp.float32),
            pltpu.VMEM((PLANE, 1, width), jnp.float32),
            pltpu.VMEM((DEPTH, DH + 16, width), jnp.float32),
            pltpu.VMEM((16, rows), jnp.float32),
        ],
        cost_estimate=pl.CostEstimate(
            flops=9_000_000_000, bytes_accessed=4_000_000, transcendentals=16_000_000
        ),
    )(pos, *sets, kv)


def merge_kernel(pos_ref, p0, p1, p2, p3, w_ref, out_ref):
    depth = pos_ref[1]
    parts = (p0, p1, p2, p3)

    def read(ref, first):
        stat = ref[2 * DH :, :].astype(jnp.float32)
        return [
            sum(stat[first + 3 * h + p : first + 3 * h + p + 1, :] for p in range(3)) for h in range(2)
        ]

    merged = []
    passed = read(p0, 6)
    levels = [read(p0, 0)]
    for d in range(1, DEPTH):
        own = read(parts[d], 0)
        lost = jnp.where(d <= depth, 0.0, -1e30)
        levels.append([own[h] + passed[h] + lost for h in range(2)])
        more = read(parts[d], 6)
        passed = [passed[h] + more[h] for h in range(2)]
    for h in range(2):
        high = levels[0][h]
        for d in range(1, DEPTH):
            high = jnp.maximum(high, levels[d][h])
        weights = [jnp.exp2(levels[d][h] - high) for d in range(DEPTH)]
        total = weights[0] + weights[1] + weights[2] + weights[3]
        mixed = None
        for d in range(DEPTH):
            term = parts[d][h * DH : (h + 1) * DH, :].astype(jnp.float32) * (weights[d] / total)
            mixed = term if mixed is None else mixed + term
        merged.append(mixed)
    attended = jnp.transpose(jnp.concatenate(merged, axis=0)).astype(jnp.bfloat16)
    for n in range(0, out_ref.shape[1], 512):
        out_ref[:, n : n + 512] = jnp.dot(
            attended, w_ref[:, n : n + 512], preferred_element_type=jnp.float32
        ).astype(jnp.bfloat16)


def merge(pos, parts, w):
    rows = parts[0].shape[1]
    return pl.pallas_call(
        merge_kernel,
        out_shape=jax.ShapeDtypeStruct((rows, w.shape[1]), jnp.bfloat16),
        in_specs=[pl.BlockSpec(memory_space=pltpu.SMEM)]
        + [pl.BlockSpec(memory_space=pltpu.VMEM)] * (DEPTH + 1),
        out_specs=pl.BlockSpec(memory_space=pltpu.VMEM),
        cost_estimate=pl.CostEstimate(
            flops=2 * rows * w.shape[0] * w.shape[1], bytes_accessed=4_000_000, transcendentals=8 * rows
        ),
    )(pos, *parts, w)


def three(x):
    hi = lax.reduce_precision(x, 8, 7)
    mid = lax.reduce_precision(x - hi, 8, 7)
    return jnp.stack([hi, mid, x - hi - mid], axis=-2).astype(jnp.bfloat16)


def pack(keys, values, gates):
    turned = values.reshape(BLOCK // DH, DH, DH).transpose(0, 2, 1).reshape(BLOCK, DH)
    parts = three(gates * ROOT).reshape(6, 2, 2 * DH).transpose(1, 0, 2)
    parts = jnp.pad(parts, ((0, 0), (0, 2), (0, 0))).reshape(16, 2 * DH)
    return jnp.concatenate([jnp.concatenate([keys, turned], axis=1), parts], axis=0)


def hidden_kernel(count, x_hbm, *refs):
    weights, (out_ref, x_ref, both, sems) = refs[: 2 * count], refs[2 * count :]
    ff = both.shape[2] // 2
    copies = [pltpu.make_async_copy(x_hbm, x_ref, sems.at[2 * count])]
    for q in range(count):
        copies.append(pltpu.make_async_copy(weights[2 * q], both.at[q, :, :ff], sems.at[2 * q]))
        copies.append(pltpu.make_async_copy(weights[2 * q + 1], both.at[q, :, ff:], sems.at[2 * q + 1]))
    for c in copies:
        c.start()
    copies[0].wait()
    for q in range(count):
        copies[1 + 2 * q].wait()
        copies[2 + 2 * q].wait()
        for r in range(0, x_ref.shape[0], 256):
            lines = slice(r, r + 256)
            pre = jnp.dot(x_ref[lines, :], both[q], preferred_element_type=jnp.float32)
            gated, lifted = pre[:, :ff], pre[:, ff:]
            out_ref[lines, q * ff : (q + 1) * ff] = (gated * jax.nn.sigmoid(gated) * lifted).astype(
                jnp.bfloat16
            )


def hidden_units(x, weights):
    rows, width = x.shape
    count, ff = len(weights) // 2, weights[0].shape[1]
    return pl.pallas_call(
        functools.partial(hidden_kernel, count),
        out_shape=jax.ShapeDtypeStruct((rows, count * ff), jnp.bfloat16),
        in_specs=[pl.BlockSpec(memory_space=pltpu.HBM)] * (1 + len(weights)),
        out_specs=pl.BlockSpec(memory_space=pltpu.VMEM),
        scratch_shapes=[
            pltpu.VMEM((rows, width), jnp.bfloat16),
            pltpu.VMEM((count, width, 2 * ff), jnp.bfloat16),
            pltpu.SemaphoreType.DMA((1 + 2 * count,)),
        ],
        cost_estimate=pl.CostEstimate(
            flops=count * 4 * rows * width * ff,
            bytes_accessed=count * 4 * width * ff,
            transcendentals=rows * count * ff,
        ),
    )(x, *weights)


def down_kernel(count, hidden_hbm, *refs):
    weights, (out_hbm, hidden, down, out, sems) = refs[:count], refs[count:]
    ff = down.shape[0] // count
    pairs = [(hidden_hbm, hidden)]
    pairs += [(w, down.at[q * ff : (q + 1) * ff, :]) for q, w in enumerate(weights)]
    copies = [pltpu.make_async_copy(src, dst, sems.at[k]) for k, (src, dst) in enumerate(pairs)]
    for c in copies:
        c.start()
    for c in copies:
        c.wait()
    stores = []
    for n in range(0, out.shape[1], 256):
        cols = slice(n, n + 256)
        out[:, cols] = jnp.dot(hidden[...], down[:, cols], preferred_element_type=jnp.float32).astype(
            out.dtype
        )
        stores.append(
            pltpu.make_async_copy(
                out.at[:, cols], out_hbm.at[:, cols], sems.at[len(pairs) + len(stores)]
            )
        )
        stores[-1].start()
    for c in stores:
        c.wait()


def down_columns(hidden, weights):
    rows, count = hidden.shape[0], len(weights)
    ff, columns = weights[0].shape
    return pl.pallas_call(
        functools.partial(down_kernel, count),
        out_shape=jax.ShapeDtypeStruct((rows, columns), jnp.bfloat16),
        in_specs=[pl.BlockSpec(memory_space=pltpu.HBM)] * (1 + count),
        out_specs=pl.BlockSpec(memory_space=pltpu.HBM),
        scratch_shapes=[
            pltpu.VMEM((rows, count * ff), jnp.bfloat16),
            pltpu.VMEM((count * ff, columns), jnp.bfloat16),
            pltpu.VMEM((rows, columns), jnp.bfloat16),
            pltpu.SemaphoreType.DMA((1 + count + columns // 256,)),
        ],
        cost_estimate=pl.CostEstimate(
            flops=2 * rows * count * ff * columns,
            bytes_accessed=2 * count * ff * columns,
            transcendentals=0,
        ),
    )(hidden, *weights)


def shift(x, by):
    count = lax.axis_size("tp")
    return lax.ppermute(x, "tp", [(i, (i + by) % count) for i in range(count)])


def rms_scale(row_block, scale_gain):
    values = row_block.astype(jnp.float32)
    return (
        values * lax.rsqrt(jnp.mean(values * values, axis=-1, keepdims=True) + 1e-06) * scale_gain
    )


def inner(
    queries,
    key_rows,
    value_rows,
    forget_logit,
    out_weight,
    out_gain,
    moe_input,
    moe_gain,
    router_group,
    router_expert,
    route_group,
    route_pick,
    expert_gate,
    expert_up,
    expert_down,
):
    tp_count = lax.axis_size("tp")
    ep_count = lax.axis_size("ep")
    tp_index = lax.axis_index("tp")
    ep_index = lax.axis_index("ep")
    group_rows, width_model = moe_input.shape
    own_rows = group_rows // tp_count
    experts = ep_count
    per_group = experts // GROUPS
    capacity = tp_count * own_rows // experts
    slots = experts * capacity

    gate, up, down = expert_gate[0], expert_up[0], expert_down[0]
    half = gate.shape[1] // 2
    low, low_a, low_b = down[:, :SPLIT], down[:half, SPLIT:], down[half:, SPLIT:]
    left_gate, right_up = shift(gate, 1), shift(up, -1)
    left_low, right_low = shift(low, 1), shift(low, -1)
    left_a, right_a = shift(low_a, 1), shift(low_a, -1)
    left_b, right_b = shift(low_b, 1), shift(low_b, -1)
    left_up, right_gate = shift(up, 1), shift(gate, -1)
    far_gate, far_up = shift(left_gate, 1), shift(right_up, -1)
    far_low = shift(left_low, 1)
    far_a, far_b = shift(right_a, -1), shift(left_b, 1)
    lows = (
        (low, left_low, right_low, far_low),
        (low_a, low_b, left_a, left_b, right_a, right_b, far_a, far_b),
    )

    running = jnp.cumsum(jax.nn.log_sigmoid(forget_logit), axis=1)
    packed = pack(key_rows, value_rows, running)
    planes = [[z * PLANE + i for i in range(PLANE)] for z in range(ep_count // PLANE)]
    gathered = lax.all_gather(packed, "ep", axis=0, tiled=True, axis_index_groups=planes)
    gathered = gathered.reshape(PLANE, *packed.shape)
    place = jnp.stack([ep_index % PLANE, ep_index // PLANE])
    asked = [queries]
    for d in range(1, DEPTH):
        pairs = [(i, i - PLANE * d) for i in range(PLANE * d, ep_count)]
        asked.append(lax.ppermute(queries, "ep", pairs))
    answers = attend(place, asked, gathered)
    told = [answers[0]]
    for d in range(1, DEPTH):
        pairs = [(i, i + PLANE * d) for i in range(ep_count - PLANE * d)]
        told.append(lax.ppermute(answers[d], "ep", pairs))

    own_first = tp_index * own_rows
    own_group = lax.dynamic_slice_in_dim(route_group, own_first, own_rows, 0)
    own_pick = lax.dynamic_slice_in_dim(route_pick, own_first, own_rows, 0)
    chosen = own_group[:, None] * per_group + own_pick
    expert_hit = chosen[:, :, None] == jnp.arange(experts, dtype=jnp.int32)
    usage = jnp.any(expert_hit, axis=1).astype(jnp.bfloat16)
    line = jnp.arange(own_rows, dtype=jnp.int32)
    earlier = (line[None, :] < line[:, None]).astype(jnp.bfloat16)
    before = jnp.dot(earlier, usage, preferred_element_type=jnp.float32).astype(jnp.int32)
    ranks = jnp.sum(jnp.where(expert_hit, before[:, None, :], 0), axis=2)
    target = jnp.where(ranks < capacity, chosen * capacity + ranks, slots)
    normed = rms_scale(
        lax.dynamic_slice_in_dim(moe_input, own_first, own_rows, 0), moe_gain
    ).astype(jnp.bfloat16)
    slot_at = jnp.arange(slots, dtype=jnp.int32)[:, None]
    sent = ((slot_at == target[None, :, 0]) | (slot_at == target[None, :, 1])).astype(jnp.bfloat16)
    outgoing = jnp.dot(sent, normed, preferred_element_type=jnp.float32).astype(jnp.bfloat16)
    outgoing = outgoing.reshape(experts, capacity, width_model)
    arrived = lax.all_to_all(outgoing, "ep", split_axis=0, concat_axis=0, tiled=True)
    arrived = arrived.reshape(slots, width_model)

    hidden = hidden_units(
        arrived, (gate, up, left_gate, left_up, right_gate, right_up, far_gate, far_up)
    )
    mixer_term = merge(place, told, out_weight)
    returned = []
    for k in range(2):
        results = down_columns(hidden, lows[k])
        back = lax.all_to_all(
            results.reshape(experts, capacity, -1), "ep", split_axis=0, concat_axis=0, tiled=True
        )
        returned.append(back.reshape(slots, -1))
    mixer_summed = lax.psum_scatter(mixer_term, "tp", scatter_dimension=0, tiled=True)
    mixer_out = rms_scale(mixer_summed, out_gain).astype(jnp.bfloat16)

    mixer_out, returned[1] = lax.optimization_barrier((mixer_out, returned[1]))
    group_logits = jnp.dot(normed, router_group, preferred_element_type=jnp.float32)
    expert_logits = jnp.dot(normed, router_expert, preferred_element_type=jnp.float32)
    group_top = jnp.max(group_logits, axis=1, keepdims=True)
    group_exp = jnp.exp(group_logits - group_top)
    group_hit = jnp.arange(GROUPS, dtype=jnp.int32)[None, :] == own_group[:, None]
    group_share = jnp.sum(jnp.where(group_hit, group_exp, 0.0), axis=1) / jnp.sum(group_exp, axis=1)
    picked_logits = jnp.sum(jnp.where(expert_hit, expert_logits[:, None, :], 0.0), axis=2)
    shares = group_share[:, None] * jax.nn.sigmoid(picked_logits - picked_logits[:, ::-1])
    column = jnp.arange(slots, dtype=jnp.int32)[None, :]
    weight = jnp.where(column == target[:, :1], shares[:, :1], 0.0) + jnp.where(
        column == target[:, 1:], shares[:, 1:], 0.0
    )
    high = lax.reduce_precision(weight, 8, 7)
    both = jnp.concatenate([high, weight - high], axis=1).astype(jnp.bfloat16)
    moe_out = jnp.concatenate(
        [
            jnp.dot(both, jnp.concatenate([back, back], axis=0), preferred_element_type=jnp.float32)
            for back in returned
        ],
        axis=1,
    )
    return (mixer_out, moe_out.astype(jnp.bfloat16))


SPLIT = 768


def solution(mesh):
    in_specs = (
        P("ep", "tp"),
        P("ep", "tp"),
        P("ep", "tp"),
        P("tp", "ep"),
        P("tp", None),
        P(),
        P("ep", None),
        P(),
        P(),
        P(),
        P("ep"),
        P("ep", None),
        P("ep", None, "tp"),
        P("ep", None, "tp"),
        P("ep", "tp", None),
    )
    out_specs = (P(("ep", "tp"), None), P(("ep", "tp"), None))
    return jax.shard_map(inner, mesh=mesh, in_specs=in_specs, out_specs=out_specs, check_vma=False)
```

```python
import functools
import math
import jax
import jax.numpy as jnp
from jax import lax
from jax.experimental import pallas as pl
from jax.experimental.pallas import tpu as pltpu
from jax.sharding import PartitionSpec as P

DH = 128
GROUPS = 4
BLOCK = 512
PLANE = 8
DEPTH = 4
ROOT = math.sqrt(DH)
LOG2E = 1.4426950408889634
SCALE = LOG2E / ROOT
QT = 256


def put_rows(stat, first, row, half):
    for h in range(2):
        rest = row[:, h * half : (h + 1) * half]
        for p in range(3):
            piece = rest.astype(jnp.bfloat16).astype(jnp.float32)
            stat[first + 3 * h + p : first + 3 * h + p + 1, :] = piece
            rest = rest - piece


def attend_kernel(
    pos_ref, q0, q1, q2, q3, kv_hbm, o0, o1, o2, o3,
    kv, raw, sems, wide, keys, values, even, odd, peak_even, peak_odd, top, gap, acc, stat,
):
    own, ahead = pos_ref[0], DEPTH - 1 - pos_ref[1]
    width = wide.shape[2]
    half = width // 2
    tiles = [slice(t * QT, (t + 1) * QT) for t in range(width // QT)]
    arriving = [pltpu.make_async_copy(q, raw.at[s], sems.at[s]) for s, q in enumerate((q0, q1, q2, q3))]
    arriving += [
        pltpu.make_async_copy(kv_hbm.at[b], kv.at[b], sems.at[DEPTH + b]) for b in range(PLANE)
    ]
    for c in arriving:
        c.start()
    top[...] = jnp.full_like(top, -1e30)
    acc[...] = jnp.zeros_like(acc)
    line = lax.broadcasted_iota(jnp.int32, (DH, width), 0)
    head = lax.broadcasted_iota(jnp.int32, (DH, width), 1) // half
    index = line % 8
    pick = (line < 16) & (index >= 3 * head) & (index < 3 * head + 3)
    picks = jnp.where(pick, -1.0, 0.0).astype(jnp.bfloat16)
    for s in range(DEPTH):
        arriving[s].wait()

    def turn(s, carry):
        turned = jnp.transpose(raw[s].astype(jnp.float32)).astype(jnp.bfloat16)
        for h in range(2):
            wide[s, :DH, h * half : (h + 1) * half] = turned[h * DH : (h + 1) * DH, :]
        wide[s, DH:, :] = picks
        return carry

    lax.fori_loop(0, ahead + 1, turn, 0)
    for b in range(PLANE):
        arriving[DEPTH + b].wait()
    sums = jnp.zeros((1, width), jnp.float32)
    first_total = None
    for b in reversed(range(PLANE)):
        gates = kv[b, BLOCK:, :]
        last = gates[:, DH:].astype(jnp.float32)
        total = jnp.concatenate(
            [
                jnp.broadcast_to(
                    last[8 + 3 * h : 9 + 3 * h, DH - 1 : DH]
                    + last[9 + 3 * h : 10 + 3 * h, DH - 1 : DH]
                    + last[10 + 3 * h : 11 + 3 * h, DH - 1 : DH],
                    (1, half),
                )
                for h in range(2)
            ],
            axis=1,
        )
        if b == PLANE - 1:
            first_total = total
        else:
            sums = sums + total
        gap[b] = sums

    def prepare(b, carry):
        gates = kv[b, BLOCK:, :]
        gates = jnp.concatenate([gates, jnp.zeros((DH - 16, 2 * DH), jnp.bfloat16)], axis=0)
        turned = jnp.transpose(gates.astype(jnp.float32)).astype(jnp.bfloat16)
        lane = lax.broadcasted_iota(jnp.int32, turned.shape, 1)
        zero = jnp.zeros_like(turned)
        keys[b, :, :DH] = kv[b, :BLOCK, :DH]
        keys[b, : 2 * DH, DH:] = jnp.where(lane < 8, turned, zero)
        keys[b, 2 * DH :, DH:] = jnp.where(lane < 8, zero, turned)
        for c in range(BLOCK // DH):
            values[b, :DH, c * DH : (c + 1) * DH] = kv[b, c * DH : (c + 1) * DH, DH:]
        values[b, DH:, :] = jnp.ones((16, BLOCK), jnp.bfloat16)
        return carry

    lax.fori_loop(0, PLANE, prepare, 0)
    steps = own + 1 + PLANE * ahead

    def place(n):
        m = jnp.maximum(n - (own + 1), 0)
        mine = n <= own
        s = jnp.where(mine, 0, jnp.minimum(1 + (m >> 3), DEPTH - 1))
        b = jnp.where(mine, own - n, PLANE - 1 - (m & 7))
        return s, b

    def score(s, b, t, into, peak, masked):
        scores = jnp.dot(keys[b], wide[s, :, tiles[t]], preferred_element_type=jnp.float32)
        if masked:
            key_at = lax.broadcasted_iota(jnp.int32, scores.shape, 0)
            query_at = lax.broadcasted_iota(jnp.int32, scores.shape, 1) + (t * QT) % half
            scores = jnp.where(key_at <= query_at, scores, -1e30)
        into[:, tiles[t]] = scores
        peak[:, tiles[t]] = jnp.max(scores, axis=0, keepdims=True)

    def absorb(s, b, dead, t, held, peak):
        cols = tiles[t]
        old = top[s, :, cols]
        shift = gap[b, :, cols] + dead
        new = jnp.maximum(old, peak[:, cols] + shift)
        top[s, :, cols] = new
        p = jnp.exp2(held[:, cols] * SCALE - (new - shift) * SCALE)
        part = jnp.dot(values[b], p.astype(jnp.bfloat16), preferred_element_type=jnp.float32)
        acc[s, :, cols] = acc[s, :, cols] * jnp.exp2((old - new) * SCALE) + part

    def phase(n, held, held_peak, into, into_peak):
        s, b = place(n)
        dead = jnp.where(n < steps, 0.0, -1e30)
        later_s, later_b = place(n + 1)
        for t in range(len(tiles)):
            score(later_s, later_b, t, into, into_peak, False)
            absorb(s, b, dead, t, held, held_peak)

    for t in range(len(tiles)):
        score(0, own, t, even, peak_even, True)

    def step(i, carry):
        phase(2 * i, even, peak_even, odd, peak_odd)
        phase(2 * i + 1, odd, peak_odd, even, peak_even)
        return carry

    lax.fori_loop(0, (steps + 1) >> 1, step, 0)
    for s, out in enumerate((o0, o1, o2, o3)):

        @pl.when(s <= ahead)
        def _():
            weight = acc[s, DH : DH + 1, :]
            mean = acc[s, :DH, :] / weight
            for h in range(2):
                out[h * DH : (h + 1) * DH, :] = mean[:, h * half : (h + 1) * half].astype(jnp.bfloat16)
            level = top[s] * SCALE + jnp.log(weight) * LOG2E
            if s == 0:
                level = level - gap[own] * SCALE
                passed = gap[0] - gap[own]
            else:
                level = level + first_total * SCALE
                passed = gap[0] + first_total
            stat[...] = jnp.zeros_like(stat)
            put_rows(stat, 0, level, half)
            put_rows(stat, 6, passed * SCALE, half)
            out[2 * DH :, :] = stat[...].astype(jnp.bfloat16)


def attend(pos, sets, kv):
    rows = sets[0].shape[0]
    width = 2 * rows
    return pl.pallas_call(
        attend_kernel,
        out_shape=[jax.ShapeDtypeStruct((2 * DH + 16, rows), jnp.bfloat16)] * DEPTH,
        in_specs=[pl.BlockSpec(memory_space=pltpu.SMEM)]
        + [pl.BlockSpec(memory_space=pltpu.HBM)] * (DEPTH + 1),
        out_specs=[pl.BlockSpec(memory_space=pltpu.VMEM)] * DEPTH,
        scratch_shapes=[
            pltpu.VMEM(kv.shape, jnp.bfloat16),
            pltpu.VMEM((DEPTH, rows, 2 * DH), jnp.bfloat16),
            pltpu.SemaphoreType.DMA((DEPTH + PLANE,)),
            pltpu.VMEM((DEPTH, 2 * DH, width), jnp.bfloat16),
            pltpu.VMEM((PLANE, BLOCK, 2 * DH), jnp.bfloat16),
            pltpu.VMEM((PLANE, DH + 16, BLOCK), jnp.bfloat16),
            pltpu.VMEM((BLOCK, width), jnp.float32),
            pltpu.VMEM((BLOCK, width), jnp.float32),
            pltpu.VMEM((1, width), jnp.float32),
            pltpu.VMEM((1, width), jnp.float32),
            pltpu.VMEM((DEPTH, 1, width), jnp.float32),
            pltpu.VMEM((PLANE, 1, width), jnp.float32),
            pltpu.VMEM((DEPTH, DH + 16, width), jnp.float32),
            pltpu.VMEM((16, rows), jnp.float32),
        ],
        cost_estimate=pl.CostEstimate(
            flops=9_000_000_000, bytes_accessed=4_000_000, transcendentals=16_000_000
        ),
    )(pos, *sets, kv)


def merge_kernel(pos_ref, p0, p1, p2, p3, w_ref, out_ref):
    depth = pos_ref[1]
    parts = (p0, p1, p2, p3)

    def read(ref, first):
        stat = ref[2 * DH :, :].astype(jnp.float32)
        return [
            sum(stat[first + 3 * h + p : first + 3 * h + p + 1, :] for p in range(3)) for h in range(2)
        ]

    merged = []
    passed = read(p0, 6)
    levels = [read(p0, 0)]
    for d in range(1, DEPTH):
        own = read(parts[d], 0)
        lost = jnp.where(d <= depth, 0.0, -1e30)
        levels.append([own[h] + passed[h] + lost for h in range(2)])
        more = read(parts[d], 6)
        passed = [passed[h] + more[h] for h in range(2)]
    for h in range(2):
        high = levels[0][h]
        for d in range(1, DEPTH):
            high = jnp.maximum(high, levels[d][h])
        weights = [jnp.exp2(levels[d][h] - high) for d in range(DEPTH)]
        total = weights[0] + weights[1] + weights[2] + weights[3]
        mixed = None
        for d in range(DEPTH):
            term = parts[d][h * DH : (h + 1) * DH, :].astype(jnp.float32) * (weights[d] / total)
            mixed = term if mixed is None else mixed + term
        merged.append(mixed)
    attended = jnp.transpose(jnp.concatenate(merged, axis=0)).astype(jnp.bfloat16)
    for n in range(0, out_ref.shape[1], 512):
        out_ref[:, n : n + 512] = jnp.dot(
            attended, w_ref[:, n : n + 512], preferred_element_type=jnp.float32
        ).astype(jnp.bfloat16)


def merge(pos, parts, w):
    rows = parts[0].shape[1]
    return pl.pallas_call(
        merge_kernel,
        out_shape=jax.ShapeDtypeStruct((rows, w.shape[1]), jnp.bfloat16),
        in_specs=[pl.BlockSpec(memory_space=pltpu.SMEM)]
        + [pl.BlockSpec(memory_space=pltpu.VMEM)] * (DEPTH + 1),
        out_specs=pl.BlockSpec(memory_space=pltpu.VMEM),
        cost_estimate=pl.CostEstimate(
            flops=2 * rows * w.shape[0] * w.shape[1], bytes_accessed=4_000_000, transcendentals=8 * rows
        ),
    )(pos, *parts, w)


def three(x):
    hi = lax.reduce_precision(x, 8, 7)
    mid = lax.reduce_precision(x - hi, 8, 7)
    return jnp.stack([hi, mid, x - hi - mid], axis=-2).astype(jnp.bfloat16)


def pack(keys, values, gates):
    turned = values.reshape(BLOCK // DH, DH, DH).transpose(0, 2, 1).reshape(BLOCK, DH)
    parts = three(gates * ROOT).reshape(6, 2, 2 * DH).transpose(1, 0, 2)
    parts = jnp.pad(parts, ((0, 0), (0, 2), (0, 0))).reshape(16, 2 * DH)
    return jnp.concatenate([jnp.concatenate([keys, turned], axis=1), parts], axis=0)


def hidden_kernel(count, x_hbm, *refs):
    weights, (out_ref, x_ref, both, sems) = refs[: 2 * count], refs[2 * count :]
    ff = both.shape[2] // 2
    copies = [pltpu.make_async_copy(x_hbm, x_ref, sems.at[2 * count])]
    for q in range(count):
        copies.append(pltpu.make_async_copy(weights[2 * q], both.at[q, :, :ff], sems.at[2 * q]))
        copies.append(pltpu.make_async_copy(weights[2 * q + 1], both.at[q, :, ff:], sems.at[2 * q + 1]))
    for c in copies:
        c.start()
    copies[0].wait()
    for q in range(count):
        copies[1 + 2 * q].wait()
        copies[2 + 2 * q].wait()
        for r in range(0, x_ref.shape[0], 256):
            lines = slice(r, r + 256)
            pre = jnp.dot(x_ref[lines, :], both[q], preferred_element_type=jnp.float32)
            gated, lifted = pre[:, :ff], pre[:, ff:]
            out_ref[lines, q * ff : (q + 1) * ff] = (gated * jax.nn.sigmoid(gated) * lifted).astype(
                jnp.bfloat16
            )


def hidden_units(x, weights):
    rows, width = x.shape
    count, ff = len(weights) // 2, weights[0].shape[1]
    return pl.pallas_call(
        functools.partial(hidden_kernel, count),
        out_shape=jax.ShapeDtypeStruct((rows, count * ff), jnp.bfloat16),
        in_specs=[pl.BlockSpec(memory_space=pltpu.HBM)] * (1 + len(weights)),
        out_specs=pl.BlockSpec(memory_space=pltpu.VMEM),
        scratch_shapes=[
            pltpu.VMEM((rows, width), jnp.bfloat16),
            pltpu.VMEM((count, width, 2 * ff), jnp.bfloat16),
            pltpu.SemaphoreType.DMA((1 + 2 * count,)),
        ],
        cost_estimate=pl.CostEstimate(
            flops=count * 4 * rows * width * ff,
            bytes_accessed=count * 4 * width * ff,
            transcendentals=rows * count * ff,
        ),
    )(x, *weights)


def down_kernel(count, near_hbm, far_hbm, *refs):
    weights, (out_hbm, hidden, down, out, sems) = refs[:count], refs[count:]
    ff = down.shape[0] // count
    split = near_hbm.shape[1]
    pairs = [(near_hbm, hidden.at[:, :split]), (far_hbm, hidden.at[:, split:])]
    pairs += [(w, down.at[q * ff : (q + 1) * ff, :]) for q, w in enumerate(weights)]
    copies = [pltpu.make_async_copy(src, dst, sems.at[k]) for k, (src, dst) in enumerate(pairs)]
    for c in copies:
        c.start()
    for c in copies:
        c.wait()
    stores = []
    for n in range(0, out.shape[1], 256):
        cols = slice(n, n + 256)
        out[:, cols] = jnp.dot(hidden[...], down[:, cols], preferred_element_type=jnp.float32).astype(
            out.dtype
        )
        stores.append(
            pltpu.make_async_copy(
                out.at[:, cols], out_hbm.at[:, cols], sems.at[len(pairs) + len(stores)]
            )
        )
        stores[-1].start()
    for c in stores:
        c.wait()


def down_columns(near, far, weights):
    rows, count = near.shape[0], len(weights)
    ff, columns = weights[0].shape
    return pl.pallas_call(
        functools.partial(down_kernel, count),
        out_shape=jax.ShapeDtypeStruct((rows, columns), jnp.bfloat16),
        in_specs=[pl.BlockSpec(memory_space=pltpu.HBM)] * (2 + count),
        out_specs=pl.BlockSpec(memory_space=pltpu.HBM),
        scratch_shapes=[
            pltpu.VMEM((rows, count * ff), jnp.bfloat16),
            pltpu.VMEM((count * ff, columns), jnp.bfloat16),
            pltpu.VMEM((rows, columns), jnp.bfloat16),
            pltpu.SemaphoreType.DMA((2 + count + columns // 256,)),
        ],
        cost_estimate=pl.CostEstimate(
            flops=2 * rows * count * ff * columns,
            bytes_accessed=2 * count * ff * columns,
            transcendentals=0,
        ),
    )(near, far, *weights)


def shift(x, by):
    count = lax.axis_size("tp")
    return lax.ppermute(x, "tp", [(i, (i + by) % count) for i in range(count)])


def rms_scale(row_block, scale_gain):
    values = row_block.astype(jnp.float32)
    return (
        values * lax.rsqrt(jnp.mean(values * values, axis=-1, keepdims=True) + 1e-06) * scale_gain
    )


def inner(
    queries,
    key_rows,
    value_rows,
    forget_logit,
    out_weight,
    out_gain,
    moe_input,
    moe_gain,
    router_group,
    router_expert,
    route_group,
    route_pick,
    expert_gate,
    expert_up,
    expert_down,
):
    tp_count = lax.axis_size("tp")
    ep_count = lax.axis_size("ep")
    tp_index = lax.axis_index("tp")
    ep_index = lax.axis_index("ep")
    group_rows, width_model = moe_input.shape
    own_rows = group_rows // tp_count
    experts = ep_count
    per_group = experts // GROUPS
    capacity = tp_count * own_rows // experts
    slots = experts * capacity

    gate, up, down = expert_gate[0], expert_up[0], expert_down[0]
    cuts = (slice(0, SPLIT), slice(SPLIT, width_model))
    low = [down[:, c] for c in cuts]
    left_gate, right_up = shift(gate, 1), shift(up, -1)
    left_low = [shift(low[0], 1), shift(low[1], 1)]
    right_low = [shift(low[0], -1), shift(low[1], -1)]
    left_up, right_gate = shift(up, 1), shift(gate, -1)
    far_gate, far_up = shift(left_gate, 1), shift(right_up, -1)
    far_low = [shift(left_low[0], 1), shift(right_low[1], -1)]

    running = jnp.cumsum(jax.nn.log_sigmoid(forget_logit), axis=1)
    packed = pack(key_rows, value_rows, running)
    planes = [[z * PLANE + i for i in range(PLANE)] for z in range(ep_count // PLANE)]
    gathered = lax.all_gather(packed, "ep", axis=0, tiled=True, axis_index_groups=planes)
    gathered = gathered.reshape(PLANE, *packed.shape)
    place = jnp.stack([ep_index % PLANE, ep_index // PLANE])
    asked = [queries]
    for d in range(1, DEPTH):
        pairs = [(i, i - PLANE * d) for i in range(PLANE * d, ep_count)]
        asked.append(lax.ppermute(queries, "ep", pairs))
    answers = attend(place, asked, gathered)
    told = [answers[0]]
    for d in range(1, DEPTH):
        pairs = [(i, i + PLANE * d) for i in range(ep_count - PLANE * d)]
        told.append(lax.ppermute(answers[d], "ep", pairs))

    own_first = tp_index * own_rows
    own_group = lax.dynamic_slice_in_dim(route_group, own_first, own_rows, 0)
    own_pick = lax.dynamic_slice_in_dim(route_pick, own_first, own_rows, 0)
    chosen = own_group[:, None] * per_group + own_pick
    expert_hit = chosen[:, :, None] == jnp.arange(experts, dtype=jnp.int32)
    usage = jnp.any(expert_hit, axis=1).astype(jnp.bfloat16)
    line = jnp.arange(own_rows, dtype=jnp.int32)
    earlier = (line[None, :] < line[:, None]).astype(jnp.bfloat16)
    before = jnp.dot(earlier, usage, preferred_element_type=jnp.float32).astype(jnp.int32)
    ranks = jnp.sum(jnp.where(expert_hit, before[:, None, :], 0), axis=2)
    target = jnp.where(ranks < capacity, chosen * capacity + ranks, slots)
    normed = rms_scale(
        lax.dynamic_slice_in_dim(moe_input, own_first, own_rows, 0), moe_gain
    ).astype(jnp.bfloat16)
    slot_at = jnp.arange(slots, dtype=jnp.int32)[:, None]
    sent = ((slot_at == target[None, :, 0]) | (slot_at == target[None, :, 1])).astype(jnp.bfloat16)
    outgoing = jnp.dot(sent, normed, preferred_element_type=jnp.float32).astype(jnp.bfloat16)
    outgoing = outgoing.reshape(experts, capacity, width_model)
    arrived = lax.all_to_all(outgoing, "ep", split_axis=0, concat_axis=0, tiled=True)
    arrived = arrived.reshape(slots, width_model)

    near = hidden_units(arrived, (gate, up, left_gate, left_up, right_gate, right_up))
    far = hidden_units(arrived, (far_gate, far_up))
    mixer_term = merge(place, told, out_weight)
    mixer_term, far_low[1] = lax.optimization_barrier((mixer_term, far_low[1]))
    returned = []
    for k in range(2):
        results = down_columns(near, far, (low[k], left_low[k], right_low[k], far_low[k]))
        back = lax.all_to_all(
            results.reshape(experts, capacity, -1), "ep", split_axis=0, concat_axis=0, tiled=True
        )
        returned.append(back.reshape(slots, -1))
    mixer_summed = lax.psum_scatter(mixer_term, "tp", scatter_dimension=0, tiled=True)
    mixer_out = rms_scale(mixer_summed, out_gain).astype(jnp.bfloat16)

    mixer_out, returned[1] = lax.optimization_barrier((mixer_out, returned[1]))
    group_logits = jnp.dot(normed, router_group, preferred_element_type=jnp.float32)
    expert_logits = jnp.dot(normed, router_expert, preferred_element_type=jnp.float32)
    group_top = jnp.max(group_logits, axis=1, keepdims=True)
    group_exp = jnp.exp(group_logits - group_top)
    group_hit = jnp.arange(GROUPS, dtype=jnp.int32)[None, :] == own_group[:, None]
    group_share = jnp.sum(jnp.where(group_hit, group_exp, 0.0), axis=1) / jnp.sum(group_exp, axis=1)
    picked_logits = jnp.sum(jnp.where(expert_hit, expert_logits[:, None, :], 0.0), axis=2)
    shares = group_share[:, None] * jax.nn.sigmoid(picked_logits - picked_logits[:, ::-1])
    column = jnp.arange(slots, dtype=jnp.int32)[None, :]
    weight = jnp.where(column == target[:, :1], shares[:, :1], 0.0) + jnp.where(
        column == target[:, 1:], shares[:, 1:], 0.0
    )
    high = lax.reduce_precision(weight, 8, 7)
    both = jnp.concatenate([high, weight - high], axis=1).astype(jnp.bfloat16)
    moe_out = jnp.concatenate(
        [
            jnp.dot(both, jnp.concatenate([back, back], axis=0), preferred_element_type=jnp.float32)
            for back in returned
        ],
        axis=1,
    )
    return (mixer_out, moe_out.astype(jnp.bfloat16))


SPLIT = 512


def solution(mesh):
    in_specs = (
        P("ep", "tp"),
        P("ep", "tp"),
        P("ep", "tp"),
        P("tp", "ep"),
        P("tp", None),
        P(),
        P("ep", None),
        P(),
        P(),
        P(),
        P("ep"),
        P("ep", None),
        P("ep", None, "tp"),
        P("ep", None, "tp"),
        P("ep", "tp", None),
    )
    out_specs = (P(("ep", "tp"), None), P(("ep", "tp"), None))
    return jax.shard_map(inner, mesh=mesh, in_specs=in_specs, out_specs=out_specs, check_vma=False)
```
